512 devices in a mesh: sp: 128 (over z, y, core), tp: 4 (over x).
Axes of the slice: x: 4, y: 8, z: 8, core: 2. Of those that a mesh axis runs over, the one named last changes fastest.
Arguments:
- tokens: bfloat16 [24576, 2048], P('sp', 'tp'), may hold values from -6 to 6
- norm_gain: float32 [2048], replicated, may hold values from 0.1 to 1.9
- query_weight: bfloat16 [2048, 512], P('sp', 'tp'), may hold values from -0.125 to 0.125
- key_weight: bfloat16 [2048, 512], P('sp', 'tp'), may hold values from -0.125 to 0.125
- value_weight: bfloat16 [2048, 512], P('sp', 'tp'), may hold values from -0.125 to 0.125
- decay_weight: bfloat16 [2048, 512], P('sp', 'tp'), may hold values from -0.09375 to 0.09375
- removal_weight: bfloat16 [2048, 512], P('sp', 'tp'), may hold values from -0.125 to 0.125
- gate_weight: bfloat16 [2048, 512], P('sp', 'tp'), may hold values from -0.125 to 0.125
- key_gain: float32 [512], P('tp'), may hold values from 0.1 to 1.9
- removal_gain: float32 [512], P('tp'), may hold values from 0.1 to 1.9
- removal_bias: float32 [512], P('tp'), may hold values from -9 to 1
- decay_bias: float32 [512], P('tp'), may hold values from -12.7 to -1.8
- decay_extra: float32 [24576, 512], P('sp', 'tp'), may hold values from 0 to 0.7
- scan_norm_gain: float32 [512], P('tp'), may hold values from 0.1 to 1.9
- conv_value_weight: bfloat16 [2048, 512], P('sp', 'tp'), may hold values from -0.125 to 0.125
- conv_gate_weight: bfloat16 [2048, 512], P('sp', 'tp'), may hold values from -0.125 to 0.125
- conv_kernel: float32 [31, 512], P(None, 'tp'), may hold values from -2 to 2
- conv_bias: float32 [512], P('tp'), may hold values from -2 to 3
- conv_norm_gain: float32 [512], P('tp'), may hold values from 0.1 to 1.9
- out_scan_weight: bfloat16 [512, 2048], P('tp', 'sp'), may hold values from -0.1875 to 0.1875
- out_conv_weight: bfloat16 [512, 2048], P('tp', 'sp'), may hold values from -0.1875 to 0.1875
Outputs:
- mixed: bfloat16 [24576, 2048], P('sp', 'tp')
The draws below stay inside these ranges and needn't reach their ends.
All inputs are finite; a program needn't handle non-finite values.
Results may differ from the reference program's by a relative error of at most 0.0073.
Values may be sent and summed in bfloat16 or wider, within the bound.
No kernel may reach another device: no remote copies, remote signals or barrier semaphores. Data moves between devices by JAX's collectives and lax.ppermute only.
A program may use at most 64 MiB of HBM per device.

```python
import math
import jax
import jax.numpy as jnp
from jax import lax

MODEL = 2048
HEADS = 8
HEAD_SIZE = 64
CONV_K = 31
TOK_DEV = 192
WIDTH = 512
TOKENS = 24576


def head_ranks(key):
    return jax.random.permutation(jax.random.fold_in(key, 5), HEADS)


def slow_count():
    return HEADS // 2


def draw_decay_bias(key, part):
    ranks = head_ranks(key)
    jitter_key = jax.random.fold_in(key, 11)
    slow_heads = ranks < slow_count()
    jitter = jax.random.uniform(jitter_key, (WIDTH,), jnp.float32, -0.7, 0.7)
    centers = jnp.repeat(jnp.where(slow_heads, -12.0, -2.5), HEAD_SIZE)
    return (centers + jitter).astype(jnp.float32)


def draw_removal_bias(key, part):
    ranks = head_ranks(key)
    jitter_key = jax.random.fold_in(key, 13)
    lasting = max(1, HEADS // 4)
    keeping = ranks < lasting
    jitter = jax.random.uniform(jitter_key, (WIDTH,), jnp.float32, -1.0, 1.0)
    centers = jnp.repeat(jnp.where(keeping, -8.0, 0.0), HEAD_SIZE)
    return (centers + jitter).astype(jnp.float32)


def draw_decay_extra(key, part):
    keys = jax.random.split(jax.random.fold_in(key, 23), 3)
    spans = TOKENS // TOK_DEV
    levels = jnp.exp(jax.random.uniform(keys[0], (spans, HEADS), jnp.float32, math.log(3e-06), math.log(2.4e-05)))
    baseline = jnp.repeat(jnp.repeat(levels, TOK_DEV, axis=0), HEAD_SIZE, axis=1)
    places = jax.random.randint(keys[1], (3,), 0, TOKENS)
    hits = jnp.any(jnp.arange(TOKENS)[:, None] == places[None, :], axis=1)
    lowest = 0.22
    sizes = jnp.repeat(jax.random.uniform(keys[2], (TOKENS, HEADS), jnp.float32, lowest, 0.69), HEAD_SIZE, axis=1)
    return (baseline + jnp.where(hits[:, None], sizes, 0.0)).astype(jnp.float32)


def draw_conv_kernel(key, part):
    keys = jax.random.split(jax.random.fold_in(key, 37), 2)
    reach = 0.8
    rising = jnp.exp(jnp.linspace(-reach, reach, WIDTH))
    jitter = jnp.exp(jax.random.uniform(keys[0], (WIDTH,), jnp.float32, -0.3, 0.3))
    taps = jax.random.normal(keys[1], (CONV_K, WIDTH), jnp.float32) * CONV_K ** (-0.5)
    return jnp.clip(taps * rising * jitter, -2.0, 2.0).astype(jnp.float32)


def draw_conv_bias(key, part):
    jitter = jax.random.uniform(jax.random.fold_in(key, 41), (WIDTH,), jnp.float32, -0.4, 0.4)
    rising = jnp.linspace(-1.5, 1.5, WIDTH)
    return jnp.clip(rising + jitter, -2.0, 3.0).astype(jnp.float32)


def steps_of(rng, dims, cuts, low, high):
    loudness = 1.0
    for position, blocks in cuts:
        steps = jax.random.uniform(jax.random.fold_in(jax.random.fold_in(rng, 6), position), (blocks,), jnp.float32, low / len(cuts), high / len(cuts))
        loudness = loudness * jnp.repeat(jnp.exp(steps), dims[position] // blocks).reshape((-1,) + (1,) * (len(dims) - 1 - position))
    return loudness


def noise(key, shape, width, most, cuts=(), kind=jnp.bfloat16):
    result = jax.random.normal(key, shape, jnp.float32) * width
    if len(cuts) > 0:
        result = steps_of(key, shape, cuts, -0.22, 0.18) * result
    return jnp.clip(result, min=-most, max=most).astype(kind)


def setup_inputs(seed: int = 0) -> dict:
    key_of = jax.random.split(jax.random.key(seed), 22)
    return {
        "tokens": noise(key_of[0], (TOKENS, MODEL), 1.0, 6.0, ((0, 128), (1, 4))),
        "norm_gain": jnp.clip(1.0 + 0.18 * jax.random.normal(key_of[1], (MODEL,), jnp.float32), 0.1, 1.9),
        "query_weight": noise(key_of[2], (MODEL, WIDTH), MODEL ** -0.5, 0.125, ((0, 128), (1, 4))),
        "key_weight": noise(key_of[3], (MODEL, WIDTH), MODEL ** -0.5, 0.125, ((0, 128), (1, 4))),
        "value_weight": noise(key_of[4], (MODEL, WIDTH), MODEL ** -0.5, 0.125, ((0, 128), (1, 4))),
        "decay_weight": noise(key_of[5], (MODEL, WIDTH), (2 * MODEL) ** -0.5, 0.09375, ((0, 128), (1, 4))),
        "removal_weight": noise(key_of[6], (MODEL, WIDTH), MODEL ** -0.5, 0.125, ((0, 128), (1, 4))),
        "gate_weight": noise(key_of[7], (MODEL, WIDTH), MODEL ** -0.5, 0.125, ((0, 128), (1, 4))),
        "key_gain": jnp.clip(1.0 + 0.18 * jax.random.normal(key_of[8], (WIDTH,), jnp.float32), 0.1, 1.9),
        "removal_gain": jnp.clip(1.0 + 0.18 * jax.random.normal(key_of[9], (WIDTH,), jnp.float32), 0.1, 1.9),
        "removal_bias": draw_removal_bias(jax.random.fold_in(key_of[21], 71), 0),
        "decay_bias": draw_decay_bias(jax.random.fold_in(key_of[21], 71), 0),
        "decay_extra": draw_decay_extra(jax.random.fold_in(key_of[21], 71), 0),
        "scan_norm_gain": jnp.clip(1.0 + 0.18 * jax.random.normal(key_of[13], (WIDTH,), jnp.float32), 0.1, 1.9),
        "conv_value_weight": noise(key_of[14], (MODEL, WIDTH), MODEL ** -0.5, 0.125, ((0, 128), (1, 4))),
        "conv_gate_weight": noise(key_of[15], (MODEL, WIDTH), MODEL ** -0.5, 0.125, ((0, 128), (1, 4))),
        "conv_kernel": draw_conv_kernel(jax.random.fold_in(key_of[21], 71), 0),
        "conv_bias": draw_conv_bias(jax.random.fold_in(key_of[21], 71), 0),
        "conv_norm_gain": jnp.clip(1.0 + 0.18 * jax.random.normal(key_of[18], (WIDTH,), jnp.float32), 0.1, 1.9),
        "out_scan_weight": noise(key_of[19], (WIDTH, MODEL), (2 * WIDTH) ** -0.5, 0.1875, ((0, 4), (1, 128))),
        "out_conv_weight": noise(key_of[20], (WIDTH, MODEL), (2 * WIDTH) ** -0.5, 0.1875, ((0, 4), (1, 128))),
    }


def reference(tokens, norm_gain, query_weight, key_weight, value_weight, decay_weight, removal_weight, gate_weight, key_gain, removal_gain, removal_bias, decay_bias, decay_extra, scan_norm_gain, conv_value_weight, conv_gate_weight, conv_kernel, conv_bias, conv_norm_gain, out_scan_weight, out_conv_weight):
    exact_setting = lax.Precision.HIGHEST
    floats = tokens.astype(jnp.float32)
    normed = (floats * lax.rsqrt(lax.optimization_barrier(jnp.mean(floats * floats, axis=-1, keepdims=True)) + 1e-06) * norm_gain).astype(jnp.bfloat16)
    matrices = (query_weight, key_weight, value_weight, decay_weight, removal_weight, gate_weight, conv_value_weight, conv_gate_weight)
    stored = tuple((jnp.dot(normed, matrix, preferred_element_type=jnp.float32).astype(jnp.bfloat16) for matrix in matrices))
    stored = lax.optimization_barrier(stored)
    recept, key_rows, value_rows, decay_pre, removal_pre, gate_pre, conv_value, conv_gate = [item.astype(jnp.float32) for item in stored]
    decay_rate = jnp.exp(-jax.nn.softplus(-(decay_bias + decay_pre)) - 0.5) + decay_extra
    decay_factor = jnp.exp(-decay_rate)
    removal = jax.nn.sigmoid(removal_bias + removal_pre)

    def split_heads(table):
        return table.reshape(TOKENS, HEADS, HEAD_SIZE)
    scaled = split_heads(key_rows * key_gain)
    unit_keys = scaled * lax.rsqrt(lax.optimization_barrier(jnp.sum(scaled * scaled, axis=-1, keepdims=True)) + 1e-06)
    written = key_rows * (1.0 + (removal - 1.0) * removal_gain)

    def advance(memory, inputs):
        recept_t, decay_t, written_t, value_t, unit_t, removal_t = inputs
        removed_value = jnp.einsum('hvk,hk->hv', memory, -unit_t, precision=exact_setting)
        memory = memory * decay_t[:, None, :] + removed_value[:, :, None] * (unit_t * removal_t)[:, None, :] + value_t[:, :, None] * written_t[:, None, :]
        return (memory, jnp.einsum('hvk,hk->hv', memory, recept_t, precision=exact_setting))
    initial = jnp.zeros((HEADS, HEAD_SIZE, HEAD_SIZE), jnp.float32)
    _, reads = lax.scan(advance, initial, (split_heads(recept), split_heads(decay_factor), split_heads(written), split_heads(value_rows), unit_keys, split_heads(removal)))
    center = lax.optimization_barrier(jnp.mean(reads, axis=-1, keepdims=True))
    spread = lax.optimization_barrier(jnp.mean((reads - center) ** 2, axis=-1, keepdims=True))
    normalized = ((reads - center) * lax.rsqrt(spread + 0.00064)).reshape(TOKENS, WIDTH)
    scan_out = (normalized * scan_norm_gain * jax.nn.sigmoid(gate_pre)).astype(jnp.bfloat16)
    conv_input = (conv_value * jax.nn.sigmoid(conv_gate)).astype(jnp.bfloat16)
    padded = jnp.concatenate([jnp.zeros((CONV_K - 1, WIDTH), jnp.float32), conv_input.astype(jnp.float32)], axis=0)
    filtered = conv_bias + conv_kernel[0] * padded[0:TOKENS]
    for index in range(1, CONV_K):
        filtered = filtered + conv_kernel[index] * padded[index:index + TOKENS]
    channel_mean = lax.optimization_barrier(jnp.mean(filtered, axis=-1, keepdims=True))
    channel_var = lax.optimization_barrier(jnp.mean((filtered - channel_mean) ** 2, axis=-1, keepdims=True))
    conv_out = jax.nn.silu((filtered - channel_mean) * lax.rsqrt(channel_var + 1e-05) * conv_norm_gain).astype(jnp.bfloat16)
    total = jnp.dot(scan_out, out_scan_weight, preferred_element_type=jnp.float32) + jnp.dot(conv_out, out_conv_weight, preferred_element_type=jnp.float32)
    return total.astype(jnp.bfloat16)
```

```python
import functools

import jax
import jax.numpy as jnp
from jax import lax
from jax.experimental import pallas as pl
from jax.experimental.pallas import tpu as pltpu
from jax.sharding import PartitionSpec as P

HEAD = 64
TAPS = 31
BLOCK = 32
LENGTH = 192
BLOCKS = LENGTH // BLOCK
MATS = 8
F32 = jnp.float32
BF16 = jnp.bfloat16

NN = (((1,), (0,)), ((), ()))
NT = (((1,), (1,)), ((), ()))
TN = (((0,), (0,)), ((), ()))


def place(z, y, c):
    return z * 16 + y * 2 + c


ALONG_Y = [[[place(z, y, c) for y in range(8)] for z in range(8)] for c in range(2)]
ALONG_Z = [[[place(z, y, c) for z in range(8)] for y in range(8)] for c in range(2)]
FIRST_AXIS = ALONG_Y[0] + ALONG_Z[1]
SECOND_AXIS = ALONG_Z[0] + ALONG_Y[1]
Y_AXIS = ALONG_Y[0] + ALONG_Y[1]
Z_AXIS = ALONG_Z[0] + ALONG_Z[1]
SWAP = [(i, i ^ 1) for i in range(128)]
ONWARD = [(i, i + 1) for i in range(127)]


def split(x):
    high = x.astype(BF16)
    return high, (x - high.astype(F32)).astype(BF16)


def dot3(a, b, dims=NN):
    a_high, a_low = split(a)
    b_high, b_low = split(b)
    one = functools.partial(lax.dot_general, dimension_numbers=dims, preferred_element_type=F32)
    return one(a_high, b_high) + (one(a_high, b_low) + one(a_low, b_high))


def exact(a, b, dims=NN):
    return lax.dot_general(
        a, b, dims, precision=lax.Precision.HIGHEST, preferred_element_type=F32
    )


def iota(shape, dim):
    return lax.broadcasted_iota(jnp.int32, shape, dim)


def pack_kernel(*refs):
    out = refs[-1]
    blocks = [ref[...] for ref in refs[:MATS]]
    blocks += [ref[...].astype(F32).T.astype(BF16) for ref in refs[MATS:-1]]
    both = jnp.concatenate(blocks, axis=0)
    for k in range(8):
        out[k] = both


def pack(mats, outs):
    rows = 16 * (len(mats) + len(outs))
    return pl.pallas_call(
        pack_kernel, out_shape=jax.ShapeDtypeStruct((8, rows, 128), BF16), name="pack"
    )(*mats, *outs)


def fill_rows(core, own, other, store):
    for a in range(8):
        for b in range(8):
            straight = (a * 16 + b * 2) * 16
            turned = (b * 16 + a * 2) * 16 + 16
            mine = jnp.where(core == 0, straight, turned)
            theirs = jnp.where(core == 0, turned, straight)
            store(pl.multiple_of(mine, 16), own, a, b)
            store(pl.multiple_of(theirs, 16), other, a, b)


def local_kernel(
    core_ref,
    own_ref,
    other_ref,
    tokens_ref,
    norm_gain_ref,
    key_gain_ref,
    removal_gain_ref,
    removal_bias_ref,
    decay_bias_ref,
    extra_ref,
    norm_out_ref,
    state_ref,
    reads_ref,
    gate_ref,
    conv_ref,
    weights,
    normed,
):
    core = core_ref[0]

    def store(row, source, a, b):
        for m in range(MATS):
            lanes = slice((m % 2) * 128, (m % 2) * 128 + 128)
            weights[m // 2, pl.ds(row, 16), lanes] = source[a, b, m * 16 : m * 16 + 16, :]

    fill_rows(core, own_ref, other_ref, store)
    parts = [tokens_ref[j].astype(F32) for j in range(4)]
    total = sum(jnp.sum(part * part, axis=-1, keepdims=True) for part in parts)
    inverse_rms = lax.rsqrt(total * (1.0 / 2048.0) + 1e-06)
    for j in range(4):
        normed[:, j * 512 : j * 512 + 512] = (
            parts[j] * inverse_rms * norm_gain_ref[j : j + 1, :]
        ).astype(BF16)
    products = []
    for p in range(4):
        product = jnp.dot(normed[...], weights[p], preferred_element_type=F32)
        product = product.astype(BF16).astype(F32)
        products += [product[:, :128], product[:, 128:]]
    recept, keys, values, decay_pre, removal_pre, gate_pre, conv_value, conv_gate = products
    gate_ref[...] = norm_out_ref[...] * jax.nn.sigmoid(gate_pre)
    conv_ref[...] = (conv_value * jax.nn.sigmoid(conv_gate)).astype(BF16)

    rate = 0.6065306597126334 * jax.nn.sigmoid(decay_bias_ref[...] + decay_pre) + extra_ref[...]
    removal = jax.nn.sigmoid(removal_bias_ref[...] + removal_pre)
    lane = iota((LENGTH, 128), 1)
    first = lane < HEAD
    scaled = keys * key_gain_ref[...]
    square = scaled * scaled
    low = jnp.sum(jnp.where(first, square, 0.0), axis=-1, keepdims=True)
    high = jnp.sum(jnp.where(first, 0.0, square), axis=-1, keepdims=True)
    unit = scaled * lax.rsqrt(jnp.where(first, low, high) + 1e-06)
    written = keys * (1.0 + (removal - 1.0) * removal_gain_ref[...])

    row, column = iota((LENGTH, LENGTH), 0), iota((LENGTH, LENGTH), 1)
    same = (row // BLOCK) == (column // BLOCK)
    strict = same & (row > column)
    inclusive = same & (row >= column)
    falling = -exact(inclusive.astype(F32), rate)
    before = falling + rate
    by_block = falling.reshape(BLOCKS, BLOCK, 128)
    middle = jnp.broadcast_to(
        by_block[:, BLOCK // 2 : BLOCK // 2 + 1], (BLOCKS, BLOCK, 128)
    ).reshape(LENGTH, 128)
    ending = jnp.broadcast_to(by_block[:, BLOCK - 1 :], (BLOCKS, BLOCK, 128)).reshape(LENGTH, 128)
    beta = unit * removal
    rising = jnp.exp(middle - falling)
    alpha_mid = -unit * jnp.exp(before - middle)
    recept_mid = recept * jnp.exp(falling - middle)
    right = jnp.concatenate([beta * rising, written * rising], axis=0)
    start_alpha = -unit * jnp.exp(before)
    start_recept = recept * jnp.exp(falling)
    closing = jnp.exp(ending - falling)
    end_beta = beta * closing
    end_keys = written * closing
    kept = jnp.exp(by_block[:, BLOCK - 1, :])
    turned_values = pltpu.roll(values, HEAD, 1)

    square_row, square_lane = iota((128, 128), 0), iota((128, 128), 1)
    diagonal = square_row == square_lane
    for h in range(2):
        mine = first if h == 0 else jnp.logical_not(first)
        mine_row = (square_row < HEAD) if h == 0 else (square_row >= HEAD)
        left = jnp.concatenate(
            [jnp.where(mine, alpha_mid, 0.0), jnp.where(mine, recept_mid, 0.0)], axis=0
        )
        pairs = dot3(left, right, NT)
        power = jnp.where(strict, pairs[:LENGTH, :LENGTH], 0.0)
        alpha_keys = jnp.where(strict, pairs[:LENGTH, LENGTH:], 0.0)
        recept_beta = jnp.where(inclusive, pairs[LENGTH:, :LENGTH], 0.0)
        recept_keys = jnp.where(inclusive, pairs[LENGTH:, LENGTH:], 0.0)
        value_rows = jnp.where(mine, 0.0, turned_values)
        solved = jnp.where(mine, start_alpha, dot3(alpha_keys, value_rows))
        for step in range(5):
            solved = solved + dot3(power, solved)
            if step < 4:
                power = dot3(power, power)
        query = jnp.where(mine, start_recept, 0.0) + dot3(
            jnp.concatenate([recept_beta, recept_keys], axis=1),
            jnp.concatenate([solved, value_rows], axis=0),
        )
        steps = []
        for b in range(BLOCKS):
            rows = slice(b * BLOCK, b * BLOCK + BLOCK)
            moved = dot3(
                jnp.concatenate([end_beta[rows], end_keys[rows]], axis=0),
                jnp.concatenate([solved[rows], value_rows[rows]], axis=0),
                TN,
            )
            held = jnp.where(diagonal, jnp.broadcast_to(kept[b : b + 1], (128, 128)), 0.0)
            whole = jnp.where(diagonal, 1.0, 0.0)
            steps.append(jnp.where(mine_row, moved + held, whole))
        one = dot3(steps[1], steps[0])
        two = dot3(steps[3], steps[2])
        three = dot3(steps[5], steps[4])
        four = dot3(two, one)
        prefixes = [None, steps[0], one, dot3(steps[2], one), four, dot3(steps[4], four)]
        final = dot3(three, four)[h * HEAD : h * HEAD + HEAD]
        if h == 1:
            final = pltpu.roll(final, HEAD, 1)
        state_ref[h] = final
        reads_ref[h, 0:BLOCK, :] = query[0:BLOCK]
        for b in range(1, BLOCKS):
            rows = slice(b * BLOCK, b * BLOCK + BLOCK)
            reads_ref[h, rows, :] = dot3(query[rows], prefixes[b])


def local_part(core, own, other, tokens, norm_gain, vectors, extra, norm_out):
    block = pl.BlockSpec((8, 8, MATS * 16, 128), lambda i: (0, 0, 0, 0))
    whole = lambda shape: pl.BlockSpec(shape, lambda i: (0,) * len(shape))
    operands = (tokens, norm_gain, *vectors, extra, norm_out)
    shapes = (
        jax.ShapeDtypeStruct((2, HEAD, 128), F32),
        jax.ShapeDtypeStruct((2, LENGTH, 128), F32),
        jax.ShapeDtypeStruct((LENGTH, 128), F32),
        jax.ShapeDtypeStruct((LENGTH, 128), BF16),
    )
    return pl.pallas_call(
        local_kernel,
        grid=(1,),
        in_specs=[pl.BlockSpec(memory_space=pltpu.SMEM), block, block]
        + [whole(x.shape) for x in operands],
        out_specs=tuple(whole(x.shape) for x in shapes),
        out_shape=shapes,
        scratch_shapes=[pltpu.VMEM((4, 2048, 256), BF16), pltpu.VMEM((LENGTH, 2048), BF16)],
        name="local",
    )(core, own, other, *operands)


def after(later, earlier):
    product = exact(later[:, :HEAD], earlier)
    return product + jnp.where(iota((HEAD, 128), 1) < HEAD, 0.0, later)


def chained(steps):
    while len(steps) > 1:
        steps = [after(steps[k + 1], steps[k]) for k in range(0, len(steps), 2)]
    return steps[0]


def nothing():
    return jnp.where(iota((HEAD, 128), 0) == iota((HEAD, 128), 1), 1.0, 0.0)


def chip_kernel(core_ref, mine_ref, theirs_ref, out_ref):
    core = core_ref[0]
    mine, theirs = mine_ref[...], theirs_ref[...]
    earlier = jnp.where(core == 0, mine, theirs)
    later = jnp.where(core == 0, theirs, mine)
    out_ref[...] = jnp.broadcast_to(after(later, earlier)[None], (8, HEAD, 128))


def row_kernel(place_ref, steps_ref, before_ref, total_ref):
    here = place_ref[0]
    steps = [steps_ref[k] for k in range(8)]
    total_ref[...] = jnp.broadcast_to(chained(steps)[None], (8, HEAD, 128))
    before_ref[...] = chained([jnp.where(k < here, steps[k], nothing()) for k in range(8)])


def incoming_kernel(place_ref, steps_ref, before_ref, mine_ref, theirs_ref, own_ref, sent_ref):
    here, core = place_ref[0], place_ref[1]
    steps = [steps_ref[k] for k in range(8)]
    start = chained([jnp.where(k < here, steps[k], nothing()) for k in range(8)])
    at_chip = after(before_ref[...], start)
    earlier = jnp.where(core == 0, mine_ref[...], theirs_ref[...])
    at_second = after(earlier, at_chip)
    own_ref[...] = jnp.where(core == 0, at_chip, at_second)
    sent_ref[...] = jnp.where(core == 0, at_second, at_chip)


def on_core(kernel, shapes, scalars, *operands, name):
    return pl.pallas_call(
        kernel,
        in_specs=[pl.BlockSpec(memory_space=pltpu.SMEM)]
        + [pl.BlockSpec(x.shape, lambda n=x.ndim: (0,) * n) for x in operands],
        out_shape=shapes,
        name=name,
    )(scalars, *operands)


def conv_kernel(input_ref, rim_ref, taps_ref, bias_ref, filtered_ref, sums_ref):
    padded = jnp.concatenate([rim_ref[...], input_ref[...]], axis=0).astype(F32)
    filtered = jnp.broadcast_to(bias_ref[...], (LENGTH, 128))
    for k in range(TAPS):
        filtered = filtered + taps_ref[k : k + 1, :] * padded[k + 2 : k + 2 + LENGTH]
    filtered_ref[...] = filtered
    ones = jnp.ones((8, 128), F32)
    sums_ref[0:8, :] = exact(ones, filtered, NT)
    sums_ref[8:16, :] = exact(ones, filtered * filtered, NT)


def columns_kernel(core_ref, own_ref, other_ref, out_ref):
    def store(row, source, a, b):
        for m in range(2):
            out_ref[pl.ds(row, 16), m * 128 : m * 128 + 128] = source[a, b, m * 16 : m * 16 + 16, :]

    fill_rows(core_ref[0], own_ref, other_ref, store)


def output_columns(core, own, other):
    block = pl.BlockSpec((8, 8, 32, 128), lambda i: (0, 0, MATS // 2, 0))
    return pl.pallas_call(
        columns_kernel,
        grid=(1,),
        in_specs=[pl.BlockSpec(memory_space=pltpu.SMEM), block, block],
        out_specs=pl.BlockSpec((2048, 256), lambda i: (0, 0)),
        out_shape=jax.ShapeDtypeStruct((2048, 256), BF16),
        name="columns",
    )(core, own, other)


def final_kernel(
    core_ref,
    reads_ref,
    mine_ref,
    theirs_ref,
    gate_ref,
    filtered_ref,
    sums_ref,
    conv_gain_ref,
    columns_ref,
    out_ref,
):
    core = core_ref[0]
    mine, theirs = mine_ref[...], theirs_ref[...]
    head0 = jnp.where(core == 0, mine, theirs)
    head1 = jnp.where(core == 0, theirs, mine)
    lane = iota((HEAD, 128), 1)
    equal = iota((HEAD, 128), 0)
    zero = jnp.zeros((HEAD, 128), F32)
    right0 = jnp.concatenate(
        [
            jnp.where(lane < HEAD, pltpu.roll(head0, HEAD, 1), zero),
            jnp.where(lane == equal, 1.0, 0.0),
        ],
        axis=0,
    )
    right1 = jnp.concatenate(
        [jnp.where(lane == equal + HEAD, 1.0, 0.0), jnp.where(lane < HEAD, zero, head1)], axis=0
    )
    reads = exact(reads_ref[0], right0) + exact(reads_ref[1], right1)
    first = iota((LENGTH, 128), 1) < HEAD

    def head_mean(x):
        low = jnp.sum(jnp.where(first, x, 0.0), axis=-1, keepdims=True)
        high = jnp.sum(jnp.where(first, 0.0, x), axis=-1, keepdims=True)
        return jnp.where(first, low, high) * (1.0 / HEAD)

    centered = reads - head_mean(reads)
    spread = head_mean(centered * centered)
    scan_out = (centered * lax.rsqrt(spread + 0.00064) * gate_ref[...]).astype(BF16)

    eighth = jnp.full((8, 128), 0.125 / 512.0, F32)
    center = exact(sums_ref[0:8, :], eighth, TN)
    second = exact(sums_ref[8:16, :], eighth, TN)
    scaled = (
        (filtered_ref[...] - center)
        * lax.rsqrt(second - center * center + 1e-05)
        * conv_gain_ref[...]
    )
    conv_out = (scaled * jax.nn.sigmoid(scaled)).astype(BF16)
    features = jnp.concatenate([scan_out, conv_out], axis=1)
    for j in range(4):
        out_ref[j] = lax.dot_general(
            features, columns_ref[j * 512 : j * 512 + 512, :], NT, preferred_element_type=F32
        ).astype(BF16)


def to_each(x, groups):
    return lax.all_to_all(x, "sp", 0, 0, tiled=True, axis_index_groups=groups)


def shards(
    tokens,
    norm_gain,
    query_weight,
    key_weight,
    value_weight,
    decay_weight,
    removal_weight,
    gate_weight,
    key_gain,
    removal_gain,
    removal_bias,
    decay_bias,
    decay_extra,
    scan_norm_gain,
    conv_value_weight,
    conv_gate_weight,
    conv_taps,
    conv_bias,
    conv_norm_gain,
    out_scan_weight,
    out_conv_weight,
):
    index = lax.axis_index("sp")
    core = (index % 2).astype(jnp.int32)
    core1 = core[None]
    z, y = index // 16, (index // 2) % 8
    row = lambda v: v.reshape(1, -1)

    packed = pack(
        (
            query_weight,
            key_weight,
            value_weight,
            decay_weight,
            removal_weight,
            gate_weight,
            conv_value_weight,
            conv_gate_weight,
        ),
        (out_scan_weight, out_conv_weight),
    )
    stage1 = to_each(packed, FIRST_AXIS)
    stage2 = to_each(jnp.broadcast_to(stage1[None], (8, *stage1.shape)), SECOND_AXIS)
    whole = lax.all_gather(tokens, "tp")
    swapped = lax.ppermute(stage2, "sp", SWAP)

    state, reads, gate, conv_input = local_part(
        core1,
        stage2,
        swapped,
        whole,
        norm_gain.reshape(4, 512),
        (row(key_gain), row(removal_gain), row(removal_bias), row(decay_bias)),
        decay_extra,
        row(scan_norm_gain),
    )

    mine = jnp.where(core == 0, state[0], state[1])
    theirs = lax.ppermute(jnp.where(core == 0, state[1], state[0]), "sp", SWAP)
    rim = lax.ppermute(conv_input[LENGTH - 32 :], "sp", ONWARD)
    table = jax.ShapeDtypeStruct((8, HEAD, 128), F32)
    step = jax.ShapeDtypeStruct((HEAD, 128), F32)
    chip = on_core(chip_kernel, table, core1, mine, theirs, name="chip")
    before, total = on_core(
        row_kernel, (step, table), y.astype(jnp.int32)[None], to_each(chip, Y_AXIS), name="row"
    )
    own_state, sent_state = on_core(
        incoming_kernel,
        (step, step),
        jnp.stack([z, core]).astype(jnp.int32),
        to_each(total, Z_AXIS),
        before,
        mine,
        theirs,
        name="incoming",
    )
    other_state = lax.ppermute(sent_state, "sp", SWAP)

    filtered, sums = pl.pallas_call(
        conv_kernel,
        out_shape=(
            jax.ShapeDtypeStruct((LENGTH, 128), F32),
            jax.ShapeDtypeStruct((16, LENGTH), F32),
        ),
        name="conv",
    )(conv_input, rim, conv_taps, row(conv_bias))
    sums = lax.psum(sums, "tp")
    columns = output_columns(core1, stage2, swapped)

    terms = on_core(
        final_kernel,
        jax.ShapeDtypeStruct((4, LENGTH, 512), BF16),
        core1,
        reads,
        own_state,
        other_state,
        gate,
        filtered,
        sums,
        row(conv_norm_gain),
        columns,
        name="final",
    )
    parts = lax.all_to_all(terms, "tp", 0, 0, tiled=True)
    return jnp.sum(parts.astype(F32), axis=0).astype(BF16)


def solution(mesh):
    weights = P("sp", "tp")
    in_specs = (
        (P("sp", "tp"), P())
        + (weights,) * 6
        + (P("tp"),) * 4
        + (P("sp", "tp"), P("tp"), weights, weights, P(None, "tp"), P("tp"), P("tp"))
        + (P("tp", "sp"), P("tp", "sp"))
    )
    return jax.shard_map(
        shards, mesh=mesh, in_specs=in_specs, out_specs=P("sp", "tp"), check_vma=False
    )
```

```python
import functools

import jax
import jax.numpy as jnp
from jax import lax
from jax.experimental import pallas as pl
from jax.experimental.pallas import tpu as pltpu
from jax.sharding import PartitionSpec as P

HEAD = 64
TAPS = 31
BLOCK = 32
LENGTH = 192
BLOCKS = LENGTH // BLOCK
MATS = 8
F32 = jnp.float32
BF16 = jnp.bfloat16

NN = (((1,), (0,)), ((), ()))
NT = (((1,), (1,)), ((), ()))
TN = (((0,), (0,)), ((), ()))


def place(z, y, c):
    return z * 16 + y * 2 + c


def near(k, parity, c):
    return (2 * k + parity + (2 if c == 1 and parity == 0 else 0)) % 8


FAR = [
    [place(z + 2 * i, y + 2 * j, c) for i in range(4) for j in range(4)]
    for c in range(2)
    for z in range(2)
    for y in range(2)
]
NEAR = [
    [
        place(near(k, p, c), near(l, q, c), c)
        for p in range(2)
        for q in range(2)
    ]
    for c in range(2)
    for k in range(4)
    for l in range(4)
]
Y_AXIS = [[place(z, y, c) for y in range(8)] for z in range(8) for c in range(2)]
Z_AXIS = [[place(z, y, c) for z in range(8)] for y in range(8) for c in range(2)]
SWAP = [(i, i ^ 1) for i in range(128)]
ONWARD = [(i, i + 1) for i in range(127)]


def split(x):
    high = x.astype(BF16)
    return high, (x - high.astype(F32)).astype(BF16)


def dot3(a, b, dims=NN):
    a_high, a_low = split(a)
    b_high, b_low = split(b)
    one = functools.partial(lax.dot_general, dimension_numbers=dims, preferred_element_type=F32)
    return one(a_high, b_high) + (one(a_high, b_low) + one(a_low, b_high))


def exact(a, b, dims=NN):
    return lax.dot_general(
        a, b, dims, precision=lax.Precision.HIGHEST, preferred_element_type=F32
    )


def iota(shape, dim):
    return lax.broadcasted_iota(jnp.int32, shape, dim)


def pack_kernel(*refs):
    out = refs[-1]
    blocks = [ref[...] for ref in refs[:-1]]
    both = jnp.concatenate(blocks, axis=0)
    for k in range(16):
        out[k] = both


def pack(*mats):
    return pl.pallas_call(
        pack_kernel,
        out_shape=jax.ShapeDtypeStruct((16, 16 * len(mats), 128), BF16),
        name="pack",
    )(*mats)


def fill_rows(core, own, other, store):
    for a in range(4):
        for b in range(16):
            z, y = a // 2 + 2 * (b // 4), a % 2 + 2 * (b % 4)
            row = (z * 16 + y * 2) * 16
            store(pl.multiple_of(row + core * 16, 16), own, a, b)
            store(pl.multiple_of(row + 16 - core * 16, 16), other, a, b)


def local_kernel(
    core_ref,
    own_ref,
    other_ref,
    tokens_ref,
    norm_gain_ref,
    key_gain_ref,
    removal_gain_ref,
    removal_bias_ref,
    decay_bias_ref,
    extra_ref,
    norm_out_ref,
    mine_ref,
    theirs_ref,
    reads_ref,
    gate_ref,
    conv_ref,
    weights,
    normed,
):
    core = core_ref[0]

    def store(row, source, a, b):
        for m in range(MATS):
            lanes = slice((m % 2) * 128, (m % 2) * 128 + 128)
            weights[m // 2, pl.ds(row, 16), lanes] = source[a, b, m * 16 : m * 16 + 16, :]

    fill_rows(core, own_ref, other_ref, store)
    parts = [tokens_ref[j].astype(F32) for j in range(4)]
    total = sum(jnp.sum(part * part, axis=-1, keepdims=True) for part in parts)
    inverse_rms = lax.rsqrt(total * (1.0 / 2048.0) + 1e-06)
    for j in range(4):
        normed[:, j * 512 : j * 512 + 512] = (
            parts[j] * inverse_rms * norm_gain_ref[j : j + 1, :]
        ).astype(BF16)
    products = []
    for p in range(4):
        product = jnp.dot(normed[...], weights[p], preferred_element_type=F32)
        product = product.astype(BF16).astype(F32)
        products += [product[:, :128], product[:, 128:]]
    recept, keys, values, decay_pre, removal_pre, gate_pre, conv_value, conv_gate = products
    gate_ref[...] = norm_out_ref[...] * jax.nn.sigmoid(gate_pre)
    conv_ref[...] = (conv_value * jax.nn.sigmoid(conv_gate)).astype(BF16)

    rate = 0.6065306597126334 * jax.nn.sigmoid(decay_bias_ref[...] + decay_pre) + extra_ref[...]
    removal = jax.nn.sigmoid(removal_bias_ref[...] + removal_pre)
    lane = iota((LENGTH, 128), 1)
    first = lane < HEAD
    scaled = keys * key_gain_ref[...]
    square = scaled * scaled
    low = jnp.sum(jnp.where(first, square, 0.0), axis=-1, keepdims=True)
    high = jnp.sum(jnp.where(first, 0.0, square), axis=-1, keepdims=True)
    unit = scaled * lax.rsqrt(jnp.where(first, low, high) + 1e-06)
    written = keys * (1.0 + (removal - 1.0) * removal_gain_ref[...])

    row, column = iota((LENGTH, LENGTH), 0), iota((LENGTH, LENGTH), 1)
    same = (row // BLOCK) == (column // BLOCK)
    strict = same & (row > column)
    inclusive = same & (row >= column)
    falling = -exact(inclusive.astype(F32), rate)
    before = falling + rate
    by_block = falling.reshape(BLOCKS, BLOCK, 128)
    middle = jnp.broadcast_to(
        by_block[:, BLOCK // 2 : BLOCK // 2 + 1], (BLOCKS, BLOCK, 128)
    ).reshape(LENGTH, 128)
    ending = jnp.broadcast_to(by_block[:, BLOCK - 1 :], (BLOCKS, BLOCK, 128)).reshape(LENGTH, 128)
    beta = unit * removal
    rising = jnp.exp(middle - falling)
    alpha_mid = -unit * jnp.exp(before - middle)
    recept_mid = recept * jnp.exp(falling - middle)
    right = jnp.concatenate([beta * rising, written * rising], axis=0)
    start_alpha = -unit * jnp.exp(before)
    start_recept = recept * jnp.exp(falling)
    closing = jnp.exp(ending - falling)
    end_beta = beta * closing
    end_keys = written * closing
    kept = jnp.exp(by_block[:, BLOCK - 1, :])
    turned_values = pltpu.roll(values, HEAD, 1)

    square_row, square_lane = iota((128, 128), 0), iota((128, 128), 1)
    diagonal = square_row == square_lane
    finals = []
    for h in range(2):
        mine = first if h == 0 else jnp.logical_not(first)
        mine_row = (square_row < HEAD) if h == 0 else (square_row >= HEAD)
        left = jnp.concatenate(
            [jnp.where(mine, alpha_mid, 0.0), jnp.where(mine, recept_mid, 0.0)], axis=0
        )
        pairs = dot3(left, right, NT)
        power = jnp.where(strict, pairs[:LENGTH, :LENGTH], 0.0)
        alpha_keys = jnp.where(strict, pairs[:LENGTH, LENGTH:], 0.0)
        recept_beta = jnp.where(inclusive, pairs[LENGTH:, :LENGTH], 0.0)
        recept_keys = jnp.where(inclusive, pairs[LENGTH:, LENGTH:], 0.0)
        value_rows = jnp.where(mine, 0.0, turned_values)
        solved = jnp.where(mine, start_alpha, dot3(alpha_keys, value_rows))
        for step in range(5):
            solved = solved + dot3(power, solved)
            if step < 4:
                power = dot3(power, power)
        query = jnp.where(mine, start_recept, 0.0) + dot3(
            jnp.concatenate([recept_beta, recept_keys], axis=1),
            jnp.concatenate([solved, value_rows], axis=0),
        )
        steps = []
        for b in range(BLOCKS):
            rows = slice(b * BLOCK, b * BLOCK + BLOCK)
            moved = dot3(
                jnp.concatenate([end_beta[rows], end_keys[rows]], axis=0),
                jnp.concatenate([solved[rows], value_rows[rows]], axis=0),
                TN,
            )
            held = jnp.where(diagonal, jnp.broadcast_to(kept[b : b + 1], (128, 128)), 0.0)
            whole = jnp.where(diagonal, 1.0, 0.0)
            steps.append(jnp.where(mine_row, moved + held, whole))
        one = dot3(steps[1], steps[0])
        two = dot3(steps[3], steps[2])
        three = dot3(steps[5], steps[4])
        four = dot3(two, one)
        prefixes = [None, steps[0], one, dot3(steps[2], one), four, dot3(steps[4], four)]
        final = dot3(three, four)[h * HEAD : h * HEAD + HEAD]
        if h == 1:
            final = pltpu.roll(final, HEAD, 1)
        finals.append(final)
        reads_ref[h, 0:BLOCK, :] = query[0:BLOCK]
        for b in range(1, BLOCKS):
            rows = slice(b * BLOCK, b * BLOCK + BLOCK)
            reads_ref[h, rows, :] = dot3(query[rows], prefixes[b])
    mine_ref[...] = jnp.where(core == 0, finals[0], finals[1])
    theirs_ref[...] = jnp.where(core == 0, finals[1], finals[0])


def local_part(core, own, other, tokens, norm_gain, vectors, extra, norm_out):
    block = pl.BlockSpec((4, 16, MATS * 16, 128), lambda i: (0, 0, 0, 0))
    whole = lambda shape: pl.BlockSpec(shape, lambda i: (0,) * len(shape))
    operands = (tokens, norm_gain, *vectors, extra, norm_out)
    shapes = (
        jax.ShapeDtypeStruct((HEAD, 128), F32),
        jax.ShapeDtypeStruct((HEAD, 128), F32),
        jax.ShapeDtypeStruct((2, LENGTH, 128), F32),
        jax.ShapeDtypeStruct((LENGTH, 128), F32),
        jax.ShapeDtypeStruct((LENGTH, 128), BF16),
    )
    return pl.pallas_call(
        local_kernel,
        grid=(1,),
        in_specs=[pl.BlockSpec(memory_space=pltpu.SMEM), block, block]
        + [whole(x.shape) for x in operands],
        out_specs=tuple(whole(x.shape) for x in shapes),
        out_shape=shapes,
        scratch_shapes=[pltpu.VMEM((4, 2048, 256), BF16), pltpu.VMEM((LENGTH, 2048), BF16)],
        name="local",
    )(core, own, other, *operands)


def after(later, earlier):
    product = dot3(later[:, :HEAD], earlier)
    return product + jnp.where(iota((HEAD, 128), 1) < HEAD, 0.0, later)


def chained(steps):
    while len(steps) > 1:
        steps = [after(steps[k + 1], steps[k]) for k in range(0, len(steps), 2)]
    return steps[0]


def nothing():
    return jnp.where(iota((HEAD, 128), 0) == iota((HEAD, 128), 1), 1.0, 0.0)


def sent(step):
    return jnp.broadcast_to((step - nothing()).astype(BF16)[None], (8, HEAD, 128))


def received(steps_ref):
    return [steps_ref[k].astype(F32) + nothing() for k in range(8)]


def chip_kernel(core_ref, mine_ref, theirs_ref, out_ref):
    core = core_ref[0]
    mine, theirs = mine_ref[...], theirs_ref[...]
    earlier = jnp.where(core == 0, mine, theirs)
    later = jnp.where(core == 0, theirs, mine)
    out_ref[...] = sent(after(later, earlier))


def row_kernel(place_ref, steps_ref, before_ref, total_ref):
    here = place_ref[0]
    steps = received(steps_ref)
    total_ref[...] = sent(chained(steps))
    before_ref[...] = chained([jnp.where(k < here, steps[k], nothing()) for k in range(8)])


def incoming_kernel(place_ref, steps_ref, before_ref, mine_ref, theirs_ref, own_ref, sent_ref):
    here, core = place_ref[0], place_ref[1]
    steps = received(steps_ref)
    start = chained([jnp.where(k < here, steps[k], nothing()) for k in range(8)])
    at_chip = after(before_ref[...], start)
    earlier = jnp.where(core == 0, mine_ref[...], theirs_ref[...])
    at_second = after(earlier, at_chip)
    own_ref[...] = jnp.where(core == 0, at_chip, at_second)
    sent_ref[...] = jnp.where(core == 0, at_second, at_chip)


def on_core(kernel, shapes, scalars, *operands):
    return pl.pallas_call(
        kernel,
        in_specs=[pl.BlockSpec(memory_space=pltpu.SMEM)]
        + [pl.BlockSpec(x.shape, lambda n=x.ndim: (0,) * n) for x in operands],
        out_shape=shapes,
    )(scalars, *operands)


def conv_kernel(input_ref, rim_ref, taps_ref, bias_ref, filtered_ref, sums_ref):
    padded = jnp.concatenate([rim_ref[...], input_ref[...]], axis=0).astype(F32)
    filtered = jnp.broadcast_to(bias_ref[...], (LENGTH, 128))
    for k in range(TAPS):
        filtered = filtered + taps_ref[k : k + 1, :] * padded[k + 2 : k + 2 + LENGTH]
    filtered_ref[...] = filtered
    ones = jnp.ones((8, 128), F32)
    sums_ref[0:8, :] = exact(ones, filtered, NT)
    sums_ref[8:16, :] = exact(ones, filtered * filtered, NT)


def columns_kernel(core_ref, own_ref, other_ref, out_ref):
    def store(row, source, a, b):
        for m in range(2):
            out_ref[pl.ds(row, 16), m * 128 : m * 128 + 128] = source[a, b, m * 16 : m * 16 + 16, :]

    fill_rows(core_ref[0], own_ref, other_ref, store)


def output_columns(core, own, other):
    block = pl.BlockSpec((4, 16, 32, 128), lambda i: (0, 0, MATS // 2, 0))
    return pl.pallas_call(
        columns_kernel,
        grid=(1,),
        in_specs=[pl.BlockSpec(memory_space=pltpu.SMEM), block, block],
        out_specs=pl.BlockSpec((2048, 256), lambda i: (0, 0)),
        out_shape=jax.ShapeDtypeStruct((2048, 256), BF16),
        name="columns",
    )(core, own, other)


def final_kernel(
    core_ref,
    reads_ref,
    mine_ref,
    theirs_ref,
    gate_ref,
    filtered_ref,
    sums_ref,
    conv_gain_ref,
    columns_ref,
    out_ref,
):
    core = core_ref[0]
    mine, theirs = mine_ref[...], theirs_ref[...]
    head0 = jnp.where(core == 0, mine, theirs)
    head1 = jnp.where(core == 0, theirs, mine)
    lane = iota((HEAD, 128), 1)
    equal = iota((HEAD, 128), 0)
    zero = jnp.zeros((HEAD, 128), F32)
    right0 = jnp.concatenate(
        [
            jnp.where(lane < HEAD, pltpu.roll(head0, HEAD, 1), zero),
            jnp.where(lane == equal, 1.0, 0.0),
        ],
        axis=0,
    )
    right1 = jnp.concatenate(
        [jnp.where(lane == equal + HEAD, 1.0, 0.0), jnp.where(lane < HEAD, zero, head1)], axis=0
    )
    reads = exact(reads_ref[0], right0) + exact(reads_ref[1], right1)
    first = iota((LENGTH, 128), 1) < HEAD

    def head_mean(x):
        low = jnp.sum(jnp.where(first, x, 0.0), axis=-1, keepdims=True)
        high = jnp.sum(jnp.where(first, 0.0, x), axis=-1, keepdims=True)
        return jnp.where(first, low, high) * (1.0 / HEAD)

    centered = reads - head_mean(reads)
    spread = head_mean(centered * centered)
    scan_out = (centered * lax.rsqrt(spread + 0.00064) * gate_ref[...]).astype(BF16)

    eighth = jnp.full((8, 128), 0.125 / 512.0, F32)
    center = exact(sums_ref[0:8, :], eighth, TN)
    second = exact(sums_ref[8:16, :], eighth, TN)
    scaled = (
        (filtered_ref[...] - center)
        * lax.rsqrt(second - center * center + 1e-05)
        * conv_gain_ref[...]
    )
    conv_out = (scaled * jax.nn.sigmoid(scaled)).astype(BF16)
    features = jnp.concatenate([scan_out, conv_out], axis=1)
    for j in range(4):
        out_ref[j] = lax.dot_general(
            features, columns_ref[j * 512 : j * 512 + 512, :], NT, preferred_element_type=F32
        ).astype(BF16)


def to_each(x, groups):
    return lax.all_to_all(x, "sp", 0, 0, tiled=True, axis_index_groups=groups)


def layer(
    tokens,
    norm_gain,
    query_weight,
    key_weight,
    value_weight,
    decay_weight,
    removal_weight,
    gate_weight,
    key_gain,
    removal_gain,
    removal_bias,
    decay_bias,
    decay_extra,
    scan_norm_gain,
    conv_value_weight,
    conv_gate_weight,
    conv_taps,
    conv_bias,
    conv_norm_gain,
    out_scan_weight,
    out_conv_weight,
):
    index = lax.axis_index("sp")
    core = (index % 2).astype(jnp.int32)
    core1 = core[None]
    z, y = index // 16, (index // 2) % 8
    row = lambda v: v.reshape(1, -1)

    packed = pack(
        query_weight,
        key_weight,
        value_weight,
        decay_weight,
        removal_weight,
        gate_weight,
        conv_value_weight,
        conv_gate_weight,
        out_scan_weight.T,
        out_conv_weight.T,
    )
    stage1 = to_each(packed, FAR)
    wide = jnp.broadcast_to(stage1[None], (4, *stage1.shape))
    stage2 = to_each(wide, NEAR)
    whole = lax.all_gather(tokens, "tp")
    swapped = lax.ppermute(stage2, "sp", SWAP)

    mine, theirs, reads, gate, conv_input = local_part(
        core1,
        stage2,
        swapped,
        whole,
        norm_gain.reshape(4, 512),
        (row(key_gain), row(removal_gain), row(removal_bias), row(decay_bias)),
        decay_extra,
        row(scan_norm_gain),
    )

    theirs = lax.ppermute(theirs, "sp", SWAP)
    rim = lax.ppermute(conv_input[LENGTH - 32 :], "sp", ONWARD)
    table = jax.ShapeDtypeStruct((8, HEAD, 128), BF16)
    step = jax.ShapeDtypeStruct((HEAD, 128), F32)
    chip = on_core(chip_kernel, table, core1, mine, theirs)
    chips = to_each(chip, Y_AXIS)
    before, total = on_core(row_kernel, (step, table), y.astype(jnp.int32)[None], chips)
    totals = to_each(total, Z_AXIS)
    own_state, sent_state = on_core(
        incoming_kernel,
        (step, step),
        jnp.stack([z, core]).astype(jnp.int32),
        totals,
        before,
        mine,
        theirs,
    )
    other_state = lax.ppermute(sent_state, "sp", SWAP)

    filtered, sums = pl.pallas_call(
        conv_kernel,
        out_shape=(
            jax.ShapeDtypeStruct((LENGTH, 128), F32),
            jax.ShapeDtypeStruct((16, LENGTH), F32),
        ),
        name="conv",
    )(conv_input, rim, conv_taps, row(conv_bias))
    sums = lax.psum(sums, "tp")
    columns = output_columns(core1, stage2, swapped)

    terms = on_core(
        final_kernel,
        jax.ShapeDtypeStruct((4, LENGTH, 512), BF16),
        core1,
        reads,
        own_state,
        other_state,
        gate,
        filtered,
        sums,
        row(conv_norm_gain),
        columns,
    )
    parts = lax.all_to_all(terms, "tp", 0, 0, tiled=True)
    return jnp.sum(parts.astype(F32), axis=0).astype(BF16)


def solution(mesh):
    weights = P("sp", "tp")
    in_specs = (
        (P("sp", "tp"), P())
        + (weights,) * 6
        + (P("tp"),) * 4
        + (P("sp", "tp"), P("tp"), weights, weights, P(None, "tp"), P("tp"), P("tp"))
        + (P("tp", "sp"), P("tp", "sp"))
    )
    return jax.shard_map(
        layer, mesh=mesh, in_specs=in_specs, out_specs=P("sp", "tp"), check_vma=False
    )
```

```python
import functools

import jax
import jax.numpy as jnp
from jax import lax
from jax.experimental import pallas as pl
from jax.experimental.pallas import tpu as pltpu
from jax.sharding import PartitionSpec as P

HEAD = 64
TAPS = 31
BLOCK = 32
LENGTH = 192
BLOCKS = LENGTH // BLOCK
MATS = 8
F32 = jnp.float32
BF16 = jnp.bfloat16

NN = (((1,), (0,)), ((), ()))
NT = (((1,), (1,)), ((), ()))
TN = (((0,), (0,)), ((), ()))


def place(z, y, c):
    return z * 16 + y * 2 + c


SETS = (((0, 2, 5, 7), (1, 3, 4, 6)), ((1, 3, 6, 0), (2, 4, 5, 7)))
FAR = [
    [place(z, y, c) for z in SETS[c][p] for y in SETS[c][q]]
    for c in range(2)
    for p in range(2)
    for q in range(2)
]


def near(k, p, c):
    pair = ((2 * k + c) % 8, (2 * k + c + 1) % 8)
    return [chip for chip in pair if chip in SETS[c][p]][0]


NEAR = [
    [place(near(k, p, c), near(l, q, c), c) for p in range(2) for q in range(2)]
    for c in range(2)
    for k in range(4)
    for l in range(4)
]
Y_AXIS = [[place(z, y, c) for y in range(8)] for z in range(8) for c in range(2)]
Z_AXIS = [[place(z, y, c) for z in range(8)] for y in range(8) for c in range(2)]
SWAP = [(i, i ^ 1) for i in range(128)]
ONWARD = [(i, i + 1) for i in range(127)]


def split(x):
    high = x.astype(BF16)
    return high, (x - high.astype(F32)).astype(BF16)


def dot3(a, b, dims=NN):
    a_high, a_low = split(a)
    b_high, b_low = split(b)
    one = functools.partial(lax.dot_general, dimension_numbers=dims, preferred_element_type=F32)
    return one(a_high, b_high) + (one(a_high, b_low) + one(a_low, b_high))


def exact(a, b, dims=NN):
    return lax.dot_general(
        a, b, dims, precision=lax.Precision.HIGHEST, preferred_element_type=F32
    )


def iota(shape, dim):
    return lax.broadcasted_iota(jnp.int32, shape, dim)


def vmem(shape, dtype):
    return pltpu.VMEM(shape, dtype)


def on_core(kernel, shapes, index, *operands, given=(), scratch=(), limit=8):
    return pl.pallas_call(
        kernel,
        in_specs=[pl.BlockSpec(memory_space=pltpu.SMEM)]
        + [pl.BlockSpec(memory_space=pltpu.VMEM)] * (len(operands) + len(given)),
        out_shape=shapes,
        scratch_shapes=scratch,
        compiler_params=pltpu.CompilerParams(vmem_limit_bytes=limit * 1024 * 1024),
    )(index, *(pltpu.with_memory_space_constraint(x, pltpu.VMEM) for x in operands), *given)


def pack_kernel(*refs):
    out = refs[-1]
    blocks = [ref[...] for ref in refs[:-1]]
    both = jnp.concatenate(blocks, axis=0)
    for k in range(16):
        out[k] = both


def pack(*mats):
    return pl.pallas_call(
        pack_kernel,
        out_shape=jax.ShapeDtypeStruct((16, 16 * len(mats), 128), BF16),
        name="pack",
    )(*mats)


def fill_rows(core, own, other, store):
    for a in range(4):
        for b in range(16):
            row0, row1 = (
                place(SETS[c][a // 2][b // 4], SETS[c][a % 2][b % 4], c) * 16 for c in range(2)
            )
            store(pl.multiple_of(jnp.where(core == 0, row0, row1), 16), own, a, b)
            store(pl.multiple_of(jnp.where(core == 0, row1, row0), 16), other, a, b)


def local_kernel(
    core_ref,
    own_ref,
    other_ref,
    tokens_ref,
    norm_gain_ref,
    key_gain_ref,
    removal_gain_ref,
    removal_bias_ref,
    decay_bias_ref,
    extra_ref,
    norm_out_ref,
    mine_ref,
    theirs_ref,
    reads_ref,
    gate_ref,
    conv_ref,
    rim_ref,
    weights,
    normed,
):
    core = core_ref[0] % 2

    def store(row, source, a, b):
        for m in range(MATS):
            lanes = slice((m % 2) * 128, (m % 2) * 128 + 128)
            weights[m // 2, pl.ds(row, 16), lanes] = source[a, b, m * 16 : m * 16 + 16, :]

    fill_rows(core, own_ref, other_ref, store)
    parts = [tokens_ref[j].astype(F32) for j in range(4)]
    total = sum(jnp.sum(part * part, axis=-1, keepdims=True) for part in parts)
    inverse_rms = lax.rsqrt(total * (1.0 / 2048.0) + 1e-06)
    for j in range(4):
        normed[:, j * 512 : j * 512 + 512] = (
            parts[j] * inverse_rms * norm_gain_ref[j : j + 1, :]
        ).astype(BF16)
    products = []
    for p in range(4):
        product = jnp.dot(normed[...], weights[p], preferred_element_type=F32)
        product = product.astype(BF16).astype(F32)
        products += [product[:, :128], product[:, 128:]]
    recept, keys, values, decay_pre, removal_pre, gate_pre, conv_value, conv_gate = products
    gate_ref[...] = norm_out_ref[...] * jax.nn.sigmoid(gate_pre)
    conv_input = (conv_value * jax.nn.sigmoid(conv_gate)).astype(BF16)
    conv_ref[...] = conv_input
    rim_ref[...] = conv_input[LENGTH - 32 :]

    rate = 0.6065306597126334 * jax.nn.sigmoid(decay_bias_ref[...] + decay_pre) + extra_ref[...]
    removal = jax.nn.sigmoid(removal_bias_ref[...] + removal_pre)
    lane = iota((LENGTH, 128), 1)
    first = lane < HEAD
    scaled = keys * key_gain_ref[...]
    square = scaled * scaled
    low = jnp.sum(jnp.where(first, square, 0.0), axis=-1, keepdims=True)
    high = jnp.sum(jnp.where(first, 0.0, square), axis=-1, keepdims=True)
    unit = scaled * lax.rsqrt(jnp.where(first, low, high) + 1e-06)
    written = keys * (1.0 + (removal - 1.0) * removal_gain_ref[...])

    row, column = iota((LENGTH, LENGTH), 0), iota((LENGTH, LENGTH), 1)
    same = (row // BLOCK) == (column // BLOCK)
    strict = same & (row > column)
    inclusive = same & (row >= column)
    falling = -exact(inclusive.astype(F32), rate)
    before = falling + rate
    by_block = falling.reshape(BLOCKS, BLOCK, 128)
    middle = jnp.broadcast_to(
        by_block[:, BLOCK // 2 : BLOCK // 2 + 1], (BLOCKS, BLOCK, 128)
    ).reshape(LENGTH, 128)
    ending = jnp.broadcast_to(by_block[:, BLOCK - 1 :], (BLOCKS, BLOCK, 128)).reshape(LENGTH, 128)
    beta = unit * removal
    rising = jnp.exp(middle - falling)
    alpha_mid = -unit * jnp.exp(before - middle)
    recept_mid = recept * jnp.exp(falling - middle)
    right = jnp.concatenate([beta * rising, written * rising], axis=0)
    start_alpha = -unit * jnp.exp(before)
    start_recept = recept * jnp.exp(falling)
    closing = jnp.exp(ending - falling)
    end_beta = beta * closing
    end_keys = written * closing
    kept = jnp.exp(by_block[:, BLOCK - 1, :])
    turned_values = pltpu.roll(values, HEAD, 1)

    square_row, square_lane = iota((128, 128), 0), iota((128, 128), 1)
    diagonal = square_row == square_lane
    finals = []
    for h in range(2):
        mine = first if h == 0 else jnp.logical_not(first)
        mine_row = (square_row < HEAD) if h == 0 else (square_row >= HEAD)
        left = jnp.concatenate(
            [jnp.where(mine, alpha_mid, 0.0), jnp.where(mine, recept_mid, 0.0)], axis=0
        )
        pairs = dot3(left, right, NT)
        power = jnp.where(strict, pairs[:LENGTH, :LENGTH], 0.0)
        alpha_keys = jnp.where(strict, pairs[:LENGTH, LENGTH:], 0.0)
        recept_beta = jnp.where(inclusive, pairs[LENGTH:, :LENGTH], 0.0)
        recept_keys = jnp.where(inclusive, pairs[LENGTH:, LENGTH:], 0.0)
        value_rows = jnp.where(mine, 0.0, turned_values)
        solved = jnp.where(mine, start_alpha, dot3(alpha_keys, value_rows))
        for step in range(5):
            solved = solved + dot3(power, solved)
            if step < 4:
                power = dot3(power, power)
        query = jnp.where(mine, start_recept, 0.0) + dot3(
            jnp.concatenate([recept_beta, recept_keys], axis=1),
            jnp.concatenate([solved, value_rows], axis=0),
        )
        steps = []
        for b in range(BLOCKS):
            rows = slice(b * BLOCK, b * BLOCK + BLOCK)
            moved = dot3(
                jnp.concatenate([end_beta[rows], end_keys[rows]], axis=0),
                jnp.concatenate([solved[rows], value_rows[rows]], axis=0),
                TN,
            )
            held = jnp.where(diagonal, jnp.broadcast_to(kept[b : b + 1], (128, 128)), 0.0)
            whole = jnp.where(diagonal, 1.0, 0.0)
            steps.append(jnp.where(mine_row, moved + held, whole))
        one = dot3(steps[1], steps[0])
        two = dot3(steps[3], steps[2])
        three = dot3(steps[5], steps[4])
        four = dot3(two, one)
        prefixes = [None, steps[0], one, dot3(steps[2], one), four, dot3(steps[4], four)]
        final = dot3(three, four)[h * HEAD : h * HEAD + HEAD]
        if h == 1:
            final = pltpu.roll(final, HEAD, 1)
        finals.append(final)
        reads_ref[h, 0:BLOCK, :] = query[0:BLOCK]
        for b in range(1, BLOCKS):
            rows = slice(b * BLOCK, b * BLOCK + BLOCK)
            reads_ref[h, rows, :] = dot3(query[rows], prefixes[b])
    mine_ref[...] = jnp.where(core == 0, finals[0], finals[1])
    theirs_ref[...] = jnp.where(core == 0, finals[1], finals[0])


def local_part(index, own, other, tokens, *given):
    return on_core(
        local_kernel,
        (
            vmem((HEAD, 128), F32),
            vmem((HEAD, 128), F32),
            vmem((2, LENGTH, 128), F32),
            vmem((LENGTH, 128), F32),
            vmem((LENGTH, 128), BF16),
            vmem((32, 128), BF16),
        ),
        index,
        own,
        other,
        tokens,
        given=given,
        scratch=[pltpu.VMEM((4, 2048, 256), BF16), pltpu.VMEM((LENGTH, 2048), BF16)],
        limit=28,
    )


def after(later, earlier):
    product = dot3(later[:, :HEAD], earlier)
    return product + jnp.where(iota((HEAD, 128), 1) < HEAD, 0.0, later)


def chained(steps):
    while len(steps) > 1:
        steps = [after(steps[k + 1], steps[k]) for k in range(0, len(steps), 2)]
    return steps[0]


def nothing():
    return jnp.where(iota((HEAD, 128), 0) == iota((HEAD, 128), 1), 1.0, 0.0)


def sent(step):
    return jnp.broadcast_to((step - nothing()).astype(BF16)[None], (8, HEAD, 128))


def received(steps_ref):
    return [steps_ref[k].astype(F32) + nothing() for k in range(8)]


def chip_kernel(core_ref, mine_ref, theirs_ref, out_ref):
    core = core_ref[0] % 2
    mine, theirs = mine_ref[...], theirs_ref[...]
    earlier = jnp.where(core == 0, mine, theirs)
    later = jnp.where(core == 0, theirs, mine)
    out_ref[...] = sent(after(later, earlier))


def row_kernel(place_ref, steps_ref, before_ref, total_ref):
    here = (place_ref[0] // 2) % 8
    steps = received(steps_ref)
    total_ref[...] = sent(chained(steps))
    before_ref[...] = chained([jnp.where(k < here, steps[k], nothing()) for k in range(8)])


def incoming_kernel(place_ref, steps_ref, before_ref, mine_ref, theirs_ref, own_ref, sent_ref):
    here, core = place_ref[0] // 16, place_ref[0] % 2
    steps = received(steps_ref)
    start = chained([jnp.where(k < here, steps[k], nothing()) for k in range(8)])
    at_chip = after(before_ref[...], start)
    earlier = jnp.where(core == 0, mine_ref[...], theirs_ref[...])
    at_second = after(earlier, at_chip)
    own_ref[...] = jnp.where(core == 0, at_chip, at_second)
    sent_ref[...] = jnp.where(core == 0, at_second, at_chip)


def conv_kernel(place_ref, input_ref, rim_ref, taps_ref, bias_ref, filtered_ref, sums_ref):
    padded = jnp.concatenate([rim_ref[...], input_ref[...]], axis=0).astype(F32)
    filtered = jnp.broadcast_to(bias_ref[...], (LENGTH, 128))
    for k in range(TAPS):
        filtered = filtered + taps_ref[k : k + 1, :] * padded[k + 2 : k + 2 + LENGTH]
    filtered_ref[...] = filtered
    ones = jnp.ones((8, 128), F32)
    square = filtered * filtered
    rest = jnp.concatenate([filtered[128:], square[128:]], axis=0)
    at = iota((8, 128), 0)
    sums = jnp.where(at == 0, exact(ones, filtered[:128], NT), 0.0)
    sums = jnp.where(at == 1, exact(ones, square[:128], NT), sums)
    sums_ref[...] = jnp.where(at == 2, exact(ones, rest, NT), sums)


def columns_kernel(core_ref, own_ref, other_ref, out_ref):
    def store(row, source, a, b):
        for m in range(2):
            at = (MATS + m) * 16
            out_ref[pl.ds(row, 16), m * 128 : m * 128 + 128] = source[a, b, at : at + 16, :]

    fill_rows(core_ref[0] % 2, own_ref, other_ref, store)


def final_kernel(
    core_ref,
    reads_ref,
    mine_ref,
    theirs_ref,
    gate_ref,
    filtered_ref,
    sums_ref,
    columns_ref,
    conv_gain_ref,
    out_ref,
):
    core = core_ref[0] % 2
    mine, theirs = mine_ref[...], theirs_ref[...]
    head0 = jnp.where(core == 0, mine, theirs)
    head1 = jnp.where(core == 0, theirs, mine)
    lane = iota((HEAD, 128), 1)
    equal = iota((HEAD, 128), 0)
    zero = jnp.zeros((HEAD, 128), F32)
    right0 = jnp.concatenate(
        [
            jnp.where(lane < HEAD, pltpu.roll(head0, HEAD, 1), zero),
            jnp.where(lane == equal, 1.0, 0.0),
        ],
        axis=0,
    )
    right1 = jnp.concatenate(
        [jnp.where(lane == equal + HEAD, 1.0, 0.0), jnp.where(lane < HEAD, zero, head1)], axis=0
    )
    reads = exact(reads_ref[0], right0) + exact(reads_ref[1], right1)
    first = iota((LENGTH, 128), 1) < HEAD

    def head_mean(x):
        low = jnp.sum(jnp.where(first, x, 0.0), axis=-1, keepdims=True)
        high = jnp.sum(jnp.where(first, 0.0, x), axis=-1, keepdims=True)
        return jnp.where(first, low, high) * (1.0 / HEAD)

    centered = reads - head_mean(reads)
    spread = head_mean(centered * centered)
    scan_out = (centered * lax.rsqrt(spread + 0.00064) * gate_ref[...]).astype(BF16)

    def spread_out(k):
        return exact(sums_ref[...], jnp.where(iota((8, 128), 0) == k, 1.0 / 512.0, 0.0), TN)

    rest = spread_out(2)
    center = jnp.concatenate([spread_out(0), rest[:64]], axis=0)
    second = jnp.concatenate([spread_out(1), rest[64:]], axis=0)
    scaled = (
        (filtered_ref[...] - center)
        * lax.rsqrt(second - center * center + 1e-05)
        * conv_gain_ref[...]
    )
    conv_out = (scaled * jax.nn.sigmoid(scaled)).astype(BF16)
    features = jnp.concatenate([scan_out, conv_out], axis=1)
    for j in range(4):
        out_ref[j] = lax.dot_general(
            features, columns_ref[j * 512 : j * 512 + 512, :], NT, preferred_element_type=F32
        ).astype(BF16)


def to_each(x, groups):
    return lax.all_to_all(x, "sp", 0, 0, tiled=True, axis_index_groups=groups)


def layer(
    tokens,
    norm_gain,
    query_weight,
    key_weight,
    value_weight,
    decay_weight,
    removal_weight,
    gate_weight,
    key_gain,
    removal_gain,
    removal_bias,
    decay_bias,
    decay_extra,
    scan_norm_gain,
    conv_value_weight,
    conv_gate_weight,
    conv_taps,
    conv_bias,
    conv_norm_gain,
    out_scan_weight,
    out_conv_weight,
):
    index = lax.axis_index("sp").astype(jnp.int32)[None]
    row = lambda v: v.reshape(1, -1)

    packed = pack(
        query_weight,
        key_weight,
        value_weight,
        decay_weight,
        removal_weight,
        gate_weight,
        conv_value_weight,
        conv_gate_weight,
        out_scan_weight.T,
        out_conv_weight.T,
    )
    stage1 = to_each(packed, FAR)
    wide = jnp.broadcast_to(stage1[None], (4, *stage1.shape))
    stage2 = to_each(wide, NEAR)
    whole = lax.all_gather(tokens, "tp")
    swapped = lax.ppermute(stage2, "sp", SWAP)

    mine, theirs, reads, gate, conv_input, rim = local_part(
        index,
        stage2,
        swapped,
        whole,
        norm_gain.reshape(4, 512),
        row(key_gain),
        row(removal_gain),
        row(removal_bias),
        row(decay_bias),
        decay_extra,
        row(scan_norm_gain),
    )

    theirs = lax.ppermute(theirs, "sp", SWAP)
    rim = lax.ppermute(rim, "sp", ONWARD)
    table = vmem((8, HEAD, 128), BF16)
    step = vmem((HEAD, 128), F32)
    chip = on_core(chip_kernel, table, index, mine, theirs)
    chips = to_each(chip, Y_AXIS)
    before, total = on_core(row_kernel, (step, table), index, chips)
    totals = to_each(total, Z_AXIS)
    own_state, sent_state = on_core(
        incoming_kernel, (step, step), index, totals, before, mine, theirs
    )
    other_state = lax.ppermute(sent_state, "sp", SWAP)

    filtered, sums = on_core(
        conv_kernel,
        (vmem((LENGTH, 128), F32), vmem((8, 128), F32)),
        index,
        conv_input,
        rim,
        given=(conv_taps, row(conv_bias)),
    )
    sums = lax.psum(sums, "tp")
    columns = on_core(columns_kernel, vmem((2048, 256), BF16), index, stage2, swapped)

    terms = on_core(
        final_kernel,
        vmem((4, LENGTH, 512), BF16),
        index,
        reads,
        own_state,
        other_state,
        gate,
        filtered,
        sums,
        columns,
        given=(row(conv_norm_gain),),
    )
    parts = lax.all_to_all(terms, "tp", 0, 0, tiled=True)
    return jnp.sum(parts.astype(F32), axis=0).astype(BF16)


def solution(mesh):
    weights = P("sp", "tp")
    in_specs = (
        (P("sp", "tp"), P())
        + (weights,) * 6
        + (P("tp"),) * 4
        + (P("sp", "tp"), P("tp"), weights, weights, P(None, "tp"), P("tp"), P("tp"))
        + (P("tp", "sp"), P("tp", "sp"))
    )
    return jax.shard_map(
        layer, mesh=mesh, in_specs=in_specs, out_specs=P("sp", "tp"), check_vma=False
    )
```

```python
import functools

import jax
import jax.numpy as jnp
from jax import lax
from jax.experimental import pallas as pl
from jax.experimental.pallas import tpu as pltpu
from jax.sharding import PartitionSpec as P

HEAD = 64
TAPS = 31
BLOCK = 32
LENGTH = 192
BLOCKS = LENGTH // BLOCK
MATS = 8
F32 = jnp.float32
BF16 = jnp.bfloat16

NN = (((1,), (0,)), ((), ()))
NT = (((1,), (1,)), ((), ()))
TN = (((0,), (0,)), ((), ()))


def place(z, y, c):
    return z * 16 + y * 2 + c


SETS = (((0, 2, 5, 7), (1, 3, 4, 6)), ((1, 3, 6, 0), (2, 4, 5, 7)))
FAR = [
    [place(z, y, c) for z in SETS[c][p] for y in SETS[c][q]]
    for c in range(2)
    for p in range(2)
    for q in range(2)
]


def near(k, p, c):
    pair = ((2 * k + c) % 8, (2 * k + c + 1) % 8)
    return [chip for chip in pair if chip in SETS[c][p]][0]


NEAR = [
    [place(near(k, p, c), near(l, q, c), c) for p in range(2) for q in range(2)]
    for c in range(2)
    for k in range(4)
    for l in range(4)
]
Y_AXIS = [[place(z, y, c) for y in range(8)] for z in range(8) for c in range(2)]
Z_AXIS = [[place(z, y, c) for z in range(8)] for y in range(8) for c in range(2)]
SWAP = [(i, i ^ 1) for i in range(128)]
ONWARD = [(i, i + 1) for i in range(127)]


def split(x):
    high = x.astype(BF16)
    return high, (x - high.astype(F32)).astype(BF16)


def dot3(a, b, dims=NN):
    a_high, a_low = split(a)
    b_high, b_low = split(b)
    one = functools.partial(lax.dot_general, dimension_numbers=dims, preferred_element_type=F32)
    return one(a_high, b_high) + (one(a_high, b_low) + one(a_low, b_high))


def exact(a, b, dims=NN):
    return lax.dot_general(
        a, b, dims, precision=lax.Precision.HIGHEST, preferred_element_type=F32
    )


def sums_of(ones, x):
    high = x.astype(BF16)
    middle, low = split(x - high.astype(F32))
    one = lambda part: jnp.dot(ones, part, preferred_element_type=F32)
    return one(high) + (one(middle) + one(low))


def iota(shape, dim):
    return lax.broadcasted_iota(jnp.int32, shape, dim)


def vmem(shape, dtype):
    return pltpu.VMEM(shape, dtype)


def on_core(kernel, shapes, index, *operands, given=(), scratch=(), limit=8):
    return pl.pallas_call(
        kernel,
        in_specs=[pl.BlockSpec(memory_space=pltpu.SMEM)]
        + [pl.BlockSpec(memory_space=pltpu.VMEM)] * (len(operands) + len(given)),
        out_shape=shapes,
        scratch_shapes=scratch,
        compiler_params=pltpu.CompilerParams(vmem_limit_bytes=limit * 1024 * 1024),
    )(index, *(pltpu.with_memory_space_constraint(x, pltpu.VMEM) for x in operands), *given)


def pack_kernel(*refs):
    out = refs[-1]
    blocks = [ref[...] for ref in refs[:-1]]
    both = jnp.concatenate(blocks, axis=0)
    for k in range(16):
        out[k] = both


def pack(*mats):
    return pl.pallas_call(
        pack_kernel,
        out_shape=jax.ShapeDtypeStruct((16, 16 * len(mats), 128), BF16),
        name="pack",
    )(*mats)


def fill_rows(core, source, height, store):
    for a in range(4):
        for b in range(16):
            row0, row1 = (
                height(SETS[c][a // 2][b // 4], SETS[c][a % 2][b % 4], c) for c in range(2)
            )
            store(pl.multiple_of(jnp.where(core == 0, row0, row1), 16), source, a, b)


def norm_kernel(place_ref, tokens_ref, gain_ref, *refs):
    vectors, (taps_ref, extra_ref), (normed_ref, table_ref, extra_out_ref) = (
        refs[:-5],
        refs[-5:-3],
        refs[-3:],
    )
    parts = [tokens_ref[j].astype(F32) for j in range(4)]
    total = sum(jnp.sum(part * part, axis=-1, keepdims=True) for part in parts)
    inverse_rms = lax.rsqrt(total * (1.0 / 2048.0) + 1e-06)
    goal = iota((256, 256), 1)
    source = ((goal % 128) // 16) * 32 + (goal // 128) * 16 + goal % 16
    moves = jnp.where(iota((256, 256), 0) == source, 1.0, 0.0).astype(BF16)
    for j in range(4):
        normed = (parts[j] * inverse_rms * gain_ref[j : j + 1, :]).astype(BF16)
        for k in range(2):
            moved = jnp.dot(
                normed[:, k * 256 : k * 256 + 256], moves, preferred_element_type=F32
            ).astype(BF16)
            z = j * 2 + k
            normed_ref[0, :, z * 128 : z * 128 + 128] = moved[:, :128]
            normed_ref[1, :, z * 128 : z * 128 + 128] = moved[:, 128:]
    for k, ref in enumerate(vectors):
        table_ref[k : k + 1, :] = ref[...]
    table_ref[8 : 8 + TAPS, :] = taps_ref[...]
    extra_out_ref[...] = extra_ref[...]


def projected(core, source_ref, normed_ref, weights):
    def store(row, source, a, b):
        for m in range(MATS):
            lanes = slice((m % 2) * 128, (m % 2) * 128 + 128)
            weights[m // 2, pl.ds(row, 16), lanes] = source[a, b, m * 16 : m * 16 + 16, :]

    fill_rows(core, source_ref, lambda z, y, c: (z * 8 + y) * 16, store)
    normed = normed_ref[core]
    return [jnp.dot(normed, weights[p], preferred_element_type=F32) for p in range(MATS // 2)]


def half_kernel(place_ref, own_ref, normed_ref, out_ref, weights):
    products = projected(place_ref[0] % 2, own_ref, normed_ref, weights)
    for p in range(MATS // 2):
        out_ref[p] = products[p]


def local_kernel(
    core_ref,
    other_ref,
    normed_ref,
    half_ref,
    table_ref,
    extra_ref,
    mine_ref,
    theirs_ref,
    reads_ref,
    gate_ref,
    conv_ref,
    rim_ref,
    weights,
):
    core = core_ref[0] % 2
    products = []
    for p, product in enumerate(projected(1 - core, other_ref, normed_ref, weights)):
        product = (product + half_ref[p]).astype(BF16).astype(F32)
        products += [product[:, :128], product[:, 128:]]
    recept, keys, values, decay_pre, removal_pre, gate_pre, conv_value, conv_gate = products
    key_gain, removal_gain, removal_bias, decay_bias, norm_out = (
        table_ref[k : k + 1, :] for k in range(5)
    )
    gate_ref[...] = norm_out * jax.nn.sigmoid(gate_pre)
    conv_input = (conv_value * jax.nn.sigmoid(conv_gate)).astype(BF16)
    conv_ref[...] = conv_input
    rim_ref[...] = conv_input[LENGTH - 32 :]

    rate = 0.6065306597126334 * jax.nn.sigmoid(decay_bias + decay_pre) + extra_ref[...]
    removal = jax.nn.sigmoid(removal_bias + removal_pre)
    lane = iota((LENGTH, 128), 1)
    first = lane < HEAD
    scaled = keys * key_gain
    square = scaled * scaled
    low = jnp.sum(jnp.where(first, square, 0.0), axis=-1, keepdims=True)
    high = jnp.sum(jnp.where(first, 0.0, square), axis=-1, keepdims=True)
    unit = scaled * lax.rsqrt(jnp.where(first, low, high) + 1e-06)
    written = keys * (1.0 + (removal - 1.0) * removal_gain)

    row, column = iota((LENGTH, LENGTH), 0), iota((LENGTH, LENGTH), 1)
    same = (row // BLOCK) == (column // BLOCK)
    strict = same & (row > column)
    inclusive = same & (row >= column)
    wide_row, wide_column = iota((LENGTH, 2 * LENGTH), 0), iota((LENGTH, 2 * LENGTH), 1)
    wide_column = jnp.where(wide_column >= LENGTH, wide_column - LENGTH, wide_column)
    inclusive_twice = ((wide_row // BLOCK) == (wide_column // BLOCK)) & (wide_row >= wide_column)
    falling = -sums_of(jnp.where(inclusive, 1.0, 0.0).astype(BF16), rate)
    before = falling + rate
    by_block = falling.reshape(BLOCKS, BLOCK, 128)
    middle = jnp.broadcast_to(
        by_block[:, BLOCK // 2 : BLOCK // 2 + 1], (BLOCKS, BLOCK, 128)
    ).reshape(LENGTH, 128)
    ending = jnp.broadcast_to(by_block[:, BLOCK - 1 :], (BLOCKS, BLOCK, 128)).reshape(LENGTH, 128)
    beta = unit * removal
    rising = jnp.exp(middle - falling)
    alpha_mid = -unit * jnp.exp(before - middle)
    recept_mid = recept * jnp.exp(falling - middle)
    right = jnp.concatenate([beta * rising, written * rising], axis=0)
    start_alpha = -unit * jnp.exp(before)
    start_recept = recept * jnp.exp(falling)
    closing = jnp.exp(ending - falling)
    end_beta = beta * closing
    end_keys = written * closing
    kept = jnp.exp(by_block[:, BLOCK - 1, :])
    turned_values = pltpu.roll(values, HEAD, 1)

    square_row, square_lane = iota((128, 128), 0), iota((128, 128), 1)
    diagonal = square_row == square_lane
    own = [first, jnp.logical_not(first)]
    own_row = [square_row < HEAD, square_row >= HEAD]
    power, solved, query, value_rows = [], [], [], []
    recept_pairs = []
    for h in range(2):
        left = jnp.concatenate(
            [jnp.where(own[h], alpha_mid, 0.0), jnp.where(own[h], recept_mid, 0.0)], axis=0
        )
        pairs = dot3(left, right, NT)
        power.append(jnp.where(strict, pairs[:LENGTH, :LENGTH], 0.0))
        alpha_keys = jnp.where(strict, pairs[:LENGTH, LENGTH:], 0.0)
        recept_pairs.append(jnp.where(inclusive_twice, pairs[LENGTH:], 0.0))
        value_rows.append(jnp.where(own[h], 0.0, turned_values))
        solved.append(jnp.where(own[h], start_alpha, dot3(alpha_keys, value_rows[h])))
    for step in range(5):
        solved = [solved[h] + dot3(power[h], solved[h]) for h in range(2)]
        if step < 4:
            power = [dot3(power[h], power[h]) for h in range(2)]
    for h in range(2):
        known = jnp.concatenate([solved[h], value_rows[h]], axis=0)
        query.append(jnp.where(own[h], start_recept, 0.0) + dot3(recept_pairs[h], known))
    steps = [[], []]
    whole = jnp.where(diagonal, 1.0, 0.0)
    for b in range(BLOCKS):
        rows = slice(b * BLOCK, b * BLOCK + BLOCK)
        ends = jnp.concatenate([end_beta[rows], end_keys[rows]], axis=0)
        held = jnp.where(diagonal, jnp.broadcast_to(kept[b : b + 1], (128, 128)), 0.0)
        for h in range(2):
            known = jnp.concatenate([solved[h][rows], value_rows[h][rows]], axis=0)
            steps[h].append(jnp.where(own_row[h], dot3(ends, known, TN) + held, whole))
    one = [dot3(steps[h][1], steps[h][0]) for h in range(2)]
    two = [dot3(steps[h][3], steps[h][2]) for h in range(2)]
    three = [dot3(steps[h][5], steps[h][4]) for h in range(2)]
    four = [dot3(two[h], one[h]) for h in range(2)]
    finals = [dot3(three[h], four[h])[h * HEAD : h * HEAD + HEAD] for h in range(2)]
    finals[1] = pltpu.roll(finals[1], HEAD, 1)
    mine_ref[...] = jnp.where(core == 0, finals[0], finals[1])
    theirs_ref[...] = jnp.where(core == 0, finals[1], finals[0])
    for h in range(2):
        prefixes = [
            None,
            steps[h][0],
            one[h],
            dot3(steps[h][2], one[h]),
            four[h],
            dot3(steps[h][4], four[h]),
        ]
        reads_ref[h, 0:BLOCK, :] = query[h][0:BLOCK]
        for b in range(1, BLOCKS):
            rows = slice(b * BLOCK, b * BLOCK + BLOCK)
            reads_ref[h, rows, :] = dot3(query[h][rows], prefixes[b])


WEIGHTS = (MATS // 2, 1024, 256)


def after(later, earlier):
    product = dot3(later[:, :HEAD], earlier)
    return product + jnp.where(iota((HEAD, 128), 1) < HEAD, 0.0, later)


def chained(steps):
    while len(steps) > 1:
        steps = [after(steps[k + 1], steps[k]) for k in range(0, len(steps), 2)]
    return steps[0]


def nothing():
    return jnp.where(iota((HEAD, 128), 0) == iota((HEAD, 128), 1), 1.0, 0.0)


def sent(step):
    return jnp.broadcast_to((step - nothing()).astype(BF16)[None], (8, HEAD, 128))


def received(steps_ref):
    return [steps_ref[k].astype(F32) + nothing() for k in range(8)]


def chip_kernel(core_ref, mine_ref, theirs_ref, out_ref):
    core = core_ref[0] % 2
    mine, theirs = mine_ref[...], theirs_ref[...]
    earlier = jnp.where(core == 0, mine, theirs)
    later = jnp.where(core == 0, theirs, mine)
    out_ref[...] = sent(after(later, earlier))


def row_kernel(place_ref, steps_ref, before_ref, total_ref):
    here = (place_ref[0] // 2) % 8
    steps = received(steps_ref)
    total_ref[...] = sent(chained(steps))
    before_ref[...] = chained([jnp.where(k < here, steps[k], nothing()) for k in range(8)])


def incoming_kernel(place_ref, steps_ref, before_ref, mine_ref, theirs_ref, own_ref, sent_ref):
    here, core = place_ref[0] // 16, place_ref[0] % 2
    steps = received(steps_ref)
    start = chained([jnp.where(k < here, steps[k], nothing()) for k in range(8)])
    at_chip = after(before_ref[...], start)
    earlier = jnp.where(core == 0, mine_ref[...], theirs_ref[...])
    at_second = after(earlier, at_chip)
    own_ref[...] = jnp.where(core == 0, at_chip, at_second)
    sent_ref[...] = jnp.where(core == 0, at_second, at_chip)


def conv_kernel(place_ref, input_ref, rim_ref, table_ref, filtered_ref, sums_ref):
    padded = jnp.concatenate([rim_ref[...], input_ref[...]], axis=0).astype(F32)
    filtered = jnp.broadcast_to(table_ref[5:6, :], (LENGTH, 128))
    for k in range(TAPS):
        filtered = filtered + table_ref[8 + k : 9 + k, :] * padded[k + 2 : k + 2 + LENGTH]
    filtered_ref[...] = filtered
    ones = jnp.ones((8, 128), F32)
    square = filtered * filtered
    rest = jnp.concatenate([filtered[128:], square[128:]], axis=0)
    at = iota((8, 128), 0)
    sums = jnp.where(at == 0, exact(ones, filtered[:128], NT), 0.0)
    sums = jnp.where(at == 1, exact(ones, square[:128], NT), sums)
    sums_ref[...] = jnp.where(at == 2, exact(ones, rest, NT), sums)


def columns_kernel(core_ref, own_ref, other_ref, out_ref):
    core = core_ref[0] % 2

    def store(row, source, a, b):
        for m in range(2):
            at = (MATS + m) * 16
            out_ref[pl.ds(row, 16), m * 128 : m * 128 + 128] = source[a, b, at : at + 16, :]

    height = lambda z, y, c: place(z, y, c) * 16
    fill_rows(core, own_ref, height, store)
    fill_rows(1 - core, other_ref, height, store)


def final_kernel(
    core_ref,
    reads_ref,
    mine_ref,
    theirs_ref,
    gate_ref,
    filtered_ref,
    sums_ref,
    columns_ref,
    table_ref,
    out_ref,
):
    core = core_ref[0] % 2
    mine, theirs = mine_ref[...], theirs_ref[...]
    head0 = jnp.where(core == 0, mine, theirs)
    head1 = jnp.where(core == 0, theirs, mine)
    lane = iota((HEAD, 128), 1)
    equal = iota((HEAD, 128), 0)
    zero = jnp.zeros((HEAD, 128), F32)
    right0 = jnp.concatenate(
        [
            jnp.where(lane < HEAD, pltpu.roll(head0, HEAD, 1), zero),
            jnp.where(lane == equal, 1.0, 0.0),
        ],
        axis=0,
    )
    right1 = jnp.concatenate(
        [jnp.where(lane == equal + HEAD, 1.0, 0.0), jnp.where(lane < HEAD, zero, head1)], axis=0
    )
    reads = exact(reads_ref[0], right0) + exact(reads_ref[1], right1)
    first = iota((LENGTH, 128), 1) < HEAD

    def head_mean(x):
        low = jnp.sum(jnp.where(first, x, 0.0), axis=-1, keepdims=True)
        high = jnp.sum(jnp.where(first, 0.0, x), axis=-1, keepdims=True)
        return jnp.where(first, low, high) * (1.0 / HEAD)

    centered = reads - head_mean(reads)
    spread = head_mean(centered * centered)
    scan_out = (centered * lax.rsqrt(spread + 0.00064) * gate_ref[...]).astype(BF16)

    def spread_out(k):
        return exact(sums_ref[...], jnp.where(iota((8, 128), 0) == k, 1.0 / 512.0, 0.0), TN)

    rest = spread_out(2)
    center = jnp.concatenate([spread_out(0), rest[:64]], axis=0)
    second = jnp.concatenate([spread_out(1), rest[64:]], axis=0)
    scaled = (
        (filtered_ref[...] - center)
        * lax.rsqrt(second - center * center + 1e-05)
        * table_ref[6:7, :]
    )
    conv_out = (scaled * jax.nn.sigmoid(scaled)).astype(BF16)
    features = jnp.concatenate([scan_out, conv_out], axis=1)
    for j in range(4):
        out_ref[j] = lax.dot_general(
            features, columns_ref[j * 512 : j * 512 + 512, :], NT, preferred_element_type=F32
        ).astype(BF16)


def to_each(x, groups):
    return lax.all_to_all(x, "sp", 0, 0, tiled=True, axis_index_groups=groups)


def layer(
    tokens,
    norm_gain,
    query_weight,
    key_weight,
    value_weight,
    decay_weight,
    removal_weight,
    gate_weight,
    key_gain,
    removal_gain,
    removal_bias,
    decay_bias,
    decay_extra,
    scan_norm_gain,
    conv_value_weight,
    conv_gate_weight,
    conv_taps,
    conv_bias,
    conv_norm_gain,
    out_scan_weight,
    out_conv_weight,
):
    index = lax.axis_index("sp").astype(jnp.int32)[None]
    row = lambda v: v.reshape(1, -1)

    packed = pack(
        query_weight,
        key_weight,
        value_weight,
        decay_weight,
        removal_weight,
        gate_weight,
        conv_value_weight,
        conv_gate_weight,
        out_scan_weight.T,
        out_conv_weight.T,
    )
    stage1 = to_each(packed, FAR)
    wide = jnp.broadcast_to(stage1[None], (4, *stage1.shape))
    stage2 = to_each(wide, NEAR)
    whole = lax.all_gather(tokens, "tp")
    normed, table, extra = on_core(
        norm_kernel,
        (vmem((2, LENGTH, 1024), BF16), vmem((40, 128), F32), vmem((LENGTH, 128), F32)),
        index,
        whole,
        given=(
            norm_gain.reshape(4, 512),
            row(key_gain),
            row(removal_gain),
            row(removal_bias),
            row(decay_bias),
            row(scan_norm_gain),
            row(conv_bias),
            row(conv_norm_gain),
            conv_taps,
            decay_extra,
        ),
    )
    swapped = lax.ppermute(stage2, "sp", SWAP)
    half = on_core(
        half_kernel,
        vmem((MATS // 2, LENGTH, 256), F32),
        index,
        stage2,
        normed,
        scratch=[pltpu.VMEM(WEIGHTS, BF16)],
        limit=16,
    )
    mine, theirs, reads, gate, conv_input, rim = on_core(
        local_kernel,
        (
            vmem((HEAD, 128), F32),
            vmem((HEAD, 128), F32),
            vmem((2, LENGTH, 128), F32),
            vmem((LENGTH, 128), F32),
            vmem((LENGTH, 128), BF16),
            vmem((32, 128), BF16),
        ),
        index,
        swapped,
        normed,
        half,
        table,
        extra,
        scratch=[pltpu.VMEM(WEIGHTS, BF16)],
        limit=28,
    )

    theirs = lax.ppermute(theirs, "sp", SWAP)
    rim = lax.ppermute(rim, "sp", ONWARD)
    message = vmem((8, HEAD, 128), BF16)
    step = vmem((HEAD, 128), F32)
    chip = on_core(chip_kernel, message, index, mine, theirs)
    chips = to_each(chip, Y_AXIS)
    before, total = on_core(row_kernel, (step, message), index, chips)
    totals = to_each(total, Z_AXIS)
    own_state, sent_state = on_core(
        incoming_kernel, (step, step), index, totals, before, mine, theirs
    )
    other_state = lax.ppermute(sent_state, "sp", SWAP)

    filtered, sums = on_core(
        conv_kernel, (vmem((LENGTH, 128), F32), vmem((8, 128), F32)), index, conv_input, rim, table
    )
    sums = lax.psum(sums, "tp")
    columns = on_core(columns_kernel, vmem((2048, 256), BF16), index, stage2, swapped)

    terms = on_core(
        final_kernel,
        vmem((4, LENGTH, 512), BF16),
        index,
        reads,
        own_state,
        other_state,
        gate,
        filtered,
        sums,
        columns,
        table,
    )
    parts = lax.all_to_all(terms, "tp", 0, 0, tiled=True)
    return jnp.sum(parts.astype(F32), axis=0).astype(BF16)


def solution(mesh):
    weights = P("sp", "tp")
    in_specs = (
        (P("sp", "tp"), P())
        + (weights,) * 6
        + (P("tp"),) * 4
        + (P("sp", "tp"), P("tp"), weights, weights, P(None, "tp"), P("tp"), P("tp"))
        + (P("tp", "sp"), P("tp", "sp"))
    )
    return jax.shard_map(
        layer, mesh=mesh, in_specs=in_specs, out_specs=P("sp", "tp"), check_vma=False
    )
```

```python
import functools

import jax
import jax.numpy as jnp
from jax import lax
from jax.experimental import pallas as pl
from jax.experimental.pallas import tpu as pltpu
from jax.sharding import PartitionSpec as P

HEAD = 64
TAPS = 31
BLOCK = 32
LENGTH = 192
BLOCKS = LENGTH // BLOCK
MATS = 8
F32 = jnp.float32
BF16 = jnp.bfloat16

NN = (((1,), (0,)), ((), ()))
NT = (((1,), (1,)), ((), ()))
TN = (((0,), (0,)), ((), ()))


def place(z, y, c):
    return z * 16 + y * 2 + c


SETS = (((0, 2, 5, 7), (1, 3, 4, 6)), ((1, 3, 6, 0), (2, 4, 5, 7)))
FAR_Y = [[[place(z, y, c) for y in ys] for z in range(8) for ys in SETS[c]] for c in range(2)]
FAR_Z = [[[place(z, y, c) for z in zs] for y in range(8) for zs in SETS[c]] for c in range(2)]
FAR_FIRST = FAR_Y[0] + FAR_Z[1]
FAR_SECOND = FAR_Z[0] + FAR_Y[1]


def partner(v, c):
    return v ^ 1 if c == 0 else (((v - 1) % 8 ^ 1) + 1) % 8


def neighbours(along_z, along_y):
    return [
        (place(z, y, c), place(partner(z, c) if along_z else z, partner(y, c) if along_y else y, c))
        for z in range(8)
        for y in range(8)
        for c in range(2)
    ]


Y_AXIS = [[place(z, y, c) for y in range(8)] for z in range(8) for c in range(2)]
Z_AXIS = [[place(z, y, c) for z in range(8)] for y in range(8) for c in range(2)]
SWAP = [(i, i ^ 1) for i in range(128)]
ONWARD = [(i, i + 1) for i in range(127)]


def split(x):
    high = x.astype(BF16)
    return high, (x - high.astype(F32)).astype(BF16)


def dot3(a, b, dims=NN):
    a_high, a_low = split(a)
    b_high, b_low = split(b)
    one = functools.partial(lax.dot_general, dimension_numbers=dims, preferred_element_type=F32)
    return one(a_high, b_high) + (one(a_high, b_low) + one(a_low, b_high))


def exact(a, b, dims=NN):
    return lax.dot_general(
        a, b, dims, precision=lax.Precision.HIGHEST, preferred_element_type=F32
    )


def sums_of(ones, x):
    high = x.astype(BF16)
    middle, low = split(x - high.astype(F32))
    one = lambda part: jnp.dot(ones, part, preferred_element_type=F32)
    return one(high) + (one(middle) + one(low))


def iota(shape, dim):
    return lax.broadcasted_iota(jnp.int32, shape, dim)


def vmem(shape, dtype):
    return pltpu.VMEM(shape, dtype)


def on_core(kernel, shapes, index, *operands, given=(), scratch=(), limit=8):
    return pl.pallas_call(
        kernel,
        in_specs=[pl.BlockSpec(memory_space=pltpu.SMEM)]
        + [pl.BlockSpec(memory_space=pltpu.VMEM)] * (len(operands) + len(given)),
        out_shape=shapes,
        scratch_shapes=scratch,
        compiler_params=pltpu.CompilerParams(vmem_limit_bytes=limit * 1024 * 1024),
    )(index, *(pltpu.with_memory_space_constraint(x, pltpu.VMEM) for x in operands), *given)


def pack_kernel(*refs):
    out = refs[-1]
    blocks = [ref[...] for ref in refs[:-1]]
    both = jnp.concatenate(blocks, axis=0)
    for k in range(4):
        out[k] = both


def pack(*mats):
    return pl.pallas_call(
        pack_kernel,
        out_shape=jax.ShapeDtypeStruct((4, 16 * len(mats), 128), BF16),
        name="pack",
    )(*mats)


FLIPS = ((0, 0), (0, 1), (1, 0), (1, 1))


def chosen(conditions, values):
    if not conditions:
        return values[0]
    half = len(values) // 2
    low, high = (chosen(conditions[1:], part) for part in (values[:half], values[half:]))
    return low if isinstance(low, int) and low == high else jnp.where(conditions[0], high, low)


def fill_rows(index, core, pieces, height, store):
    second = core == 1

    def axis(position):
        in_set1 = functools.reduce(
            jnp.logical_or,
            [
                jnp.logical_and(second == (c == 1), position == v)
                for c in range(2)
                for v in SETS[c][1]
            ],
        )
        return [
            [
                chosen(
                    (second, in_set1),
                    [SETS[c][p ^ flip][k] for c in range(2) for p in range(2)],
                )
                for k in range(4)
            ]
            for flip in range(2)
        ]

    zs, ys = axis(index // 16), axis((index // 2) % 8)
    for piece, (flip_z, flip_y) in zip(pieces, FLIPS):
        for b in range(16):
            i, j = b // 4, b % 4
            z = jnp.where(second, zs[flip_z][j], zs[flip_z][i])
            y = jnp.where(second, ys[flip_y][i], ys[flip_y][j])
            store(pl.multiple_of(height(z, y, core), 16), piece, b)


def norm_kernel(place_ref, t0_ref, t1_ref, t2_ref, t3_ref, gain_ref, *refs):
    vectors, (taps_ref, extra_ref), (normed_ref, table_ref, extra_out_ref) = (
        refs[:-5],
        refs[-5:-3],
        refs[-3:],
    )
    parts = [ref[...].astype(F32) for ref in (t0_ref, t1_ref, t2_ref, t3_ref)]
    total = sum(jnp.sum(part * part, axis=-1, keepdims=True) for part in parts)
    inverse_rms = lax.rsqrt(total * (1.0 / 2048.0) + 1e-06)
    goal = iota((256, 256), 1)
    source = ((goal % 128) // 16) * 32 + (goal // 128) * 16 + goal % 16
    moves = jnp.where(iota((256, 256), 0) == source, 1.0, 0.0).astype(BF16)
    for k, part in enumerate(parts):
        j = (place_ref[1] + 4 - k) % 4
        normed = (part * inverse_rms * gain_ref[pl.ds(j, 1), :]).astype(BF16)
        for h in range(2):
            moved = jnp.dot(
                normed[:, h * 256 : h * 256 + 256], moves, preferred_element_type=F32
            ).astype(BF16)
            normed_ref[0, j * 2 + h] = moved[:, :128]
            normed_ref[1, j * 2 + h] = moved[:, 128:]
    for k, ref in enumerate(vectors):
        table_ref[k : k + 1, :] = ref[...]
    table_ref[8 : 8 + TAPS, :] = taps_ref[...]
    extra_out_ref[...] = extra_ref[...]


def projected(index, core, pieces, normed_ref, weights):
    def store(row, piece, b):
        for m in range(MATS):
            lanes = slice((m % 2) * 128, (m % 2) * 128 + 128)
            weights[m // 2, pl.ds(row, 16), lanes] = piece[b, m * 16 : m * 16 + 16, :]

    fill_rows(index, core, pieces, lambda z, y, c: (z * 8 + y) * 16, store)
    normed = jnp.concatenate([normed_ref[core, z] for z in range(8)], axis=1)
    return [jnp.dot(normed, weights[p], preferred_element_type=F32) for p in range(MATS // 2)]


def half_kernel(place_ref, p0, p1, p2, p3, normed_ref, out_ref, weights):
    index = place_ref[0]
    products = projected(index, index % 2, (p0, p1, p2, p3), normed_ref, weights)
    for p in range(MATS // 2):
        out_ref[p] = products[p]


def local_kernel(
    core_ref,
    p0,
    p1,
    p2,
    p3,
    normed_ref,
    half_ref,
    table_ref,
    extra_ref,
    mine_ref,
    theirs_ref,
    reads_ref,
    gate_ref,
    conv_ref,
    rim_ref,
    weights,
):
    core = core_ref[0] % 2
    products = []
    others = projected(core_ref[0], 1 - core, (p0, p1, p2, p3), normed_ref, weights)
    for p, product in enumerate(others):
        product = (product + half_ref[p]).astype(BF16).astype(F32)
        products += [product[:, :128], product[:, 128:]]
    recept, keys, values, decay_pre, removal_pre, gate_pre, conv_value, conv_gate = products
    key_gain, removal_gain, removal_bias, decay_bias, norm_out = (
        table_ref[k : k + 1, :] for k in range(5)
    )
    gate_ref[...] = norm_out * jax.nn.sigmoid(gate_pre)
    conv_input = (conv_value * jax.nn.sigmoid(conv_gate)).astype(BF16)
    conv_ref[...] = conv_input
    rim_ref[...] = conv_input[LENGTH - 32 :]

    rate = 0.6065306597126334 * jax.nn.sigmoid(decay_bias + decay_pre) + extra_ref[...]
    removal = jax.nn.sigmoid(removal_bias + removal_pre)
    lane = iota((LENGTH, 128), 1)
    first = lane < HEAD
    scaled = keys * key_gain
    square = scaled * scaled
    low = jnp.sum(jnp.where(first, square, 0.0), axis=-1, keepdims=True)
    high = jnp.sum(jnp.where(first, 0.0, square), axis=-1, keepdims=True)
    unit = scaled * lax.rsqrt(jnp.where(first, low, high) + 1e-06)
    written = keys * (1.0 + (removal - 1.0) * removal_gain)

    row, column = iota((LENGTH, LENGTH), 0), iota((LENGTH, LENGTH), 1)
    same = (row // BLOCK) == (column // BLOCK)
    strict = same & (row > column)
    inclusive = same & (row >= column)
    wide_row, wide_column = iota((LENGTH, 2 * LENGTH), 0), iota((LENGTH, 2 * LENGTH), 1)
    wide_column = jnp.where(wide_column >= LENGTH, wide_column - LENGTH, wide_column)
    inclusive_twice = ((wide_row // BLOCK) == (wide_column // BLOCK)) & (wide_row >= wide_column)
    falling = -sums_of(jnp.where(inclusive, 1.0, 0.0).astype(BF16), rate)
    before = falling + rate
    by_block = falling.reshape(BLOCKS, BLOCK, 128)
    middle = jnp.broadcast_to(
        by_block[:, BLOCK // 2 : BLOCK // 2 + 1], (BLOCKS, BLOCK, 128)
    ).reshape(LENGTH, 128)
    ending = jnp.broadcast_to(by_block[:, BLOCK - 1 :], (BLOCKS, BLOCK, 128)).reshape(LENGTH, 128)
    beta = unit * removal
    rising = jnp.exp(middle - falling)
    alpha_mid = -unit * jnp.exp(before - middle)
    recept_mid = recept * jnp.exp(falling - middle)
    right = jnp.concatenate([beta * rising, written * rising], axis=0)
    start_alpha = -unit * jnp.exp(before)
    start_recept = recept * jnp.exp(falling)
    closing = jnp.exp(ending - falling)
    end_beta = beta * closing
    end_keys = written * closing
    kept = jnp.exp(by_block[:, BLOCK - 1, :])
    turned_values = pltpu.roll(values, HEAD, 1)

    square_row, square_lane = iota((128, 128), 0), iota((128, 128), 1)
    diagonal = square_row == square_lane
    own = [first, jnp.logical_not(first)]
    own_row = [square_row < HEAD, square_row >= HEAD]
    power, solved, query, value_rows = [], [], [], []
    recept_pairs = []
    for h in range(2):
        left = jnp.concatenate(
            [jnp.where(own[h], alpha_mid, 0.0), jnp.where(own[h], recept_mid, 0.0)], axis=0
        )
        pairs = dot3(left, right, NT)
        power.append(jnp.where(strict, pairs[:LENGTH, :LENGTH], 0.0))
        alpha_keys = jnp.where(strict, pairs[:LENGTH, LENGTH:], 0.0)
        recept_pairs.append(jnp.where(inclusive_twice, pairs[LENGTH:], 0.0))
        value_rows.append(jnp.where(own[h], 0.0, turned_values))
        solved.append(jnp.where(own[h], start_alpha, dot3(alpha_keys, value_rows[h])))
    for step in range(5):
        solved = [solved[h] + dot3(power[h], solved[h]) for h in range(2)]
        if step < 4:
            power = [dot3(power[h], power[h]) for h in range(2)]
    for h in range(2):
        known = jnp.concatenate([solved[h], value_rows[h]], axis=0)
        query.append(jnp.where(own[h], start_recept, 0.0) + dot3(recept_pairs[h], known))
    steps = [[], []]
    whole = jnp.where(diagonal, 1.0, 0.0)
    for b in range(BLOCKS):
        rows = slice(b * BLOCK, b * BLOCK + BLOCK)
        ends = jnp.concatenate([end_beta[rows], end_keys[rows]], axis=0)
        held = jnp.where(diagonal, jnp.broadcast_to(kept[b : b + 1], (128, 128)), 0.0)
        for h in range(2):
            known = jnp.concatenate([solved[h][rows], value_rows[h][rows]], axis=0)
            steps[h].append(jnp.where(own_row[h], dot3(ends, known, TN) + held, whole))
    one = [dot3(steps[h][1], steps[h][0]) for h in range(2)]
    two = [dot3(steps[h][3], steps[h][2]) for h in range(2)]
    three = [dot3(steps[h][5], steps[h][4]) for h in range(2)]
    four = [dot3(two[h], one[h]) for h in range(2)]
    finals = [dot3(three[h], four[h])[h * HEAD : h * HEAD + HEAD] for h in range(2)]
    finals[1] = pltpu.roll(finals[1], HEAD, 1)
    mine_ref[...] = jnp.where(core == 0, finals[0], finals[1])
    theirs_ref[...] = jnp.where(core == 0, finals[1], finals[0])
    for h in range(2):
        prefixes = [
            None,
            steps[h][0],
            one[h],
            dot3(steps[h][2], one[h]),
            four[h],
            dot3(steps[h][4], four[h]),
        ]
        reads_ref[h, 0:BLOCK, :] = query[h][0:BLOCK]
        for b in range(1, BLOCKS):
            rows = slice(b * BLOCK, b * BLOCK + BLOCK)
            reads_ref[h, rows, :] = dot3(query[h][rows], prefixes[b])


WEIGHTS = (MATS // 2, 1024, 256)


def after(later, earlier):
    product = dot3(later[:, :HEAD], earlier)
    return product + jnp.where(iota((HEAD, 128), 1) < HEAD, 0.0, later)


def chained(steps):
    while len(steps) > 1:
        steps = [after(steps[k + 1], steps[k]) for k in range(0, len(steps), 2)]
    return steps[0]


def nothing():
    return jnp.where(iota((HEAD, 128), 0) == iota((HEAD, 128), 1), 1.0, 0.0)


def sent(step):
    return jnp.broadcast_to((step - nothing()).astype(BF16)[None], (8, HEAD, 128))


def received(steps_ref):
    return [steps_ref[k].astype(F32) + nothing() for k in range(8)]


def chip_kernel(core_ref, mine_ref, theirs_ref, out_ref):
    core = core_ref[0] % 2
    mine, theirs = mine_ref[...], theirs_ref[...]
    earlier = jnp.where(core == 0, mine, theirs)
    later = jnp.where(core == 0, theirs, mine)
    out_ref[...] = sent(after(later, earlier))


def row_kernel(place_ref, steps_ref, before_ref, total_ref):
    here = (place_ref[0] // 2) % 8
    steps = received(steps_ref)
    total_ref[...] = sent(chained(steps))
    before_ref[...] = chained([jnp.where(k < here, steps[k], nothing()) for k in range(8)])


def incoming_kernel(place_ref, steps_ref, before_ref, mine_ref, theirs_ref, own_ref, sent_ref):
    here, core = place_ref[0] // 16, place_ref[0] % 2
    steps = received(steps_ref)
    start = chained([jnp.where(k < here, steps[k], nothing()) for k in range(8)])
    at_chip = after(before_ref[...], start)
    earlier = jnp.where(core == 0, mine_ref[...], theirs_ref[...])
    at_second = after(earlier, at_chip)
    own_ref[...] = jnp.where(core == 0, at_chip, at_second)
    sent_ref[...] = jnp.where(core == 0, at_second, at_chip)


def conv_kernel(place_ref, input_ref, rim_ref, table_ref, filtered_ref, sums_ref):
    padded = jnp.concatenate([rim_ref[...], input_ref[...]], axis=0).astype(F32)
    filtered = jnp.broadcast_to(table_ref[5:6, :], (LENGTH, 128))
    for k in range(TAPS):
        filtered = filtered + table_ref[8 + k : 9 + k, :] * padded[k + 2 : k + 2 + LENGTH]
    filtered_ref[...] = filtered
    ones = jnp.ones((8, 128), F32)
    square = filtered * filtered
    rest = jnp.concatenate([filtered[128:], square[128:]], axis=0)
    at = iota((8, 128), 0)
    sums = jnp.where(at == 0, exact(ones, filtered[:128], NT), 0.0)
    sums = jnp.where(at == 1, exact(ones, square[:128], NT), sums)
    sums_ref[...] = jnp.where(at == 2, exact(ones, rest, NT), sums)


def columns_kernel(core_ref, *refs):
    index, out_ref = core_ref[0], refs[-1]
    core = index % 2

    def store(row, piece, b):
        for m in range(2):
            at = (MATS + m) * 16
            out_ref[pl.ds(row, 16), m * 128 : m * 128 + 128] = piece[b, at : at + 16, :]

    height = lambda z, y, c: place(z, y, c) * 16
    fill_rows(index, core, refs[:4], height, store)
    fill_rows(index, 1 - core, refs[4:8], height, store)


def final_kernel(
    core_ref,
    reads_ref,
    mine_ref,
    theirs_ref,
    gate_ref,
    filtered_ref,
    sums_ref,
    columns_ref,
    table_ref,
    out_ref,
):
    core = core_ref[0] % 2
    mine, theirs = mine_ref[...], theirs_ref[...]
    head0 = jnp.where(core == 0, mine, theirs)
    head1 = jnp.where(core == 0, theirs, mine)
    lane = iota((HEAD, 128), 1)
    equal = iota((HEAD, 128), 0)
    zero = jnp.zeros((HEAD, 128), F32)
    right0 = jnp.concatenate(
        [
            jnp.where(lane < HEAD, pltpu.roll(head0, HEAD, 1), zero),
            jnp.where(lane == equal, 1.0, 0.0),
        ],
        axis=0,
    )
    right1 = jnp.concatenate(
        [jnp.where(lane == equal + HEAD, 1.0, 0.0), jnp.where(lane < HEAD, zero, head1)], axis=0
    )
    reads = exact(reads_ref[0], right0) + exact(reads_ref[1], right1)
    first = iota((LENGTH, 128), 1) < HEAD

    def head_mean(x):
        low = jnp.sum(jnp.where(first, x, 0.0), axis=-1, keepdims=True)
        high = jnp.sum(jnp.where(first, 0.0, x), axis=-1, keepdims=True)
        return jnp.where(first, low, high) * (1.0 / HEAD)

    centered = reads - head_mean(reads)
    spread = head_mean(centered * centered)
    scan_out = (centered * lax.rsqrt(spread + 0.00064) * gate_ref[...]).astype(BF16)

    def spread_out(k):
        return exact(sums_ref[...], jnp.where(iota((8, 128), 0) == k, 1.0 / 512.0, 0.0), TN)

    rest = spread_out(2)
    center = jnp.concatenate([spread_out(0), rest[:64]], axis=0)
    second = jnp.concatenate([spread_out(1), rest[64:]], axis=0)
    scaled = (
        (filtered_ref[...] - center)
        * lax.rsqrt(second - center * center + 1e-05)
        * table_ref[6:7, :]
    )
    conv_out = (scaled * jax.nn.sigmoid(scaled)).astype(BF16)
    features = jnp.concatenate([scan_out, conv_out], axis=1)
    for j in range(4):
        out_ref[j] = lax.dot_general(
            features, columns_ref[j * 512 : j * 512 + 512, :], NT, preferred_element_type=F32
        ).astype(BF16)


def to_each(x, groups):
    return lax.all_to_all(x, "sp", 0, 0, tiled=True, axis_index_groups=groups)


def layer(
    tokens,
    norm_gain,
    query_weight,
    key_weight,
    value_weight,
    decay_weight,
    removal_weight,
    gate_weight,
    key_gain,
    removal_gain,
    removal_bias,
    decay_bias,
    decay_extra,
    scan_norm_gain,
    conv_value_weight,
    conv_gate_weight,
    conv_taps,
    conv_bias,
    conv_norm_gain,
    out_scan_weight,
    out_conv_weight,
):
    index = jnp.stack([lax.axis_index("sp"), lax.axis_index("tp")]).astype(jnp.int32)
    row = lambda v: v.reshape(1, -1)

    packed = pack(
        query_weight,
        key_weight,
        value_weight,
        decay_weight,
        removal_weight,
        gate_weight,
        conv_value_weight,
        conv_gate_weight,
        out_scan_weight.T,
        out_conv_weight.T,
    )
    line = to_each(packed, FAR_FIRST)
    around = [tokens]
    for k in range(1, 4):
        around.append(lax.ppermute(tokens, "tp", [(x, (x + k) % 4) for x in range(4)]))
    plane = to_each(jnp.broadcast_to(line[None], (4, *line.shape)), FAR_SECOND)
    pieces = [plane.reshape(16, *plane.shape[2:])]
    for along_z, along_y in FLIPS[1:]:
        pieces.append(lax.ppermute(pieces[0], "sp", neighbours(along_z, along_y)))
    swapped = []
    for piece in pieces:
        swapped.append(lax.ppermute(piece, "sp", SWAP))
    normed, table, extra = on_core(
        norm_kernel,
        (vmem((2, 8, LENGTH, 128), BF16), vmem((40, 128), F32), vmem((LENGTH, 128), F32)),
        index,
        *around,
        given=(
            norm_gain.reshape(4, 512),
            row(key_gain),
            row(removal_gain),
            row(removal_bias),
            row(decay_bias),
            row(scan_norm_gain),
            row(conv_bias),
            row(conv_norm_gain),
            conv_taps,
            decay_extra,
        ),
    )
    half = on_core(
        half_kernel,
        vmem((MATS // 2, LENGTH, 256), F32),
        index,
        *pieces,
        normed,
        scratch=[pltpu.VMEM(WEIGHTS, BF16)],
        limit=16,
    )
    mine, theirs, reads, gate, conv_input, rim = on_core(
        local_kernel,
        (
            vmem((HEAD, 128), F32),
            vmem((HEAD, 128), F32),
            vmem((2, LENGTH, 128), F32),
            vmem((LENGTH, 128), F32),
            vmem((LENGTH, 128), BF16),
            vmem((32, 128), BF16),
        ),
        index,
        *swapped,
        normed,
        half,
        table,
        extra,
        scratch=[pltpu.VMEM(WEIGHTS, BF16)],
        limit=28,
    )

    theirs = lax.ppermute(theirs, "sp", SWAP)
    rim = lax.ppermute(rim, "sp", ONWARD)
    message = vmem((8, HEAD, 128), BF16)
    step = vmem((HEAD, 128), F32)
    chip = on_core(chip_kernel, message, index, mine, theirs)
    chips = to_each(chip, Y_AXIS)
    before, total = on_core(row_kernel, (step, message), index, chips)
    totals = to_each(total, Z_AXIS)
    own_state, sent_state = on_core(
        incoming_kernel, (step, step), index, totals, before, mine, theirs
    )
    other_state = lax.ppermute(sent_state, "sp", SWAP)

    filtered, sums = on_core(
        conv_kernel, (vmem((LENGTH, 128), F32), vmem((8, 128), F32)), index, conv_input, rim, table
    )
    sums = lax.psum(sums, "tp")
    columns = on_core(columns_kernel, vmem((2048, 256), BF16), index, *pieces, *swapped)

    terms = on_core(
        final_kernel,
        vmem((4, LENGTH, 512), BF16),
        index,
        reads,
        own_state,
        other_state,
        gate,
        filtered,
        sums,
        columns,
        table,
    )
    parts = lax.all_to_all(terms, "tp", 0, 0, tiled=True)
    return jnp.sum(parts.astype(F32), axis=0).astype(BF16)


def solution(mesh):
    weights = P("sp", "tp")
    in_specs = (
        (P("sp", "tp"), P())
        + (weights,) * 6
        + (P("tp"),) * 4
        + (P("sp", "tp"), P("tp"), weights, weights, P(None, "tp"), P("tp"), P("tp"))
        + (P("tp", "sp"), P("tp", "sp"))
    )
    return jax.shard_map(
        layer, mesh=mesh, in_specs=in_specs, out_specs=P("sp", "tp"), check_vma=False
    )
```

```python
import functools

import jax
import jax.numpy as jnp
from jax import lax
from jax.experimental import pallas as pl
from jax.experimental.pallas import tpu as pltpu
from jax.sharding import PartitionSpec as P

HEAD = 64
TAPS = 31
BLOCK = 32
LENGTH = 192
BLOCKS = LENGTH // BLOCK
MATS = 8
F32 = jnp.float32
BF16 = jnp.bfloat16

NN = (((1,), (0,)), ((), ()))
NT = (((1,), (1,)), ((), ()))
TN = (((0,), (0,)), ((), ()))


def place(z, y, c):
    return z * 16 + y * 2 + c


SETS = (((0, 2, 5, 7), (1, 3, 4, 6)), ((1, 3, 6, 0), (2, 4, 5, 7)))
FAR_Y = [[[place(z, y, c) for y in ys] for z in range(8) for ys in SETS[c]] for c in range(2)]
FAR_Z = [[[place(z, y, c) for z in zs] for y in range(8) for zs in SETS[c]] for c in range(2)]
FAR_FIRST = FAR_Y[0] + FAR_Z[1]
FAR_SECOND = FAR_Z[0] + FAR_Y[1]


def near(k, p, c):
    pair = ((2 * k + c) % 8, (2 * k + c + 1) % 8)
    return [chip for chip in pair if chip in SETS[c][p]][0]


NEAR = [
    [place(near(k, p, c), near(l, q, c), c) for p in range(2) for q in range(2)]
    for c in range(2)
    for k in range(4)
    for l in range(4)
]
Y_AXIS = [[place(z, y, c) for y in range(8)] for z in range(8) for c in range(2)]
Z_AXIS = [[place(z, y, c) for z in range(8)] for y in range(8) for c in range(2)]
SWAP = [(i, i ^ 1) for i in range(128)]
ONWARD = [(i, i + 1) for i in range(127)]


def split(x):
    high = x.astype(BF16)
    return high, (x - high.astype(F32)).astype(BF16)


def dot3(a, b, dims=NN):
    a_high, a_low = split(a)
    b_high, b_low = split(b)
    one = functools.partial(lax.dot_general, dimension_numbers=dims, preferred_element_type=F32)
    return one(a_high, b_high) + (one(a_high, b_low) + one(a_low, b_high))


def exact(a, b, dims=NN):
    return lax.dot_general(
        a, b, dims, precision=lax.Precision.HIGHEST, preferred_element_type=F32
    )


def sums_of(ones, x):
    high = x.astype(BF16)
    middle, low = split(x - high.astype(F32))
    one = lambda part: jnp.dot(ones, part, preferred_element_type=F32)
    return one(high) + (one(middle) + one(low))


def iota(shape, dim):
    return lax.broadcasted_iota(jnp.int32, shape, dim)


def vmem(shape, dtype):
    return pltpu.VMEM(shape, dtype)


def on_core(kernel, shapes, index, *operands, given=(), scratch=(), limit=8):
    return pl.pallas_call(
        kernel,
        in_specs=[pl.BlockSpec(memory_space=pltpu.SMEM)]
        + [pl.BlockSpec(memory_space=pltpu.VMEM)] * (len(operands) + len(given)),
        out_shape=shapes,
        scratch_shapes=scratch,
        compiler_params=pltpu.CompilerParams(vmem_limit_bytes=limit * 1024 * 1024),
    )(index, *(pltpu.with_memory_space_constraint(x, pltpu.VMEM) for x in operands), *given)


def pack_kernel(*refs):
    out = refs[-1]
    blocks = [ref[...] for ref in refs[:-1]]
    both = jnp.concatenate(blocks, axis=0)
    for k in range(4):
        out[k] = both


def pack(*mats):
    return pl.pallas_call(
        pack_kernel,
        out_shape=jax.ShapeDtypeStruct((4, 16 * len(mats), 128), BF16),
        name="pack",
    )(*mats)


def fill_rows(core, source, height, store):
    for a in range(4):
        for b in range(16):
            i, j = b // 4, b % 4
            row0 = height(SETS[0][a // 2][i], SETS[0][a % 2][j], 0)
            row1 = height(SETS[1][a // 2][j], SETS[1][a % 2][i], 1)
            store(pl.multiple_of(jnp.where(core == 0, row0, row1), 16), source, a, b)


def table_kernel(place_ref, *refs):
    vectors, taps_ref, extra_ref, table_ref, extra_out_ref = refs[:-4], *refs[-4:]
    for k, ref in enumerate(vectors):
        table_ref[k : k + 1, :] = ref[...]
    table_ref[8 : 8 + TAPS, :] = taps_ref[...]
    extra_out_ref[...] = extra_ref[...]


def norm_kernel(place_ref, tokens_ref, gain_ref, normed_ref):
    parts = [tokens_ref[j].astype(F32) for j in range(4)]
    total = sum(jnp.sum(part * part, axis=-1, keepdims=True) for part in parts)
    inverse_rms = lax.rsqrt(total * (1.0 / 2048.0) + 1e-06)
    goal = iota((256, 256), 1)
    source = ((goal % 128) // 16) * 32 + (goal // 128) * 16 + goal % 16
    moves = jnp.where(iota((256, 256), 0) == source, 1.0, 0.0).astype(BF16)
    for j in range(4):
        normed = (parts[j] * inverse_rms * gain_ref[j : j + 1, :]).astype(BF16)
        for k in range(2):
            moved = jnp.dot(
                normed[:, k * 256 : k * 256 + 256], moves, preferred_element_type=F32
            ).astype(BF16)
            z = j * 2 + k
            normed_ref[0, :, z * 128 : z * 128 + 128] = moved[:, :128]
            normed_ref[1, :, z * 128 : z * 128 + 128] = moved[:, 128:]


def projected(core, source_ref, normed_ref, weights):
    def store(row, source, a, b):
        for m in range(MATS):
            lanes = slice((m % 2) * 128, (m % 2) * 128 + 128)
            weights[m // 2, pl.ds(row, 16), lanes] = source[a, b, m * 16 : m * 16 + 16, :]

    fill_rows(core, source_ref, lambda z, y, c: (z * 8 + y) * 16, store)
    normed = normed_ref[core]
    return [jnp.dot(normed, weights[p], preferred_element_type=F32) for p in range(MATS // 2)]


def half_kernel(place_ref, own_ref, normed_ref, out_ref, rest_ref, weights):
    rest_ref[...] = own_ref[:, :, MATS * 16 :, :]
    products = projected(place_ref[0] % 2, own_ref, normed_ref, weights)
    for p in range(MATS // 2):
        out_ref[p] = products[p]


def local_kernel(
    core_ref,
    other_ref,
    normed_ref,
    half_ref,
    table_ref,
    extra_ref,
    mine_ref,
    theirs_ref,
    reads_ref,
    gate_ref,
    conv_ref,
    rim_ref,
    rest_ref,
    weights,
):
    core = core_ref[0] % 2
    rest_ref[...] = other_ref[:, :, MATS * 16 :, :]
    products = []
    for p, product in enumerate(projected(1 - core, other_ref, normed_ref, weights)):
        product = (product + half_ref[p]).astype(BF16).astype(F32)
        products += [product[:, :128], product[:, 128:]]
    recept, keys, values, decay_pre, removal_pre, gate_pre, conv_value, conv_gate = products
    key_gain, removal_gain, removal_bias, decay_bias, norm_out = (
        table_ref[k : k + 1, :] for k in range(5)
    )
    gate_ref[...] = norm_out * jax.nn.sigmoid(gate_pre)
    conv_input = (conv_value * jax.nn.sigmoid(conv_gate)).astype(BF16)
    conv_ref[...] = conv_input
    rim_ref[...] = conv_input[LENGTH - 32 :]

    rate = 0.6065306597126334 * jax.nn.sigmoid(decay_bias + decay_pre) + extra_ref[...]
    removal = jax.nn.sigmoid(removal_bias + removal_pre)
    lane = iota((LENGTH, 128), 1)
    first = lane < HEAD
    scaled = keys * key_gain
    square = scaled * scaled
    low = jnp.sum(jnp.where(first, square, 0.0), axis=-1, keepdims=True)
    high = jnp.sum(jnp.where(first, 0.0, square), axis=-1, keepdims=True)
    unit = scaled * lax.rsqrt(jnp.where(first, low, high) + 1e-06)
    written = keys * (1.0 + (removal - 1.0) * removal_gain)

    row, column = iota((LENGTH, LENGTH), 0), iota((LENGTH, LENGTH), 1)
    same = (row // BLOCK) == (column // BLOCK)
    strict = same & (row > column)
    inclusive = same & (row >= column)
    wide_row, wide_column = iota((LENGTH, 2 * LENGTH), 0), iota((LENGTH, 2 * LENGTH), 1)
    wide_column = jnp.where(wide_column >= LENGTH, wide_column - LENGTH, wide_column)
    inclusive_twice = ((wide_row // BLOCK) == (wide_column // BLOCK)) & (wide_row >= wide_column)
    falling = -sums_of(jnp.where(inclusive, 1.0, 0.0).astype(BF16), rate)
    before = falling + rate
    by_block = falling.reshape(BLOCKS, BLOCK, 128)
    middle = jnp.broadcast_to(
        by_block[:, BLOCK // 2 : BLOCK // 2 + 1], (BLOCKS, BLOCK, 128)
    ).reshape(LENGTH, 128)
    ending = jnp.broadcast_to(by_block[:, BLOCK - 1 :], (BLOCKS, BLOCK, 128)).reshape(LENGTH, 128)
    beta = unit * removal
    rising = jnp.exp(middle - falling)
    alpha_mid = -unit * jnp.exp(before - middle)
    recept_mid = recept * jnp.exp(falling - middle)
    right = jnp.concatenate([beta * rising, written * rising], axis=0)
    start_alpha = -unit * jnp.exp(before)
    start_recept = recept * jnp.exp(falling)
    closing = jnp.exp(ending - falling)
    end_beta = beta * closing
    end_keys = written * closing
    kept = jnp.exp(by_block[:, BLOCK - 1, :])
    turned_values = pltpu.roll(values, HEAD, 1)

    square_row, square_lane = iota((128, 128), 0), iota((128, 128), 1)
    diagonal = square_row == square_lane
    own = [first, jnp.logical_not(first)]
    own_row = [square_row < HEAD, square_row >= HEAD]
    power, solved, query, value_rows = [], [], [], []
    recept_pairs = []
    for h in range(2):
        left = jnp.concatenate(
            [jnp.where(own[h], alpha_mid, 0.0), jnp.where(own[h], recept_mid, 0.0)], axis=0
        )
        pairs = dot3(left, right, NT)
        power.append(jnp.where(strict, pairs[:LENGTH, :LENGTH], 0.0))
        alpha_keys = jnp.where(strict, pairs[:LENGTH, LENGTH:], 0.0)
        recept_pairs.append(jnp.where(inclusive_twice, pairs[LENGTH:], 0.0))
        value_rows.append(jnp.where(own[h], 0.0, turned_values))
        solved.append(jnp.where(own[h], start_alpha, dot3(alpha_keys, value_rows[h])))
    for step in range(5):
        solved = [solved[h] + dot3(power[h], solved[h]) for h in range(2)]
        if step < 4:
            power = [dot3(power[h], power[h]) for h in range(2)]
    for h in range(2):
        known = jnp.concatenate([solved[h], value_rows[h]], axis=0)
        query.append(jnp.where(own[h], start_recept, 0.0) + dot3(recept_pairs[h], known))
    steps = [[], []]
    whole = jnp.where(diagonal, 1.0, 0.0)
    for b in range(BLOCKS):
        rows = slice(b * BLOCK, b * BLOCK + BLOCK)
        ends = jnp.concatenate([end_beta[rows], end_keys[rows]], axis=0)
        held = jnp.where(diagonal, jnp.broadcast_to(kept[b : b + 1], (128, 128)), 0.0)
        for h in range(2):
            known = jnp.concatenate([solved[h][rows], value_rows[h][rows]], axis=0)
            steps[h].append(jnp.where(own_row[h], dot3(ends, known, TN) + held, whole))
    one = [dot3(steps[h][1], steps[h][0]) for h in range(2)]
    two = [dot3(steps[h][3], steps[h][2]) for h in range(2)]
    three = [dot3(steps[h][5], steps[h][4]) for h in range(2)]
    four = [dot3(two[h], one[h]) for h in range(2)]
    finals = [dot3(three[h], four[h])[h * HEAD : h * HEAD + HEAD] for h in range(2)]
    finals[1] = pltpu.roll(finals[1], HEAD, 1)
    mine_ref[...] = jnp.where(core == 0, finals[0], finals[1])
    theirs_ref[...] = jnp.where(core == 0, finals[1], finals[0])
    for h in range(2):
        prefixes = [
            None,
            steps[h][0],
            one[h],
            dot3(steps[h][2], one[h]),
            four[h],
            dot3(steps[h][4], four[h]),
        ]
        reads_ref[h, 0:BLOCK, :] = query[h][0:BLOCK]
        for b in range(1, BLOCKS):
            rows = slice(b * BLOCK, b * BLOCK + BLOCK)
            reads_ref[h, rows, :] = dot3(query[h][rows], prefixes[b])


WEIGHTS = (MATS // 2, 1024, 256)


def after(later, earlier):
    product = dot3(later[:, :HEAD], earlier)
    return product + jnp.where(iota((HEAD, 128), 1) < HEAD, 0.0, later)


def chained(steps):
    while len(steps) > 1:
        steps = [after(steps[k + 1], steps[k]) for k in range(0, len(steps), 2)]
    return steps[0]


def nothing():
    return jnp.where(iota((HEAD, 128), 0) == iota((HEAD, 128), 1), 1.0, 0.0)


def sent(step):
    return jnp.broadcast_to((step - nothing()).astype(BF16)[None], (8, HEAD, 128))


def received(steps_ref):
    return [steps_ref[k].astype(F32) + nothing() for k in range(8)]


def chip_kernel(core_ref, mine_ref, theirs_ref, out_ref):
    core = core_ref[0] % 2
    mine, theirs = mine_ref[...], theirs_ref[...]
    earlier = jnp.where(core == 0, mine, theirs)
    later = jnp.where(core == 0, theirs, mine)
    out_ref[...] = sent(after(later, earlier))


def row_kernel(place_ref, steps_ref, before_ref, total_ref):
    here = (place_ref[0] // 2) % 8
    steps = received(steps_ref)
    total_ref[...] = sent(chained(steps))
    before_ref[...] = chained([jnp.where(k < here, steps[k], nothing()) for k in range(8)])


def incoming_kernel(place_ref, steps_ref, before_ref, mine_ref, theirs_ref, own_ref, sent_ref):
    here, core = place_ref[0] // 16, place_ref[0] % 2
    steps = received(steps_ref)
    start = chained([jnp.where(k < here, steps[k], nothing()) for k in range(8)])
    at_chip = after(before_ref[...], start)
    earlier = jnp.where(core == 0, mine_ref[...], theirs_ref[...])
    at_second = after(earlier, at_chip)
    own_ref[...] = jnp.where(core == 0, at_chip, at_second)
    sent_ref[...] = jnp.where(core == 0, at_second, at_chip)


def conv_kernel(place_ref, input_ref, rim_ref, table_ref, filtered_ref, sums_ref):
    padded = jnp.concatenate([rim_ref[...], input_ref[...]], axis=0).astype(F32)
    filtered = jnp.broadcast_to(table_ref[5:6, :], (LENGTH, 128))
    for k in range(TAPS):
        filtered = filtered + table_ref[8 + k : 9 + k, :] * padded[k + 2 : k + 2 + LENGTH]
    filtered_ref[...] = filtered
    ones = jnp.ones((8, 128), F32)
    square = filtered * filtered
    rest = jnp.concatenate([filtered[128:], square[128:]], axis=0)
    at = iota((8, 128), 0)
    sums = jnp.where(at == 0, exact(ones, filtered[:128], NT), 0.0)
    sums = jnp.where(at == 1, exact(ones, square[:128], NT), sums)
    sums_ref[...] = jnp.where(at == 2, exact(ones, rest, NT), sums)


def fill_columns(core, own_ref, other_ref, columns):
    def store(row, source, a, b):
        for m in range(2):
            columns[pl.ds(row, 16), m * 128 : m * 128 + 128] = source[a, b, m * 16 : m * 16 + 16, :]

    height = lambda z, y, c: place(z, y, c) * 16
    fill_rows(core, own_ref, height, store)
    fill_rows(1 - core, other_ref, height, store)


def product(features, columns):
    return lax.dot_general(features, columns, NT, preferred_element_type=F32)


def final_kernel(
    core_ref,
    reads_ref,
    mine_ref,
    theirs_ref,
    gate_ref,
    filtered_ref,
    sums_ref,
    own_ref,
    other_ref,
    table_ref,
    out_ref,
    features_ref,
    kept_ref,
    columns,
):
    core = core_ref[0] % 2
    mine, theirs = mine_ref[...], theirs_ref[...]
    head0 = jnp.where(core == 0, mine, theirs)
    head1 = jnp.where(core == 0, theirs, mine)
    lane = iota((HEAD, 128), 1)
    equal = iota((HEAD, 128), 0)
    zero = jnp.zeros((HEAD, 128), F32)
    right0 = jnp.concatenate(
        [
            jnp.where(lane < HEAD, pltpu.roll(head0, HEAD, 1), zero),
            jnp.where(lane == equal, 1.0, 0.0),
        ],
        axis=0,
    )
    right1 = jnp.concatenate(
        [jnp.where(lane == equal + HEAD, 1.0, 0.0), jnp.where(lane < HEAD, zero, head1)], axis=0
    )
    reads = exact(reads_ref[0], right0) + exact(reads_ref[1], right1)
    first = iota((LENGTH, 128), 1) < HEAD

    def head_mean(x):
        low = jnp.sum(jnp.where(first, x, 0.0), axis=-1, keepdims=True)
        high = jnp.sum(jnp.where(first, 0.0, x), axis=-1, keepdims=True)
        return jnp.where(first, low, high) * (1.0 / HEAD)

    centered = reads - head_mean(reads)
    spread = head_mean(centered * centered)
    scan_out = (centered * lax.rsqrt(spread + 0.00064) * gate_ref[...]).astype(BF16)

    def spread_out(k):
        return exact(sums_ref[...], jnp.where(iota((8, 128), 0) == k, 1.0 / 512.0, 0.0), TN)

    rest = spread_out(2)
    center = jnp.concatenate([spread_out(0), rest[:64]], axis=0)
    second = jnp.concatenate([spread_out(1), rest[64:]], axis=0)
    scaled = (
        (filtered_ref[...] - center)
        * lax.rsqrt(second - center * center + 1e-05)
        * table_ref[6:7, :]
    )
    conv_out = (scaled * jax.nn.sigmoid(scaled)).astype(BF16)
    features = jnp.concatenate([scan_out, conv_out], axis=1)
    features_ref[...] = features
    fill_columns(core, own_ref, other_ref, columns)
    for j in range(4):
        out_ref[j] = product(features, columns[j * 512 : j * 512 + 512, :]).astype(BF16)
    kept_ref[...] = columns[pl.ds(pl.multiple_of(core_ref[1] * 512, 512), 512), :]


def stay_kernel(place_ref, features_ref, columns_ref, out_ref):
    out_ref[...] = product(features_ref[...], columns_ref[...])


def add_kernel(place_ref, parts_ref, stay_ref, out_ref):
    total = stay_ref[...]
    for j in range(4):
        total = total + jnp.where(place_ref[1] == j, 0.0, parts_ref[j].astype(F32))
    out_ref[...] = total.astype(BF16)


def to_each(x, groups):
    return lax.all_to_all(x, "sp", 0, 0, tiled=True, axis_index_groups=groups)


def layer(
    tokens,
    norm_gain,
    query_weight,
    key_weight,
    value_weight,
    decay_weight,
    removal_weight,
    gate_weight,
    key_gain,
    removal_gain,
    removal_bias,
    decay_bias,
    decay_extra,
    scan_norm_gain,
    conv_value_weight,
    conv_gate_weight,
    conv_taps,
    conv_bias,
    conv_norm_gain,
    out_scan_weight,
    out_conv_weight,
):
    index = jnp.stack([lax.axis_index("sp"), lax.axis_index("tp")]).astype(jnp.int32)
    row = lambda v: v.reshape(1, -1)

    packed = pack(
        query_weight,
        key_weight,
        value_weight,
        decay_weight,
        removal_weight,
        gate_weight,
        conv_value_weight,
        conv_gate_weight,
        out_scan_weight.T,
        out_conv_weight.T,
    )
    line = to_each(packed, FAR_FIRST)
    wide = jnp.broadcast_to(line[None], (4, *line.shape))
    plane = to_each(wide, FAR_SECOND)
    table, extra = on_core(
        table_kernel,
        (vmem((40, 128), F32), vmem((LENGTH, 128), F32)),
        index,
        given=(
            row(key_gain),
            row(removal_gain),
            row(removal_bias),
            row(decay_bias),
            row(scan_norm_gain),
            row(conv_bias),
            row(conv_norm_gain),
            conv_taps,
            decay_extra,
        ),
    )
    wide = jnp.broadcast_to(plane[None], (4, *plane.shape))
    stage2 = to_each(wide, NEAR).reshape(4, 16, *plane.shape[2:])
    whole = lax.all_gather(tokens, "tp")
    normed = on_core(
        norm_kernel, vmem((2, LENGTH, 1024), BF16), index, whole, given=(norm_gain.reshape(4, 512),)
    )
    swapped = lax.ppermute(stage2, "sp", SWAP)
    half, rest = on_core(
        half_kernel,
        (vmem((MATS // 2, LENGTH, 256), F32), vmem((4, 16, 32, 128), BF16)),
        index,
        stage2,
        normed,
        scratch=[pltpu.VMEM(WEIGHTS, BF16)],
        limit=16,
    )
    mine, theirs, reads, gate, conv_input, rim, other_rest = on_core(
        local_kernel,
        (
            vmem((HEAD, 128), F32),
            vmem((HEAD, 128), F32),
            vmem((2, LENGTH, 128), F32),
            vmem((LENGTH, 128), F32),
            vmem((LENGTH, 128), BF16),
            vmem((32, 128), BF16),
            vmem((4, 16, 32, 128), BF16),
        ),
        index,
        swapped,
        normed,
        half,
        table,
        extra,
        scratch=[pltpu.VMEM(WEIGHTS, BF16)],
        limit=28,
    )

    theirs = lax.ppermute(theirs, "sp", SWAP)
    rim = lax.ppermute(rim, "sp", ONWARD)
    message = vmem((8, HEAD, 128), BF16)
    step = vmem((HEAD, 128), F32)
    chip = on_core(chip_kernel, message, index, mine, theirs)
    chips = to_each(chip, Y_AXIS)
    before, total = on_core(row_kernel, (step, message), index, chips)
    totals = to_each(total, Z_AXIS)
    own_state, sent_state = on_core(
        incoming_kernel, (step, step), index, totals, before, mine, theirs
    )
    other_state = lax.ppermute(sent_state, "sp", SWAP)

    filtered, sums = on_core(
        conv_kernel, (vmem((LENGTH, 128), F32), vmem((8, 128), F32)), index, conv_input, rim, table
    )
    sums = lax.psum(sums, "tp")

    terms, features, kept = on_core(
        final_kernel,
        (vmem((4, LENGTH, 512), BF16), vmem((LENGTH, 256), BF16), vmem((512, 256), BF16)),
        index,
        reads,
        own_state,
        other_state,
        gate,
        filtered,
        sums,
        rest,
        other_rest,
        table,
        scratch=[pltpu.VMEM((2048, 256), BF16)],
        limit=12,
    )
    parts = lax.all_to_all(terms, "tp", 0, 0, tiled=True)
    stay = on_core(stay_kernel, vmem((LENGTH, 512), F32), index, features, kept)
    return on_core(add_kernel, jax.ShapeDtypeStruct((LENGTH, 512), BF16), index, parts, stay)


def solution(mesh):
    weights = P("sp", "tp")
    in_specs = (
        (P("sp", "tp"), P())
        + (weights,) * 6
        + (P("tp"),) * 4
        + (P("sp", "tp"), P("tp"), weights, weights, P(None, "tp"), P("tp"), P("tp"))
        + (P("tp", "sp"), P("tp", "sp"))
    )
    return jax.shard_map(
        layer, mesh=mesh, in_specs=in_specs, out_specs=P("sp", "tp"), check_vma=False
    )
```

```python
import functools

import jax
import jax.numpy as jnp
from jax import lax
from jax.experimental import pallas as pl
from jax.experimental.pallas import tpu as pltpu
from jax.sharding import PartitionSpec as P

HEAD = 64
TAPS = 31
BLOCK = 32
LENGTH = 192
BLOCKS = LENGTH // BLOCK
MATS = 8
F32 = jnp.float32
BF16 = jnp.bfloat16

NN = (((1,), (0,)), ((), ()))
NT = (((1,), (1,)), ((), ()))
TN = (((0,), (0,)), ((), ()))


def place(z, y, c):
    return z * 16 + y * 2 + c


SETS = (((0, 2, 5, 7), (1, 3, 4, 6)), ((1, 3, 6, 0), (2, 4, 5, 7)))
FAR = [
    [place(z, y, c) for z in SETS[c][p] for y in SETS[c][q]]
    for c in range(2)
    for p in range(2)
    for q in range(2)
]


def partner(v, c):
    return v ^ 1 if c == 0 else (((v - 1) % 8 ^ 1) + 1) % 8


def neighbours(along_z, along_y):
    return [
        (place(z, y, c), place(partner(z, c) if along_z else z, partner(y, c) if along_y else y, c))
        for z in range(8)
        for y in range(8)
        for c in range(2)
    ]


Y_AXIS = [[place(z, y, c) for y in range(8)] for z in range(8) for c in range(2)]
Z_AXIS = [[place(z, y, c) for z in range(8)] for y in range(8) for c in range(2)]
SWAP = [(i, i ^ 1) for i in range(128)]
ONWARD = [(i, i + 1) for i in range(127)]


def split(x):
    high = x.astype(BF16)
    return high, (x - high.astype(F32)).astype(BF16)


def dot3(a, b, dims=NN):
    a_high, a_low = split(a)
    b_high, b_low = split(b)
    one = functools.partial(lax.dot_general, dimension_numbers=dims, preferred_element_type=F32)
    return one(a_high, b_high) + (one(a_high, b_low) + one(a_low, b_high))


def exact(a, b, dims=NN):
    return lax.dot_general(
        a, b, dims, precision=lax.Precision.HIGHEST, preferred_element_type=F32
    )


def sums_of(ones, x):
    high = x.astype(BF16)
    middle, low = split(x - high.astype(F32))
    one = lambda part: jnp.dot(ones, part, preferred_element_type=F32)
    return one(high) + (one(middle) + one(low))


def iota(shape, dim):
    return lax.broadcasted_iota(jnp.int32, shape, dim)


def vmem(shape, dtype):
    return pltpu.VMEM(shape, dtype)


def on_core(kernel, shapes, index, *operands, given=(), scratch=(), limit=8):
    return pl.pallas_call(
        kernel,
        in_specs=[pl.BlockSpec(memory_space=pltpu.SMEM)]
        + [pl.BlockSpec(memory_space=pltpu.VMEM)] * (len(operands) + len(given)),
        out_shape=shapes,
        scratch_shapes=scratch,
        compiler_params=pltpu.CompilerParams(vmem_limit_bytes=limit * 1024 * 1024),
    )(index, *(pltpu.with_memory_space_constraint(x, pltpu.VMEM) for x in operands), *given)


def pack_kernel(*refs):
    out = refs[-1]
    blocks = [ref[...] for ref in refs[:-1]]
    both = jnp.concatenate(blocks, axis=0)
    for k in range(16):
        out[k] = both


def pack(*mats):
    return pl.pallas_call(
        pack_kernel,
        out_shape=jax.ShapeDtypeStruct((16, 16 * len(mats), 128), BF16),
        name="pack",
    )(*mats)


FLIPS = ((0, 0), (0, 1), (1, 0), (1, 1))


def chosen(conditions, values):
    if not conditions:
        return values[0]
    half = len(values) // 2
    low, high = (chosen(conditions[1:], part) for part in (values[:half], values[half:]))
    return low if isinstance(low, int) and low == high else jnp.where(conditions[0], high, low)


def fill_rows(index, core, pieces, height, store):
    second = core == 1

    def axis(position):
        in_set1 = functools.reduce(
            jnp.logical_or,
            [
                jnp.logical_and(second == (c == 1), position == v)
                for c in range(2)
                for v in SETS[c][1]
            ],
        )
        return [
            [
                chosen(
                    (second, in_set1),
                    [SETS[c][p ^ flip][k] for c in range(2) for p in range(2)],
                )
                for k in range(4)
            ]
            for flip in range(2)
        ]

    zs, ys = axis(index // 16), axis((index // 2) % 8)
    for piece, (flip_z, flip_y) in zip(pieces, FLIPS):
        for b in range(16):
            row = height(zs[flip_z][b // 4], ys[flip_y][b % 4], core)
            store(pl.multiple_of(row, 16), piece, b)


def table_kernel(place_ref, *refs):
    vectors, taps_ref, extra_ref, table_ref, extra_out_ref = refs[:-4], *refs[-4:]
    for k, ref in enumerate(vectors):
        table_ref[k : k + 1, :] = ref[...]
    table_ref[8 : 8 + TAPS, :] = taps_ref[...]
    extra_out_ref[...] = extra_ref[...]


def norm_kernel(place_ref, tokens_ref, gain_ref, normed_ref):
    parts = [tokens_ref[j].astype(F32) for j in range(4)]
    total = sum(jnp.sum(part * part, axis=-1, keepdims=True) for part in parts)
    inverse_rms = lax.rsqrt(total * (1.0 / 2048.0) + 1e-06)
    goal = iota((256, 256), 1)
    source = ((goal % 128) // 16) * 32 + (goal // 128) * 16 + goal % 16
    moves = jnp.where(iota((256, 256), 0) == source, 1.0, 0.0).astype(BF16)
    for j, part in enumerate(parts):
        normed = (part * inverse_rms * gain_ref[j : j + 1, :]).astype(BF16)
        for h in range(2):
            moved = jnp.dot(
                normed[:, h * 256 : h * 256 + 256], moves, preferred_element_type=F32
            ).astype(BF16)
            z = j * 2 + h
            normed_ref[0, :, z * 128 : z * 128 + 128] = moved[:, :128]
            normed_ref[1, :, z * 128 : z * 128 + 128] = moved[:, 128:]


def projected(index, core, pieces, normed_ref, weights):
    def store(row, piece, b):
        for m in range(MATS):
            lanes = slice((m % 2) * 128, (m % 2) * 128 + 128)
            weights[m // 2, pl.ds(row, 16), lanes] = piece[b, m * 16 : m * 16 + 16, :]

    fill_rows(index, core, pieces, lambda z, y, c: (z * 8 + y) * 16, store)
    normed = normed_ref[core % 2]
    return [jnp.dot(normed, weights[p], preferred_element_type=F32) for p in range(MATS // 2)]


def half_kernel(place_ref, p0, p1, p2, p3, normed_ref, out_ref, weights):
    index = place_ref[0]
    products = projected(index, index % 2, (p0, p1, p2, p3), normed_ref, weights)
    for p in range(MATS // 2):
        out_ref[p] = products[p]


def local_kernel(
    core_ref,
    p0,
    p1,
    p2,
    p3,
    normed_ref,
    half_ref,
    table_ref,
    extra_ref,
    mine_ref,
    theirs_ref,
    reads_ref,
    gate_ref,
    conv_ref,
    rim_ref,
    weights,
):
    core = core_ref[0] % 2
    products = []
    others = projected(core_ref[0], 1 - core, (p0, p1, p2, p3), normed_ref, weights)
    for p, product in enumerate(others):
        product = (product + half_ref[p]).astype(BF16).astype(F32)
        products += [product[:, :128], product[:, 128:]]
    recept, keys, values, decay_pre, removal_pre, gate_pre, conv_value, conv_gate = products
    key_gain, removal_gain, removal_bias, decay_bias, norm_out = (
        table_ref[k : k + 1, :] for k in range(5)
    )
    gate_ref[...] = norm_out * jax.nn.sigmoid(gate_pre)
    conv_input = (conv_value * jax.nn.sigmoid(conv_gate)).astype(BF16)
    conv_ref[...] = conv_input
    rim_ref[...] = conv_input[LENGTH - 32 :]

    rate = 0.6065306597126334 * jax.nn.sigmoid(decay_bias + decay_pre) + extra_ref[...]
    removal = jax.nn.sigmoid(removal_bias + removal_pre)
    lane = iota((LENGTH, 128), 1)
    first = lane < HEAD
    scaled = keys * key_gain
    square = scaled * scaled
    low = jnp.sum(jnp.where(first, square, 0.0), axis=-1, keepdims=True)
    high = jnp.sum(jnp.where(first, 0.0, square), axis=-1, keepdims=True)
    unit = scaled * lax.rsqrt(jnp.where(first, low, high) + 1e-06)
    written = keys * (1.0 + (removal - 1.0) * removal_gain)

    row, column = iota((LENGTH, LENGTH), 0), iota((LENGTH, LENGTH), 1)
    same = (row // BLOCK) == (column // BLOCK)
    strict = same & (row > column)
    inclusive = same & (row >= column)
    wide_row, wide_column = iota((LENGTH, 2 * LENGTH), 0), iota((LENGTH, 2 * LENGTH), 1)
    wide_column = jnp.where(wide_column >= LENGTH, wide_column - LENGTH, wide_column)
    inclusive_twice = ((wide_row // BLOCK) == (wide_column // BLOCK)) & (wide_row >= wide_column)
    falling = -sums_of(jnp.where(inclusive, 1.0, 0.0).astype(BF16), rate)
    before = falling + rate
    by_block = falling.reshape(BLOCKS, BLOCK, 128)
    middle = jnp.broadcast_to(
        by_block[:, BLOCK // 2 : BLOCK // 2 + 1], (BLOCKS, BLOCK, 128)
    ).reshape(LENGTH, 128)
    ending = jnp.broadcast_to(by_block[:, BLOCK - 1 :], (BLOCKS, BLOCK, 128)).reshape(LENGTH, 128)
    beta = unit * removal
    rising = jnp.exp(middle - falling)
    alpha_mid = -unit * jnp.exp(before - middle)
    recept_mid = recept * jnp.exp(falling - middle)
    right = jnp.concatenate([beta * rising, written * rising], axis=0)
    start_alpha = -unit * jnp.exp(before)
    start_recept = recept * jnp.exp(falling)
    closing = jnp.exp(ending - falling)
    end_beta = beta * closing
    end_keys = written * closing
    kept = jnp.exp(by_block[:, BLOCK - 1, :])
    turned_values = pltpu.roll(values, HEAD, 1)

    square_row, square_lane = iota((128, 128), 0), iota((128, 128), 1)
    diagonal = square_row == square_lane
    own = [first, jnp.logical_not(first)]
    own_row = [square_row < HEAD, square_row >= HEAD]
    power, solved, query, value_rows = [], [], [], []
    recept_pairs = []
    for h in range(2):
        left = jnp.concatenate(
            [jnp.where(own[h], alpha_mid, 0.0), jnp.where(own[h], recept_mid, 0.0)], axis=0
        )
        pairs = dot3(left, right, NT)
        power.append(jnp.where(strict, pairs[:LENGTH, :LENGTH], 0.0))
        alpha_keys = jnp.where(strict, pairs[:LENGTH, LENGTH:], 0.0)
        recept_pairs.append(jnp.where(inclusive_twice, pairs[LENGTH:], 0.0))
        value_rows.append(jnp.where(own[h], 0.0, turned_values))
        solved.append(jnp.where(own[h], start_alpha, dot3(alpha_keys, value_rows[h])))
    for step in range(5):
        solved = [solved[h] + dot3(power[h], solved[h]) for h in range(2)]
        if step < 4:
            power = [dot3(power[h], power[h]) for h in range(2)]
    for h in range(2):
        known = jnp.concatenate([solved[h], value_rows[h]], axis=0)
        query.append(jnp.where(own[h], start_recept, 0.0) + dot3(recept_pairs[h], known))
    steps = [[], []]
    whole = jnp.where(diagonal, 1.0, 0.0)
    for b in range(BLOCKS):
        rows = slice(b * BLOCK, b * BLOCK + BLOCK)
        ends = jnp.concatenate([end_beta[rows], end_keys[rows]], axis=0)
        held = jnp.where(diagonal, jnp.broadcast_to(kept[b : b + 1], (128, 128)), 0.0)
        for h in range(2):
            known = jnp.concatenate([solved[h][rows], value_rows[h][rows]], axis=0)
            steps[h].append(jnp.where(own_row[h], dot3(ends, known, TN) + held, whole))
    one = [dot3(steps[h][1], steps[h][0]) for h in range(2)]
    two = [dot3(steps[h][3], steps[h][2]) for h in range(2)]
    three = [dot3(steps[h][5], steps[h][4]) for h in range(2)]
    four = [dot3(two[h], one[h]) for h in range(2)]
    finals = [dot3(three[h], four[h])[h * HEAD : h * HEAD + HEAD] for h in range(2)]
    finals[1] = pltpu.roll(finals[1], HEAD, 1)
    mine_ref[...] = jnp.where(core == 0, finals[0], finals[1])
    theirs_ref[...] = jnp.where(core == 0, finals[1], finals[0])
    for h in range(2):
        prefixes = [
            None,
            steps[h][0],
            one[h],
            dot3(steps[h][2], one[h]),
            four[h],
            dot3(steps[h][4], four[h]),
        ]
        reads_ref[h, 0:BLOCK, :] = query[h][0:BLOCK]
        for b in range(1, BLOCKS):
            rows = slice(b * BLOCK, b * BLOCK + BLOCK)
            reads_ref[h, rows, :] = dot3(query[h][rows], prefixes[b])


WEIGHTS = (MATS // 2, 1024, 256)


def after(later, earlier):
    product = dot3(later[:, :HEAD], earlier)
    return product + jnp.where(iota((HEAD, 128), 1) < HEAD, 0.0, later)


def chained(steps):
    while len(steps) > 1:
        steps = [after(steps[k + 1], steps[k]) for k in range(0, len(steps), 2)]
    return steps[0]


def nothing():
    return jnp.where(iota((HEAD, 128), 0) == iota((HEAD, 128), 1), 1.0, 0.0)


def sent(step):
    return jnp.broadcast_to((step - nothing()).astype(BF16)[None], (8, HEAD, 128))


def received(steps_ref):
    return [steps_ref[k].astype(F32) + nothing() for k in range(8)]


def chip_kernel(core_ref, mine_ref, theirs_ref, out_ref):
    core = core_ref[0] % 2
    mine, theirs = mine_ref[...], theirs_ref[...]
    earlier = jnp.where(core == 0, mine, theirs)
    later = jnp.where(core == 0, theirs, mine)
    out_ref[...] = sent(after(later, earlier))


def row_kernel(place_ref, steps_ref, before_ref, total_ref):
    here = (place_ref[0] // 2) % 8
    steps = received(steps_ref)
    total_ref[...] = sent(chained(steps))
    before_ref[...] = chained([jnp.where(k < here, steps[k], nothing()) for k in range(8)])


def incoming_kernel(place_ref, steps_ref, before_ref, mine_ref, theirs_ref, own_ref, sent_ref):
    here, core = place_ref[0] // 16, place_ref[0] % 2
    steps = received(steps_ref)
    start = chained([jnp.where(k < here, steps[k], nothing()) for k in range(8)])
    at_chip = after(before_ref[...], start)
    earlier = jnp.where(core == 0, mine_ref[...], theirs_ref[...])
    at_second = after(earlier, at_chip)
    own_ref[...] = jnp.where(core == 0, at_chip, at_second)
    sent_ref[...] = jnp.where(core == 0, at_second, at_chip)


def conv_kernel(place_ref, input_ref, rim_ref, table_ref, filtered_ref, sums_ref):
    padded = jnp.concatenate([rim_ref[...], input_ref[...]], axis=0).astype(F32)
    filtered = jnp.broadcast_to(table_ref[5:6, :], (LENGTH, 128))
    for k in range(TAPS):
        filtered = filtered + table_ref[8 + k : 9 + k, :] * padded[k + 2 : k + 2 + LENGTH]
    filtered_ref[...] = filtered
    ones = jnp.ones((8, 128), F32)
    square = filtered * filtered
    rest = jnp.concatenate([filtered[128:], square[128:]], axis=0)
    at = iota((8, 128), 0)
    sums = jnp.where(at == 0, exact(ones, filtered[:128], NT), 0.0)
    sums = jnp.where(at == 1, exact(ones, square[:128], NT), sums)
    sums_ref[...] = jnp.where(at == 2, exact(ones, rest, NT), sums)


def columns_kernel(core_ref, *refs):
    index, out_ref = core_ref[0], refs[-1]
    core = index % 2

    def store(row, piece, b):
        for m in range(2):
            at = (MATS + m) * 16
            out_ref[pl.ds(row, 16), m * 128 : m * 128 + 128] = piece[b, at : at + 16, :]

    height = lambda z, y, c: place(z, y, c) * 16
    fill_rows(index, core, refs[:4], height, store)
    fill_rows(index, 1 - core, refs[4:8], height, store)


def final_kernel(
    core_ref,
    reads_ref,
    mine_ref,
    theirs_ref,
    gate_ref,
    filtered_ref,
    sums_ref,
    columns_ref,
    table_ref,
    out_ref,
):
    core = core_ref[0] % 2
    mine, theirs = mine_ref[...], theirs_ref[...]
    head0 = jnp.where(core == 0, mine, theirs)
    head1 = jnp.where(core == 0, theirs, mine)
    lane = iota((HEAD, 128), 1)
    equal = iota((HEAD, 128), 0)
    zero = jnp.zeros((HEAD, 128), F32)
    right0 = jnp.concatenate(
        [
            jnp.where(lane < HEAD, pltpu.roll(head0, HEAD, 1), zero),
            jnp.where(lane == equal, 1.0, 0.0),
        ],
        axis=0,
    )
    right1 = jnp.concatenate(
        [jnp.where(lane == equal + HEAD, 1.0, 0.0), jnp.where(lane < HEAD, zero, head1)], axis=0
    )
    reads = exact(reads_ref[0], right0) + exact(reads_ref[1], right1)
    first = iota((LENGTH, 128), 1) < HEAD

    def head_mean(x):
        low = jnp.sum(jnp.where(first, x, 0.0), axis=-1, keepdims=True)
        high = jnp.sum(jnp.where(first, 0.0, x), axis=-1, keepdims=True)
        return jnp.where(first, low, high) * (1.0 / HEAD)

    centered = reads - head_mean(reads)
    spread = head_mean(centered * centered)
    scan_out = (centered * lax.rsqrt(spread + 0.00064) * gate_ref[...]).astype(BF16)

    def spread_out(k):
        return exact(sums_ref[...], jnp.where(iota((8, 128), 0) == k, 1.0 / 512.0, 0.0), TN)

    rest = spread_out(2)
    center = jnp.concatenate([spread_out(0), rest[:64]], axis=0)
    second = jnp.concatenate([spread_out(1), rest[64:]], axis=0)
    scaled = (
        (filtered_ref[...] - center)
        * lax.rsqrt(second - center * center + 1e-05)
        * table_ref[6:7, :]
    )
    conv_out = (scaled * jax.nn.sigmoid(scaled)).astype(BF16)
    features = jnp.concatenate([scan_out, conv_out], axis=1)
    for j in range(4):
        out_ref[j] = lax.dot_general(
            features, columns_ref[j * 512 : j * 512 + 512, :], NT, preferred_element_type=F32
        ).astype(BF16)


def to_each(x, groups):
    return lax.all_to_all(x, "sp", 0, 0, tiled=True, axis_index_groups=groups)


def layer(
    tokens,
    norm_gain,
    query_weight,
    key_weight,
    value_weight,
    decay_weight,
    removal_weight,
    gate_weight,
    key_gain,
    removal_gain,
    removal_bias,
    decay_bias,
    decay_extra,
    scan_norm_gain,
    conv_value_weight,
    conv_gate_weight,
    conv_taps,
    conv_bias,
    conv_norm_gain,
    out_scan_weight,
    out_conv_weight,
):
    index = lax.axis_index("sp").astype(jnp.int32)[None]
    row = lambda v: v.reshape(1, -1)

    packed = pack(
        query_weight,
        key_weight,
        value_weight,
        decay_weight,
        removal_weight,
        gate_weight,
        conv_value_weight,
        conv_gate_weight,
        out_scan_weight.T,
        out_conv_weight.T,
    )
    plane = to_each(packed, FAR)
    whole = lax.all_gather(tokens, "tp")
    table, extra = on_core(
        table_kernel,
        (vmem((40, 128), F32), vmem((LENGTH, 128), F32)),
        index,
        given=(
            row(key_gain),
            row(removal_gain),
            row(removal_bias),
            row(decay_bias),
            row(scan_norm_gain),
            row(conv_bias),
            row(conv_norm_gain),
            conv_taps,
            decay_extra,
        ),
    )
    normed = on_core(
        norm_kernel, vmem((2, LENGTH, 1024), BF16), index, whole, given=(norm_gain.reshape(4, 512),)
    )
    pieces = [plane]
    for along_z, along_y in FLIPS[1:]:
        pieces.append(lax.ppermute(pieces[0], "sp", neighbours(along_z, along_y)))
    swapped = []
    for piece in pieces:
        swapped.append(lax.ppermute(piece, "sp", SWAP))
    half = on_core(
        half_kernel,
        vmem((MATS // 2, LENGTH, 256), F32),
        index,
        *pieces,
        normed,
        scratch=[pltpu.VMEM(WEIGHTS, BF16)],
        limit=16,
    )
    mine, theirs, reads, gate, conv_input, rim = on_core(
        local_kernel,
        (
            vmem((HEAD, 128), F32),
            vmem((HEAD, 128), F32),
            vmem((2, LENGTH, 128), F32),
            vmem((LENGTH, 128), F32),
            vmem((LENGTH, 128), BF16),
            vmem((32, 128), BF16),
        ),
        index,
        *swapped,
        normed,
        half,
        table,
        extra,
        scratch=[pltpu.VMEM(WEIGHTS, BF16)],
        limit=28,
    )

    theirs = lax.ppermute(theirs, "sp", SWAP)
    rim = lax.ppermute(rim, "sp", ONWARD)
    message = vmem((8, HEAD, 128), BF16)
    step = vmem((HEAD, 128), F32)
    chip = on_core(chip_kernel, message, index, mine, theirs)
    chips = to_each(chip, Y_AXIS)
    before, total = on_core(row_kernel, (step, message), index, chips)
    totals = to_each(total, Z_AXIS)
    own_state, sent_state = on_core(
        incoming_kernel, (step, step), index, totals, before, mine, theirs
    )
    other_state = lax.ppermute(sent_state, "sp", SWAP)

    filtered, sums = on_core(
        conv_kernel, (vmem((LENGTH, 128), F32), vmem((8, 128), F32)), index, conv_input, rim, table
    )
    sums = lax.psum(sums, "tp")
    columns = on_core(columns_kernel, vmem((2048, 256), BF16), index, *pieces, *swapped)

    terms = on_core(
        final_kernel,
        vmem((4, LENGTH, 512), BF16),
        index,
        reads,
        own_state,
        other_state,
        gate,
        filtered,
        sums,
        columns,
        table,
    )
    parts = lax.all_to_all(terms, "tp", 0, 0, tiled=True)
    return jnp.sum(parts.astype(F32), axis=0).astype(BF16)


def solution(mesh):
    weights = P("sp", "tp")
    in_specs = (
        (P("sp", "tp"), P())
        + (weights,) * 6
        + (P("tp"),) * 4
        + (P("sp", "tp"), P("tp"), weights, weights, P(None, "tp"), P("tp"), P("tp"))
        + (P("tp", "sp"), P("tp", "sp"))
    )
    return jax.shard_map(
        layer, mesh=mesh, in_specs=in_specs, out_specs=P("sp", "tp"), check_vma=False
    )
```

```python
import functools

import jax
import jax.numpy as jnp
from jax import lax
from jax.experimental import pallas as pl
from jax.experimental.pallas import tpu as pltpu
from jax.sharding import PartitionSpec as P

HEAD = 64
TAPS = 31
BLOCK = 32
LENGTH = 192
BLOCKS = LENGTH // BLOCK
MATS = 8
F32 = jnp.float32
BF16 = jnp.bfloat16

NN = (((1,), (0,)), ((), ()))
NT = (((1,), (1,)), ((), ()))
TN = (((0,), (0,)), ((), ()))


def place(z, y, c):
    return z * 16 + y * 2 + c


SETS = (((0, 2, 5, 7), (1, 3, 4, 6)), ((1, 3, 6, 0), (2, 4, 5, 7)))
FAR = [
    [place(z, y, c) for z in SETS[c][p] for y in SETS[c][q]]
    for c in range(2)
    for p in range(2)
    for q in range(2)
]


def partner(v, c):
    return v ^ 1 if c == 0 else (((v - 1) % 8 ^ 1) + 1) % 8


def neighbours(along_z, along_y):
    return [
        (place(z, y, c), place(partner(z, c) if along_z else z, partner(y, c) if along_y else y, c))
        for z in range(8)
        for y in range(8)
        for c in range(2)
    ]


Y_AXIS = [[place(z, y, c) for y in range(8)] for z in range(8) for c in range(2)]
Z_AXIS = [[place(z, y, c) for z in range(8)] for y in range(8) for c in range(2)]
SWAP = [(i, i ^ 1) for i in range(128)]
ONWARD = [(i, i + 1) for i in range(127)]


def split(x):
    high = x.astype(BF16)
    return high, (x - high.astype(F32)).astype(BF16)


def dot3(a, b, dims=NN):
    a_high, a_low = split(a)
    b_high, b_low = split(b)
    one = functools.partial(lax.dot_general, dimension_numbers=dims, preferred_element_type=F32)
    return one(a_high, b_high) + (one(a_high, b_low) + one(a_low, b_high))


def exact(a, b, dims=NN):
    return lax.dot_general(
        a, b, dims, precision=lax.Precision.HIGHEST, preferred_element_type=F32
    )


def sums_of(ones, x):
    high = x.astype(BF16)
    middle, low = split(x - high.astype(F32))
    one = lambda part: jnp.dot(ones, part, preferred_element_type=F32)
    return one(high) + (one(middle) + one(low))


def iota(shape, dim):
    return lax.broadcasted_iota(jnp.int32, shape, dim)


def vmem(shape, dtype):
    return pltpu.VMEM(shape, dtype)


def on_core(kernel, shapes, index, *operands, given=(), scratch=(), limit=8):
    return pl.pallas_call(
        kernel,
        in_specs=[pl.BlockSpec(memory_space=pltpu.SMEM)]
        + [pl.BlockSpec(memory_space=pltpu.VMEM)] * (len(operands) + len(given)),
        out_shape=shapes,
        scratch_shapes=scratch,
        compiler_params=pltpu.CompilerParams(vmem_limit_bytes=limit * 1024 * 1024),
    )(index, *(pltpu.with_memory_space_constraint(x, pltpu.VMEM) for x in operands), *given)


def pack_kernel(*refs):
    out = refs[-1]
    blocks = [ref[...] for ref in refs[:-1]]
    both = jnp.concatenate(blocks, axis=0)
    for k in range(16):
        out[k] = both


def pack(*mats):
    return pl.pallas_call(
        pack_kernel,
        out_shape=jax.ShapeDtypeStruct((16, 16 * len(mats), 128), BF16),
        name="pack",
    )(*mats)


FLIPS = ((0, 0), (0, 1), (1, 0), (1, 1))


def chosen(conditions, values):
    if not conditions:
        return values[0]
    half = len(values) // 2
    low, high = (chosen(conditions[1:], part) for part in (values[:half], values[half:]))
    return low if isinstance(low, int) and low == high else jnp.where(conditions[0], high, low)


def fill_rows(index, core, pieces, height, store):
    second = core == 1

    def axis(position):
        in_set1 = functools.reduce(
            jnp.logical_or,
            [
                jnp.logical_and(second == (c == 1), position == v)
                for c in range(2)
                for v in SETS[c][1]
            ],
        )
        return [
            [
                chosen(
                    (second, in_set1),
                    [SETS[c][p ^ flip][k] for c in range(2) for p in range(2)],
                )
                for k in range(4)
            ]
            for flip in range(2)
        ]

    zs, ys = axis(index // 16), axis((index // 2) % 8)
    for piece, (flip_z, flip_y) in zip(pieces, FLIPS):
        for b in range(16):
            row = height(zs[flip_z][b // 4], ys[flip_y][b % 4], core)
            store(pl.multiple_of(row, 16), piece, b)


def table_kernel(place_ref, *refs):
    vectors, taps_ref, extra_ref, table_ref, extra_out_ref = refs[:-4], *refs[-4:]
    for k, ref in enumerate(vectors):
        table_ref[k : k + 1, :] = ref[...]
    table_ref[8 : 8 + TAPS, :] = taps_ref[...]
    extra_out_ref[...] = extra_ref[...]


def norm_kernel(place_ref, tokens_ref, gain_ref, normed_ref):
    parts = [tokens_ref[j].astype(F32) for j in range(4)]
    total = sum(jnp.sum(part * part, axis=-1, keepdims=True) for part in parts)
    inverse_rms = lax.rsqrt(total * (1.0 / 2048.0) + 1e-06)
    goal = iota((256, 256), 1)
    source = ((goal % 128) // 16) * 32 + (goal // 128) * 16 + goal % 16
    moves = jnp.where(iota((256, 256), 0) == source, 1.0, 0.0).astype(BF16)
    for j, part in enumerate(parts):
        normed = (part * inverse_rms * gain_ref[j : j + 1, :]).astype(BF16)
        for h in range(2):
            moved = jnp.dot(
                normed[:, h * 256 : h * 256 + 256], moves, preferred_element_type=F32
            ).astype(BF16)
            z = j * 2 + h
            normed_ref[0, :, z * 128 : z * 128 + 128] = moved[:, :128]
            normed_ref[1, :, z * 128 : z * 128 + 128] = moved[:, 128:]


def projected(index, core, pieces, normed_ref, weights):
    def store(row, piece, b):
        for m in range(MATS):
            lanes = slice((m % 2) * 128, (m % 2) * 128 + 128)
            weights[m // 2, pl.ds(row, 16), lanes] = piece[b, m * 16 : m * 16 + 16, :]

    fill_rows(index, core, pieces, lambda z, y, c: (z * 8 + y) * 16, store)
    normed = normed_ref[core % 2]
    return [jnp.dot(normed, weights[p], preferred_element_type=F32) for p in range(MATS // 2)]


def half_kernel(place_ref, p0, p1, p2, p3, normed_ref, out_ref, weights):
    index = place_ref[0]
    products = projected(index, index % 2, (p0, p1, p2, p3), normed_ref, weights)
    for p in range(MATS // 2):
        out_ref[p] = products[p]


def local_kernel(
    core_ref,
    p0,
    p1,
    p2,
    p3,
    normed_ref,
    half_ref,
    table_ref,
    extra_ref,
    mine_ref,
    theirs_ref,
    gate_ref,
    conv_ref,
    rim_ref,
    tables_ref,
    solved_ref,
    steps_ref,
    weights,
):
    core = core_ref[0] % 2
    products = []
    others = projected(core_ref[0], 1 - core, (p0, p1, p2, p3), normed_ref, weights)
    for p, product in enumerate(others):
        product = (product + half_ref[p]).astype(BF16).astype(F32)
        products += [product[:, :128], product[:, 128:]]
    recept, keys, values, decay_pre, removal_pre, gate_pre, conv_value, conv_gate = products
    key_gain, removal_gain, removal_bias, decay_bias, norm_out = (
        table_ref[k : k + 1, :] for k in range(5)
    )
    gate_ref[...] = norm_out * jax.nn.sigmoid(gate_pre)
    conv_input = (conv_value * jax.nn.sigmoid(conv_gate)).astype(BF16)
    conv_ref[...] = conv_input
    rim_ref[...] = conv_input[LENGTH - 32 :]

    rate = 0.6065306597126334 * jax.nn.sigmoid(decay_bias + decay_pre) + extra_ref[...]
    removal = jax.nn.sigmoid(removal_bias + removal_pre)
    lane = iota((LENGTH, 128), 1)
    first = lane < HEAD
    scaled = keys * key_gain
    square = scaled * scaled
    low = jnp.sum(jnp.where(first, square, 0.0), axis=-1, keepdims=True)
    high = jnp.sum(jnp.where(first, 0.0, square), axis=-1, keepdims=True)
    unit = scaled * lax.rsqrt(jnp.where(first, low, high) + 1e-06)
    written = keys * (1.0 + (removal - 1.0) * removal_gain)

    row, column = iota((LENGTH, LENGTH), 0), iota((LENGTH, LENGTH), 1)
    same = (row // BLOCK) == (column // BLOCK)
    strict = same & (row > column)
    inclusive = same & (row >= column)
    falling = -sums_of(jnp.where(inclusive, 1.0, 0.0).astype(BF16), rate)
    before = falling + rate
    by_block = falling.reshape(BLOCKS, BLOCK, 128)
    middle = jnp.broadcast_to(
        by_block[:, BLOCK // 2 : BLOCK // 2 + 1], (BLOCKS, BLOCK, 128)
    ).reshape(LENGTH, 128)
    ending = jnp.broadcast_to(by_block[:, BLOCK - 1 :], (BLOCKS, BLOCK, 128)).reshape(LENGTH, 128)
    beta = unit * removal
    rising = jnp.exp(middle - falling)
    alpha_mid = -unit * jnp.exp(before - middle)
    tables_ref[0] = recept * jnp.exp(falling - middle)
    right = jnp.concatenate([beta * rising, written * rising], axis=0)
    start_alpha = -unit * jnp.exp(before)
    tables_ref[1] = recept * jnp.exp(falling)
    closing = jnp.exp(ending - falling)
    end_beta = beta * closing
    end_keys = written * closing
    kept = jnp.exp(by_block[:, BLOCK - 1, :])
    turned_values = pltpu.roll(values, HEAD, 1)
    tables_ref[2] = right[:LENGTH]
    tables_ref[3] = right[LENGTH:]
    tables_ref[4] = turned_values

    square_row, square_lane = iota((128, 128), 0), iota((128, 128), 1)
    diagonal = square_row == square_lane
    own = [first, jnp.logical_not(first)]
    own_row = [square_row < HEAD, square_row >= HEAD]
    power, solved, value_rows = [], [], []
    for h in range(2):
        pairs = dot3(jnp.where(own[h], alpha_mid, 0.0), right, NT)
        power.append(jnp.where(strict, pairs[:, :LENGTH], 0.0))
        alpha_keys = jnp.where(strict, pairs[:, LENGTH:], 0.0)
        value_rows.append(jnp.where(own[h], 0.0, turned_values))
        solved.append(jnp.where(own[h], start_alpha, dot3(alpha_keys, value_rows[h])))
    for step in range(5):
        solved = [solved[h] + dot3(power[h], solved[h]) for h in range(2)]
        if step < 4:
            power = [dot3(power[h], power[h]) for h in range(2)]
    for h in range(2):
        solved_ref[h] = solved[h]
    steps = [[], []]
    whole = jnp.where(diagonal, 1.0, 0.0)
    for b in range(BLOCKS):
        rows = slice(b * BLOCK, b * BLOCK + BLOCK)
        ends = jnp.concatenate([end_beta[rows], end_keys[rows]], axis=0)
        held = jnp.where(diagonal, jnp.broadcast_to(kept[b : b + 1], (128, 128)), 0.0)
        for h in range(2):
            known = jnp.concatenate([solved[h][rows], value_rows[h][rows]], axis=0)
            steps[h].append(jnp.where(own_row[h], dot3(ends, known, TN) + held, whole))
    one = [dot3(steps[h][1], steps[h][0]) for h in range(2)]
    two = [dot3(steps[h][3], steps[h][2]) for h in range(2)]
    three = [dot3(steps[h][5], steps[h][4]) for h in range(2)]
    four = [dot3(two[h], one[h]) for h in range(2)]
    finals = [dot3(three[h], four[h])[h * HEAD : h * HEAD + HEAD] for h in range(2)]
    finals[1] = pltpu.roll(finals[1], HEAD, 1)
    mine_ref[...] = jnp.where(core == 0, finals[0], finals[1])
    theirs_ref[...] = jnp.where(core == 0, finals[1], finals[0])
    for h in range(2):
        for k, step in enumerate((steps[h][0], one[h], steps[h][2], four[h], steps[h][4])):
            steps_ref[h, k] = step


def reads_kernel(place_ref, tables_ref, solved_ref, steps_ref, reads_ref):
    recept_mid, start_recept, turned_values = tables_ref[0], tables_ref[1], tables_ref[4]
    right = jnp.concatenate([tables_ref[2], tables_ref[3]], axis=0)
    first = iota((LENGTH, 128), 1) < HEAD
    wide_row, wide_column = iota((LENGTH, 2 * LENGTH), 0), iota((LENGTH, 2 * LENGTH), 1)
    wide_column = jnp.where(wide_column >= LENGTH, wide_column - LENGTH, wide_column)
    inclusive_twice = ((wide_row // BLOCK) == (wide_column // BLOCK)) & (wide_row >= wide_column)
    own = [first, jnp.logical_not(first)]
    query = []
    for h in range(2):
        pairs = dot3(jnp.where(own[h], recept_mid, 0.0), right, NT)
        pairs = jnp.where(inclusive_twice, pairs, 0.0)
        known = jnp.concatenate(
            [solved_ref[h], jnp.where(own[h], 0.0, turned_values)], axis=0
        )
        query.append(jnp.where(own[h], start_recept, 0.0) + dot3(pairs, known))
    for h in range(2):
        zero, one, two, four, five = (steps_ref[h, k] for k in range(5))
        prefixes = (None, zero, one, dot3(two, one), four, dot3(five, four))
        reads_ref[h, 0:BLOCK, :] = query[h][0:BLOCK]
        for b in range(1, BLOCKS):
            rows = slice(b * BLOCK, b * BLOCK + BLOCK)
            reads_ref[h, rows, :] = dot3(query[h][rows], prefixes[b])


WEIGHTS = (MATS // 2, 1024, 256)


def after(later, earlier):
    product = dot3(later[:, :HEAD], earlier)
    return product + jnp.where(iota((HEAD, 128), 1) < HEAD, 0.0, later)


def chained(steps):
    while len(steps) > 1:
        steps = [after(steps[k + 1], steps[k]) for k in range(0, len(steps), 2)]
    return steps[0]


def nothing():
    return jnp.where(iota((HEAD, 128), 0) == iota((HEAD, 128), 1), 1.0, 0.0)


def sent(step):
    return jnp.broadcast_to((step - nothing()).astype(BF16)[None], (8, HEAD, 128))


def received(steps_ref):
    return [steps_ref[k].astype(F32) + nothing() for k in range(8)]


def chip_kernel(core_ref, mine_ref, theirs_ref, out_ref):
    core = core_ref[0] % 2
    mine, theirs = mine_ref[...], theirs_ref[...]
    earlier = jnp.where(core == 0, mine, theirs)
    later = jnp.where(core == 0, theirs, mine)
    out_ref[...] = sent(after(later, earlier))


def row_kernel(place_ref, steps_ref, before_ref, total_ref):
    here = (place_ref[0] // 2) % 8
    steps = received(steps_ref)
    total_ref[...] = sent(chained(steps))
    before_ref[...] = chained([jnp.where(k < here, steps[k], nothing()) for k in range(8)])


def incoming_kernel(place_ref, steps_ref, before_ref, mine_ref, theirs_ref, own_ref, sent_ref):
    here, core = place_ref[0] // 16, place_ref[0] % 2
    steps = received(steps_ref)
    start = chained([jnp.where(k < here, steps[k], nothing()) for k in range(8)])
    at_chip = after(before_ref[...], start)
    earlier = jnp.where(core == 0, mine_ref[...], theirs_ref[...])
    at_second = after(earlier, at_chip)
    own_ref[...] = jnp.where(core == 0, at_chip, at_second)
    sent_ref[...] = jnp.where(core == 0, at_second, at_chip)


def conv_kernel(place_ref, input_ref, rim_ref, table_ref, filtered_ref, sums_ref):
    padded = jnp.concatenate([rim_ref[...], input_ref[...]], axis=0).astype(F32)
    filtered = jnp.broadcast_to(table_ref[5:6, :], (LENGTH, 128))
    for k in range(TAPS):
        filtered = filtered + table_ref[8 + k : 9 + k, :] * padded[k + 2 : k + 2 + LENGTH]
    filtered_ref[...] = filtered
    ones = jnp.ones((8, 128), F32)
    square = filtered * filtered
    rest = jnp.concatenate([filtered[128:], square[128:]], axis=0)
    at = iota((8, 128), 0)
    sums = jnp.where(at == 0, exact(ones, filtered[:128], NT), 0.0)
    sums = jnp.where(at == 1, exact(ones, square[:128], NT), sums)
    sums_ref[...] = jnp.where(at == 2, exact(ones, rest, NT), sums)


def columns_kernel(core_ref, *refs):
    index, out_ref = core_ref[0], refs[-1]
    core = index % 2

    def store(row, piece, b):
        for m in range(2):
            at = (MATS + m) * 16
            out_ref[pl.ds(row, 16), m * 128 : m * 128 + 128] = piece[b, at : at + 16, :]

    height = lambda z, y, c: place(z, y, c) * 16
    fill_rows(index, core, refs[:4], height, store)
    fill_rows(index, 1 - core, refs[4:8], height, store)


def final_kernel(
    core_ref,
    reads_ref,
    mine_ref,
    theirs_ref,
    gate_ref,
    filtered_ref,
    sums0_ref,
    sums1_ref,
    sums2_ref,
    sums3_ref,
    columns_ref,
    table_ref,
    out_ref,
):
    core = core_ref[0] % 2
    mine, theirs = mine_ref[...], theirs_ref[...]
    head0 = jnp.where(core == 0, mine, theirs)
    head1 = jnp.where(core == 0, theirs, mine)
    lane = iota((HEAD, 128), 1)
    equal = iota((HEAD, 128), 0)
    zero = jnp.zeros((HEAD, 128), F32)
    right0 = jnp.concatenate(
        [
            jnp.where(lane < HEAD, pltpu.roll(head0, HEAD, 1), zero),
            jnp.where(lane == equal, 1.0, 0.0),
        ],
        axis=0,
    )
    right1 = jnp.concatenate(
        [jnp.where(lane == equal + HEAD, 1.0, 0.0), jnp.where(lane < HEAD, zero, head1)], axis=0
    )
    reads = exact(reads_ref[0], right0) + exact(reads_ref[1], right1)
    first = iota((LENGTH, 128), 1) < HEAD

    def head_mean(x):
        low = jnp.sum(jnp.where(first, x, 0.0), axis=-1, keepdims=True)
        high = jnp.sum(jnp.where(first, 0.0, x), axis=-1, keepdims=True)
        return jnp.where(first, low, high) * (1.0 / HEAD)

    centered = reads - head_mean(reads)
    spread = head_mean(centered * centered)
    scan_out = (centered * lax.rsqrt(spread + 0.00064) * gate_ref[...]).astype(BF16)

    sums = (sums0_ref[...] + sums1_ref[...]) + (sums2_ref[...] + sums3_ref[...])

    def spread_out(k):
        return exact(sums, jnp.where(iota((8, 128), 0) == k, 1.0 / 512.0, 0.0), TN)

    rest = spread_out(2)
    center = jnp.concatenate([spread_out(0), rest[:64]], axis=0)
    second = jnp.concatenate([spread_out(1), rest[64:]], axis=0)
    scaled = (
        (filtered_ref[...] - center)
        * lax.rsqrt(second - center * center + 1e-05)
        * table_ref[6:7, :]
    )
    conv_out = (scaled * jax.nn.sigmoid(scaled)).astype(BF16)
    features = jnp.concatenate([scan_out, conv_out], axis=1)
    for j in range(4):
        out_ref[j] = lax.dot_general(
            features, columns_ref[j * 512 : j * 512 + 512, :], NT, preferred_element_type=F32
        ).astype(BF16)


def to_each(x, groups):
    return lax.all_to_all(x, "sp", 0, 0, tiled=True, axis_index_groups=groups)


def layer(
    tokens,
    norm_gain,
    query_weight,
    key_weight,
    value_weight,
    decay_weight,
    removal_weight,
    gate_weight,
    key_gain,
    removal_gain,
    removal_bias,
    decay_bias,
    decay_extra,
    scan_norm_gain,
    conv_value_weight,
    conv_gate_weight,
    conv_taps,
    conv_bias,
    conv_norm_gain,
    out_scan_weight,
    out_conv_weight,
):
    index = lax.axis_index("sp").astype(jnp.int32)[None]
    row = lambda v: v.reshape(1, -1)

    packed = pack(
        query_weight,
        key_weight,
        value_weight,
        decay_weight,
        removal_weight,
        gate_weight,
        conv_value_weight,
        conv_gate_weight,
        out_scan_weight.T,
        out_conv_weight.T,
    )
    plane = to_each(packed, FAR)
    whole = lax.all_gather(tokens, "tp")
    table, extra = on_core(
        table_kernel,
        (vmem((40, 128), F32), vmem((LENGTH, 128), F32)),
        index,
        given=(
            row(key_gain),
            row(removal_gain),
            row(removal_bias),
            row(decay_bias),
            row(scan_norm_gain),
            row(conv_bias),
            row(conv_norm_gain),
            conv_taps,
            decay_extra,
        ),
    )
    normed = on_core(
        norm_kernel, vmem((2, LENGTH, 1024), BF16), index, whole, given=(norm_gain.reshape(4, 512),)
    )
    pieces = [plane]
    for along_z, along_y in FLIPS[1:]:
        pieces.append(lax.ppermute(pieces[0], "sp", neighbours(along_z, along_y)))
    swapped = []
    for piece in pieces:
        swapped.append(lax.ppermute(piece, "sp", SWAP))
    half = on_core(
        half_kernel,
        vmem((MATS // 2, LENGTH, 256), F32),
        index,
        *pieces,
        normed,
        scratch=[pltpu.VMEM(WEIGHTS, BF16)],
        limit=16,
    )
    mine, theirs, gate, conv_input, rim, tables, solved, steps = on_core(
        local_kernel,
        (
            vmem((HEAD, 128), F32),
            vmem((HEAD, 128), F32),
            vmem((LENGTH, 128), F32),
            vmem((LENGTH, 128), BF16),
            vmem((32, 128), BF16),
            vmem((5, LENGTH, 128), F32),
            vmem((2, LENGTH, 128), F32),
            vmem((2, 5, 128, 128), F32),
        ),
        index,
        *swapped,
        normed,
        half,
        table,
        extra,
        scratch=[pltpu.VMEM(WEIGHTS, BF16)],
        limit=28,
    )

    theirs = lax.ppermute(theirs, "sp", SWAP)
    rim = lax.ppermute(rim, "sp", ONWARD)
    message = vmem((8, HEAD, 128), BF16)
    step = vmem((HEAD, 128), F32)
    chip = on_core(chip_kernel, message, index, mine, theirs)
    chips = to_each(chip, Y_AXIS)
    before, total = on_core(row_kernel, (step, message), index, chips)
    totals = to_each(total, Z_AXIS)
    own_state, sent_state = on_core(
        incoming_kernel, (step, step), index, totals, before, mine, theirs
    )
    other_state = lax.ppermute(sent_state, "sp", SWAP)

    filtered, sums = on_core(
        conv_kernel, (vmem((LENGTH, 128), F32), vmem((8, 128), F32)), index, conv_input, rim, table
    )
    shares = [sums]
    for k in range(1, 4):
        shares.append(lax.ppermute(sums, "tp", [(x, (x + k) % 4) for x in range(4)]))
    reads = on_core(
        reads_kernel, vmem((2, LENGTH, 128), F32), index, tables, solved, steps, limit=12
    )
    columns = on_core(columns_kernel, vmem((2048, 256), BF16), index, *pieces, *swapped)

    terms = on_core(
        final_kernel,
        vmem((4, LENGTH, 512), BF16),
        index,
        reads,
        own_state,
        other_state,
        gate,
        filtered,
        *shares,
        columns,
        table,
    )
    parts = lax.all_to_all(terms, "tp", 0, 0, tiled=True)
    return jnp.sum(parts.astype(F32), axis=0).astype(BF16)


def solution(mesh):
    weights = P("sp", "tp")
    in_specs = (
        (P("sp", "tp"), P())
        + (weights,) * 6
        + (P("tp"),) * 4
        + (P("sp", "tp"), P("tp"), weights, weights, P(None, "tp"), P("tp"), P("tp"))
        + (P("tp", "sp"), P("tp", "sp"))
    )
    return jax.shard_map(
        layer, mesh=mesh, in_specs=in_specs, out_specs=P("sp", "tp"), check_vma=False
    )
```

```python
import functools

import jax
import jax.numpy as jnp
from jax import lax
from jax.experimental import pallas as pl
from jax.experimental.pallas import tpu as pltpu
from jax.sharding import PartitionSpec as P

HEAD = 64
TAPS = 31
BLOCK = 32
LENGTH = 192
BLOCKS = LENGTH // BLOCK
MATS = 8
F32 = jnp.float32
BF16 = jnp.bfloat16

NN = (((1,), (0,)), ((), ()))
NT = (((1,), (1,)), ((), ()))
TN = (((0,), (0,)), ((), ()))


def place(z, y, c):
    return z * 16 + y * 2 + c


SETS = (((0, 2, 5, 7), (1, 3, 4, 6)), ((1, 3, 6, 0), (2, 4, 5, 7)))
FAR = [
    [place(z, y, c) for z in SETS[c][p] for y in SETS[c][q]]
    for c in range(2)
    for p in range(2)
    for q in range(2)
]


def partner(v, c):
    return v ^ 1 if c == 0 else (((v - 1) % 8 ^ 1) + 1) % 8


def neighbours(along_z, along_y):
    return [
        (place(z, y, c), place(partner(z, c) if along_z else z, partner(y, c) if along_y else y, c))
        for z in range(8)
        for y in range(8)
        for c in range(2)
    ]


Y_AXIS = [[place(z, y, c) for y in range(8)] for z in range(8) for c in range(2)]
Z_AXIS = [[place(z, y, c) for z in range(8)] for y in range(8) for c in range(2)]
SWAP = [(i, i ^ 1) for i in range(128)]
ONWARD = [(i, i + 1) for i in range(127)]


def split(x):
    high = x.astype(BF16)
    return high, (x - high.astype(F32)).astype(BF16)


def dot3(a, b, dims=NN):
    a_high, a_low = split(a)
    b_high, b_low = split(b)
    one = functools.partial(lax.dot_general, dimension_numbers=dims, preferred_element_type=F32)
    return one(a_high, b_high) + (one(a_high, b_low) + one(a_low, b_high))


def exact(a, b, dims=NN):
    return lax.dot_general(
        a, b, dims, precision=lax.Precision.HIGHEST, preferred_element_type=F32
    )


def sums_of(ones, x):
    high = x.astype(BF16)
    middle, low = split(x - high.astype(F32))
    one = lambda part: jnp.dot(ones, part, preferred_element_type=F32)
    return one(high) + (one(middle) + one(low))


def iota(shape, dim):
    return lax.broadcasted_iota(jnp.int32, shape, dim)


def vmem(shape, dtype):
    return pltpu.VMEM(shape, dtype)


def on_core(kernel, shapes, index, *operands, given=(), scratch=(), limit=8):
    return pl.pallas_call(
        kernel,
        in_specs=[pl.BlockSpec(memory_space=pltpu.SMEM)]
        + [pl.BlockSpec(memory_space=pltpu.VMEM)] * (len(operands) + len(given)),
        out_shape=shapes,
        scratch_shapes=scratch,
        compiler_params=pltpu.CompilerParams(vmem_limit_bytes=limit * 1024 * 1024),
    )(index, *(pltpu.with_memory_space_constraint(x, pltpu.VMEM) for x in operands), *given)


def pack_kernel(*refs):
    out = refs[-1]
    blocks = [ref[...] for ref in refs[:-1]]
    both = jnp.concatenate(blocks, axis=0)
    for k in range(16):
        out[k] = both


def pack(*mats):
    return pl.pallas_call(
        pack_kernel,
        out_shape=jax.ShapeDtypeStruct((16, 16 * len(mats), 128), BF16),
        name="pack",
    )(*mats)


FLIPS = ((0, 0), (0, 1), (1, 0), (1, 1))


def chosen(conditions, values):
    if not conditions:
        return values[0]
    half = len(values) // 2
    low, high = (chosen(conditions[1:], part) for part in (values[:half], values[half:]))
    return low if isinstance(low, int) and low == high else jnp.where(conditions[0], high, low)


def fill_rows(index, core, pieces, height, store):
    second = core == 1

    def axis(position):
        in_set1 = functools.reduce(
            jnp.logical_or,
            [
                jnp.logical_and(second == (c == 1), position == v)
                for c in range(2)
                for v in SETS[c][1]
            ],
        )
        return [
            [
                chosen(
                    (second, in_set1),
                    [SETS[c][p ^ flip][k] for c in range(2) for p in range(2)],
                )
                for k in range(4)
            ]
            for flip in range(2)
        ]

    zs, ys = axis(index // 16), axis((index // 2) % 8)
    for piece, (flip_z, flip_y) in zip(pieces, FLIPS):
        for b in range(16):
            row = height(zs[flip_z][b // 4], ys[flip_y][b % 4], core)
            store(pl.multiple_of(row, 16), piece, b)


def table_kernel(place_ref, *refs):
    vectors, taps_ref, extra_ref, table_ref, extra_out_ref = refs[:-4], *refs[-4:]
    for k, ref in enumerate(vectors):
        table_ref[k : k + 1, :] = ref[...]
    table_ref[8 : 8 + TAPS, :] = taps_ref[...]
    extra_out_ref[...] = extra_ref[...]


def norm_kernel(place_ref, tokens_ref, gain_ref, normed_ref):
    parts = [tokens_ref[j].astype(F32) for j in range(4)]
    total = sum(jnp.sum(part * part, axis=-1, keepdims=True) for part in parts)
    inverse_rms = lax.rsqrt(total * (1.0 / 2048.0) + 1e-06)
    goal = iota((256, 256), 1)
    source = ((goal % 128) // 16) * 32 + (goal // 128) * 16 + goal % 16
    moves = jnp.where(iota((256, 256), 0) == source, 1.0, 0.0).astype(BF16)
    for j, part in enumerate(parts):
        normed = (part * inverse_rms * gain_ref[j : j + 1, :]).astype(BF16)
        for h in range(2):
            moved = jnp.dot(
                normed[:, h * 256 : h * 256 + 256], moves, preferred_element_type=F32
            ).astype(BF16)
            z = j * 2 + h
            normed_ref[0, :, z * 128 : z * 128 + 128] = moved[:, :128]
            normed_ref[1, :, z * 128 : z * 128 + 128] = moved[:, 128:]


def projected(index, core, pieces, normed_ref, weights):
    def store(row, piece, b):
        for m in range(MATS):
            lanes = slice((m % 2) * 128, (m % 2) * 128 + 128)
            weights[m // 2, pl.ds(row, 16), lanes] = piece[b, m * 16 : m * 16 + 16, :]

    fill_rows(index, core, pieces, lambda z, y, c: (z * 8 + y) * 16, store)
    normed = normed_ref[core % 2]
    return [jnp.dot(normed, weights[p], preferred_element_type=F32) for p in range(MATS // 2)]


def half_kernel(place_ref, p0, p1, p2, p3, normed_ref, out_ref, weights):
    index = place_ref[0]
    products = projected(index, index % 2, (p0, p1, p2, p3), normed_ref, weights)
    for p in range(MATS // 2):
        out_ref[p] = products[p]


def local_kernel(
    core_ref,
    p0,
    p1,
    p2,
    p3,
    normed_ref,
    half_ref,
    table_ref,
    extra_ref,
    mine_ref,
    theirs_ref,
    gate_ref,
    conv_ref,
    rim_ref,
    tables_ref,
    solved_ref,
    steps_ref,
    weights,
):
    core = core_ref[0] % 2
    products = []
    others = projected(core_ref[0], 1 - core, (p0, p1, p2, p3), normed_ref, weights)
    for p, product in enumerate(others):
        product = (product + half_ref[p]).astype(BF16).astype(F32)
        products += [product[:, :128], product[:, 128:]]
    recept, keys, values, decay_pre, removal_pre, gate_pre, conv_value, conv_gate = products
    key_gain, removal_gain, removal_bias, decay_bias, norm_out = (
        table_ref[k : k + 1, :] for k in range(5)
    )
    gate_ref[...] = norm_out * jax.nn.sigmoid(gate_pre)
    conv_input = (conv_value * jax.nn.sigmoid(conv_gate)).astype(BF16)
    conv_ref[...] = conv_input
    rim_ref[...] = conv_input[LENGTH - 32 :]

    rate = 0.6065306597126334 * jax.nn.sigmoid(decay_bias + decay_pre) + extra_ref[...]
    removal = jax.nn.sigmoid(removal_bias + removal_pre)
    lane = iota((LENGTH, 128), 1)
    first = lane < HEAD
    scaled = keys * key_gain
    square = scaled * scaled
    low = jnp.sum(jnp.where(first, square, 0.0), axis=-1, keepdims=True)
    high = jnp.sum(jnp.where(first, 0.0, square), axis=-1, keepdims=True)
    unit = scaled * lax.rsqrt(jnp.where(first, low, high) + 1e-06)
    written = keys * (1.0 + (removal - 1.0) * removal_gain)

    row, column = iota((LENGTH, LENGTH), 0), iota((LENGTH, LENGTH), 1)
    same = (row // BLOCK) == (column // BLOCK)
    strict = same & (row > column)
    inclusive = same & (row >= column)
    falling = -sums_of(jnp.where(inclusive, 1.0, 0.0).astype(BF16), rate)
    before = falling + rate
    by_block = falling.reshape(BLOCKS, BLOCK, 128)
    middle = jnp.broadcast_to(
        by_block[:, BLOCK // 2 : BLOCK // 2 + 1], (BLOCKS, BLOCK, 128)
    ).reshape(LENGTH, 128)
    ending = jnp.broadcast_to(by_block[:, BLOCK - 1 :], (BLOCKS, BLOCK, 128)).reshape(LENGTH, 128)
    beta = unit * removal
    rising = jnp.exp(middle - falling)
    alpha_mid = -unit * jnp.exp(before - middle)
    tables_ref[0] = recept * jnp.exp(falling - middle)
    right = jnp.concatenate([beta * rising, written * rising], axis=0)
    start_alpha = -unit * jnp.exp(before)
    tables_ref[1] = recept * jnp.exp(falling)
    closing = jnp.exp(ending - falling)
    end_beta = beta * closing
    end_keys = written * closing
    kept = jnp.exp(by_block[:, BLOCK - 1, :])
    turned_values = pltpu.roll(values, HEAD, 1)
    tables_ref[2] = right[:LENGTH]
    tables_ref[3] = right[LENGTH:]
    tables_ref[4] = turned_values

    square_row, square_lane = iota((128, 128), 0), iota((128, 128), 1)
    diagonal = square_row == square_lane
    own = [first, jnp.logical_not(first)]
    own_row = [square_row < HEAD, square_row >= HEAD]
    power, solved, value_rows = [], [], []
    for h in range(2):
        pairs = dot3(jnp.where(own[h], alpha_mid, 0.0), right, NT)
        power.append(jnp.where(strict, pairs[:, :LENGTH], 0.0))
        alpha_keys = jnp.where(strict, pairs[:, LENGTH:], 0.0)
        value_rows.append(jnp.where(own[h], 0.0, turned_values))
        solved.append(jnp.where(own[h], start_alpha, dot3(alpha_keys, value_rows[h])))
    for step in range(5):
        solved = [solved[h] + dot3(power[h], solved[h]) for h in range(2)]
        if step < 4:
            power = [dot3(power[h], power[h]) for h in range(2)]
    for h in range(2):
        solved_ref[h] = solved[h]
    steps = [[], []]
    whole = jnp.where(diagonal, 1.0, 0.0)
    for b in range(BLOCKS):
        rows = slice(b * BLOCK, b * BLOCK + BLOCK)
        ends = jnp.concatenate([end_beta[rows], end_keys[rows]], axis=0)
        held = jnp.where(diagonal, jnp.broadcast_to(kept[b : b + 1], (128, 128)), 0.0)
        for h in range(2):
            known = jnp.concatenate([solved[h][rows], value_rows[h][rows]], axis=0)
            steps[h].append(jnp.where(own_row[h], dot3(ends, known, TN) + held, whole))
    one = [dot3(steps[h][1], steps[h][0]) for h in range(2)]
    two = [dot3(steps[h][3], steps[h][2]) for h in range(2)]
    three = [dot3(steps[h][5], steps[h][4]) for h in range(2)]
    four = [dot3(two[h], one[h]) for h in range(2)]
    finals = [dot3(three[h], four[h])[h * HEAD : h * HEAD + HEAD] for h in range(2)]
    finals[1] = pltpu.roll(finals[1], HEAD, 1)
    mine_ref[...] = jnp.where(core == 0, finals[0], finals[1])
    theirs_ref[...] = jnp.where(core == 0, finals[1], finals[0])
    for h in range(2):
        for k, step in enumerate((steps[h][0], one[h], steps[h][2], four[h], steps[h][4])):
            steps_ref[h, k] = step[h * HEAD : h * HEAD + HEAD]


def reads_kernel(place_ref, tables_ref, solved_ref, steps_ref, reads_ref):
    recept_mid, start_recept, turned_values = tables_ref[0], tables_ref[1], tables_ref[4]
    right = jnp.concatenate([tables_ref[2], tables_ref[3]], axis=0)
    first = iota((LENGTH, 128), 1) < HEAD
    wide_row, wide_column = iota((LENGTH, 2 * LENGTH), 0), iota((LENGTH, 2 * LENGTH), 1)
    wide_column = jnp.where(wide_column >= LENGTH, wide_column - LENGTH, wide_column)
    inclusive_twice = ((wide_row // BLOCK) == (wide_column // BLOCK)) & (wide_row >= wide_column)
    own = [first, jnp.logical_not(first)]
    query = []
    for h in range(2):
        pairs = dot3(jnp.where(own[h], recept_mid, 0.0), right, NT)
        pairs = jnp.where(inclusive_twice, pairs, 0.0)
        known = jnp.concatenate(
            [solved_ref[h], jnp.where(own[h], 0.0, turned_values)], axis=0
        )
        query.append(jnp.where(own[h], start_recept, 0.0) + dot3(pairs, known))
    lane, equal = iota((HEAD, 128), 1), iota((HEAD, 128), 0)
    for h in range(2):
        rest = jnp.where(lane == equal + (HEAD if h == 0 else 0), 1.0, 0.0)
        zero, one, two, four, five = (
            jnp.concatenate(
                [steps_ref[h, k], rest] if h == 0 else [rest, steps_ref[h, k]], axis=0
            )
            for k in range(5)
        )
        prefixes = (None, zero, one, dot3(two, one), four, dot3(five, four))
        reads_ref[h, 0:BLOCK, :] = query[h][0:BLOCK]
        for b in range(1, BLOCKS):
            rows = slice(b * BLOCK, b * BLOCK + BLOCK)
            reads_ref[h, rows, :] = dot3(query[h][rows], prefixes[b])


WEIGHTS = (MATS // 2, 1024, 256)


def after(later, earlier):
    product = dot3(later[:, :HEAD], earlier)
    return product + jnp.where(iota((HEAD, 128), 1) < HEAD, 0.0, later)


def chained(steps):
    while len(steps) > 1:
        steps = [after(steps[k + 1], steps[k]) for k in range(0, len(steps), 2)]
    return steps[0]


def nothing():
    return jnp.where(iota((HEAD, 128), 0) == iota((HEAD, 128), 1), 1.0, 0.0)


def sent(step):
    return jnp.broadcast_to((step - nothing()).astype(BF16)[None], (8, HEAD, 128))


def received(steps_ref):
    return [steps_ref[k].astype(F32) + nothing() for k in range(8)]


def chip_kernel(core_ref, mine_ref, theirs_ref, out_ref):
    core = core_ref[0] % 2
    mine, theirs = mine_ref[...], theirs_ref[...]
    earlier = jnp.where(core == 0, mine, theirs)
    later = jnp.where(core == 0, theirs, mine)
    out_ref[...] = sent(after(later, earlier))


def row_kernel(place_ref, steps_ref, before_ref, total_ref):
    here = (place_ref[0] // 2) % 8
    steps = received(steps_ref)
    total_ref[...] = sent(chained(steps))
    before_ref[...] = chained([jnp.where(k < here, steps[k], nothing()) for k in range(8)])


def incoming_kernel(place_ref, steps_ref, before_ref, mine_ref, theirs_ref, own_ref, sent_ref):
    here, core = place_ref[0] // 16, place_ref[0] % 2
    steps = received(steps_ref)
    start = chained([jnp.where(k < here, steps[k], nothing()) for k in range(8)])
    at_chip = after(before_ref[...], start)
    earlier = jnp.where(core == 0, mine_ref[...], theirs_ref[...])
    at_second = after(earlier, at_chip)
    own_ref[...] = jnp.where(core == 0, at_chip, at_second)
    sent_ref[...] = jnp.where(core == 0, at_second, at_chip)


def conv_kernel(place_ref, input_ref, rim_ref, table_ref, filtered_ref, sums_ref):
    padded = jnp.concatenate([rim_ref[...], input_ref[...]], axis=0).astype(F32)
    filtered = jnp.broadcast_to(table_ref[5:6, :], (LENGTH, 128))
    for k in range(TAPS):
        filtered = filtered + table_ref[8 + k : 9 + k, :] * padded[k + 2 : k + 2 + LENGTH]
    filtered_ref[...] = filtered
    ones = jnp.ones((8, 128), F32)
    square = filtered * filtered
    rest = jnp.concatenate([filtered[128:], square[128:]], axis=0)
    at = iota((8, 128), 0)
    sums = jnp.where(at == 0, exact(ones, filtered[:128], NT), 0.0)
    sums = jnp.where(at == 1, exact(ones, square[:128], NT), sums)
    sums_ref[...] = jnp.where(at == 2, exact(ones, rest, NT), sums)


def columns_kernel(core_ref, *refs):
    index, out_ref = core_ref[0], refs[-1]
    core = index % 2

    def store(row, piece, b):
        for m in range(2):
            at = (MATS + m) * 16
            out_ref[pl.ds(row, 16), m * 128 : m * 128 + 128] = piece[b, at : at + 16, :]

    height = lambda z, y, c: place(z, y, c) * 16
    fill_rows(index, core, refs[:4], height, store)
    fill_rows(index, 1 - core, refs[4:8], height, store)


def final_kernel(
    core_ref,
    reads_ref,
    mine_ref,
    theirs_ref,
    gate_ref,
    filtered_ref,
    shares_ref,
    columns_ref,
    table_ref,
    out_ref,
):
    core = core_ref[0] % 2
    mine, theirs = mine_ref[...], theirs_ref[...]
    head0 = jnp.where(core == 0, mine, theirs)
    head1 = jnp.where(core == 0, theirs, mine)
    lane = iota((HEAD, 128), 1)
    equal = iota((HEAD, 128), 0)
    zero = jnp.zeros((HEAD, 128), F32)
    right0 = jnp.concatenate(
        [
            jnp.where(lane < HEAD, pltpu.roll(head0, HEAD, 1), zero),
            jnp.where(lane == equal, 1.0, 0.0),
        ],
        axis=0,
    )
    right1 = jnp.concatenate(
        [jnp.where(lane == equal + HEAD, 1.0, 0.0), jnp.where(lane < HEAD, zero, head1)], axis=0
    )
    reads = exact(reads_ref[0], right0) + exact(reads_ref[1], right1)
    first = iota((LENGTH, 128), 1) < HEAD

    def head_mean(x):
        low = jnp.sum(jnp.where(first, x, 0.0), axis=-1, keepdims=True)
        high = jnp.sum(jnp.where(first, 0.0, x), axis=-1, keepdims=True)
        return jnp.where(first, low, high) * (1.0 / HEAD)

    centered = reads - head_mean(reads)
    spread = head_mean(centered * centered)
    scan_out = (centered * lax.rsqrt(spread + 0.00064) * gate_ref[...]).astype(BF16)

    sums = (shares_ref[0] + shares_ref[1]) + (shares_ref[2] + shares_ref[3])

    def spread_out(k):
        return exact(sums, jnp.where(iota((8, 128), 0) == k, 1.0 / 512.0, 0.0), TN)

    rest = spread_out(2)
    center = jnp.concatenate([spread_out(0), rest[:64]], axis=0)
    second = jnp.concatenate([spread_out(1), rest[64:]], axis=0)
    scaled = (
        (filtered_ref[...] - center)
        * lax.rsqrt(second - center * center + 1e-05)
        * table_ref[6:7, :]
    )
    conv_out = (scaled * jax.nn.sigmoid(scaled)).astype(BF16)
    features = jnp.concatenate([scan_out, conv_out], axis=1)
    for j in range(4):
        out_ref[j] = lax.dot_general(
            features, columns_ref[j * 512 : j * 512 + 512, :], NT, preferred_element_type=F32
        ).astype(BF16)


def to_each(x, groups):
    return lax.all_to_all(x, "sp", 0, 0, tiled=True, axis_index_groups=groups)


def layer(
    tokens,
    norm_gain,
    query_weight,
    key_weight,
    value_weight,
    decay_weight,
    removal_weight,
    gate_weight,
    key_gain,
    removal_gain,
    removal_bias,
    decay_bias,
    decay_extra,
    scan_norm_gain,
    conv_value_weight,
    conv_gate_weight,
    conv_taps,
    conv_bias,
    conv_norm_gain,
    out_scan_weight,
    out_conv_weight,
):
    index = lax.axis_index("sp").astype(jnp.int32)[None]
    row = lambda v: v.reshape(1, -1)

    packed = pack(
        query_weight,
        key_weight,
        value_weight,
        decay_weight,
        removal_weight,
        gate_weight,
        conv_value_weight,
        conv_gate_weight,
        out_scan_weight.T,
        out_conv_weight.T,
    )
    plane = to_each(packed, FAR)
    whole = lax.all_gather(tokens, "tp")
    table, extra = on_core(
        table_kernel,
        (vmem((40, 128), F32), vmem((LENGTH, 128), F32)),
        index,
        given=(
            row(key_gain),
            row(removal_gain),
            row(removal_bias),
            row(decay_bias),
            row(scan_norm_gain),
            row(conv_bias),
            row(conv_norm_gain),
            conv_taps,
            decay_extra,
        ),
    )
    normed = on_core(
        norm_kernel, vmem((2, LENGTH, 1024), BF16), index, whole, given=(norm_gain.reshape(4, 512),)
    )
    pieces = [plane]
    for along_z, along_y in FLIPS[1:]:
        pieces.append(lax.ppermute(pieces[0], "sp", neighbours(along_z, along_y)))
    swapped = []
    for piece in pieces:
        swapped.append(lax.ppermute(piece, "sp", SWAP))
    half = on_core(
        half_kernel,
        vmem((MATS // 2, LENGTH, 256), F32),
        index,
        *pieces,
        normed,
        scratch=[pltpu.VMEM(WEIGHTS, BF16)],
        limit=16,
    )
    mine, theirs, gate, conv_input, rim, tables, solved, steps = on_core(
        local_kernel,
        (
            vmem((HEAD, 128), F32),
            vmem((HEAD, 128), F32),
            vmem((LENGTH, 128), F32),
            vmem((LENGTH, 128), BF16),
            vmem((32, 128), BF16),
            vmem((5, LENGTH, 128), F32),
            vmem((2, LENGTH, 128), F32),
            vmem((2, 5, HEAD, 128), F32),
        ),
        index,
        *swapped,
        normed,
        half,
        table,
        extra,
        scratch=[pltpu.VMEM(WEIGHTS, BF16)],
        limit=28,
    )

    theirs = lax.ppermute(theirs, "sp", SWAP)
    rim = lax.ppermute(rim, "sp", ONWARD)
    message = vmem((8, HEAD, 128), BF16)
    step = vmem((HEAD, 128), F32)
    chip = on_core(chip_kernel, message, index, mine, theirs)
    chips = to_each(chip, Y_AXIS)
    before, total = on_core(row_kernel, (step, message), index, chips)
    totals = to_each(total, Z_AXIS)
    own_state, sent_state = on_core(
        incoming_kernel, (step, step), index, totals, before, mine, theirs
    )
    other_state = lax.ppermute(sent_state, "sp", SWAP)

    filtered, sums = on_core(
        conv_kernel, (vmem((LENGTH, 128), F32), vmem((8, 128), F32)), index, conv_input, rim, table
    )
    shares = lax.all_gather(sums, "tp")
    reads = on_core(
        reads_kernel, vmem((2, LENGTH, 128), F32), index, tables, solved, steps, limit=12
    )
    columns = on_core(columns_kernel, vmem((2048, 256), BF16), index, *pieces, *swapped)

    terms = on_core(
        final_kernel,
        vmem((4, LENGTH, 512), BF16),
        index,
        reads,
        own_state,
        other_state,
        gate,
        filtered,
        shares,
        columns,
        table,
    )
    parts = lax.all_to_all(terms, "tp", 0, 0, tiled=True)
    return jnp.sum(parts.astype(F32), axis=0).astype(BF16)


def solution(mesh):
    weights = P("sp", "tp")
    in_specs = (
        (P("sp", "tp"), P())
        + (weights,) * 6
        + (P("tp"),) * 4
        + (P("sp", "tp"), P("tp"), weights, weights, P(None, "tp"), P("tp"), P("tp"))
        + (P("tp", "sp"), P("tp", "sp"))
    )
    return jax.shard_map(
        layer, mesh=mesh, in_specs=in_specs, out_specs=P("sp", "tp"), check_vma=False
    )
```

```python
import functools

import jax
import jax.numpy as jnp
from jax import lax
from jax.experimental import pallas as pl
from jax.experimental.pallas import tpu as pltpu
from jax.sharding import PartitionSpec as P

HEAD = 64
TAPS = 31
BLOCK = 32
LENGTH = 192
BLOCKS = LENGTH // BLOCK
MATS = 8
F32 = jnp.float32
BF16 = jnp.bfloat16

NN = (((1,), (0,)), ((), ()))
NT = (((1,), (1,)), ((), ()))
TN = (((0,), (0,)), ((), ()))


def place(z, y, c):
    return z * 16 + y * 2 + c


SETS = (((0, 2, 5, 7), (1, 3, 4, 6)), ((1, 3, 6, 0), (2, 4, 5, 7)))
FAR = [
    [place(z, y, c) for z in SETS[c][p] for y in SETS[c][q]]
    for c in range(2)
    for p in range(2)
    for q in range(2)
]


def partner(v, c):
    return v ^ 1 if c == 0 else (((v - 1) % 8 ^ 1) + 1) % 8


def neighbours(along_z, along_y):
    return [
        (place(z, y, c), place(partner(z, c) if along_z else z, partner(y, c) if along_y else y, c))
        for z in range(8)
        for y in range(8)
        for c in range(2)
    ]


Y_AXIS = [[place(z, y, c) for y in range(8)] for z in range(8) for c in range(2)]
Z_AXIS = [[place(z, y, c) for z in range(8)] for y in range(8) for c in range(2)]
SWAP = [(i, i ^ 1) for i in range(128)]
ONWARD = [(i, i + 1) for i in range(127)]


def split(x):
    high = x.astype(BF16)
    return high, (x - high.astype(F32)).astype(BF16)


def dot3(a, b, dims=NN):
    a_high, a_low = split(a)
    b_high, b_low = split(b)
    one = functools.partial(lax.dot_general, dimension_numbers=dims, preferred_element_type=F32)
    return one(a_high, b_high) + (one(a_high, b_low) + one(a_low, b_high))


def exact(a, b, dims=NN):
    return lax.dot_general(
        a, b, dims, precision=lax.Precision.HIGHEST, preferred_element_type=F32
    )


def sums_of(ones, x):
    high = x.astype(BF16)
    middle, low = split(x - high.astype(F32))
    one = lambda part: jnp.dot(ones, part, preferred_element_type=F32)
    return one(high) + (one(middle) + one(low))


def iota(shape, dim):
    return lax.broadcasted_iota(jnp.int32, shape, dim)


def vmem(shape, dtype):
    return pltpu.VMEM(shape, dtype)


def on_core(kernel, shapes, index, *operands, given=(), scratch=(), limit=8):
    return pl.pallas_call(
        kernel,
        in_specs=[pl.BlockSpec(memory_space=pltpu.SMEM)]
        + [pl.BlockSpec(memory_space=pltpu.VMEM)] * (len(operands) + len(given)),
        out_shape=shapes,
        scratch_shapes=scratch,
        compiler_params=pltpu.CompilerParams(vmem_limit_bytes=limit * 1024 * 1024),
    )(index, *(pltpu.with_memory_space_constraint(x, pltpu.VMEM) for x in operands), *given)


def pack_kernel(*refs):
    out = refs[-1]
    blocks = [ref[...] for ref in refs[:-1]]
    both = jnp.concatenate(blocks, axis=0)
    for k in range(16):
        out[k] = both


def pack(*mats):
    return pl.pallas_call(
        pack_kernel,
        out_shape=jax.ShapeDtypeStruct((16, 16 * len(mats), 128), BF16),
        name="pack",
    )(*mats)


FLIPS = ((0, 0), (0, 1), (1, 0), (1, 1))


def chosen(conditions, values):
    if not conditions:
        return values[0]
    half = len(values) // 2
    low, high = (chosen(conditions[1:], part) for part in (values[:half], values[half:]))
    return low if isinstance(low, int) and low == high else jnp.where(conditions[0], high, low)


def fill_rows(index, core, pieces, height, store):
    second = core == 1

    def axis(position):
        in_set1 = functools.reduce(
            jnp.logical_or,
            [
                jnp.logical_and(second == (c == 1), position == v)
                for c in range(2)
                for v in SETS[c][1]
            ],
        )
        return [
            [
                chosen(
                    (second, in_set1),
                    [SETS[c][p ^ flip][k] for c in range(2) for p in range(2)],
                )
                for k in range(4)
            ]
            for flip in range(2)
        ]

    zs, ys = axis(index // 16), axis((index // 2) % 8)
    for piece, (flip_z, flip_y) in zip(pieces, FLIPS):
        for b in range(16):
            row = height(zs[flip_z][b // 4], ys[flip_y][b % 4], core)
            store(pl.multiple_of(row, 16), piece, b)


def table_kernel(place_ref, *refs):
    vectors, taps_ref, extra_ref, table_ref, extra_out_ref = refs[:-4], *refs[-4:]
    for k, ref in enumerate(vectors):
        table_ref[k : k + 1, :] = ref[...]
    table_ref[8 : 8 + TAPS, :] = taps_ref[...]
    extra_out_ref[...] = extra_ref[...]


def norm_kernel(place_ref, tokens_ref, gain_ref, normed_ref):
    parts = [tokens_ref[j].astype(F32) for j in range(4)]
    total = sum(jnp.sum(part * part, axis=-1, keepdims=True) for part in parts)
    inverse_rms = lax.rsqrt(total * (1.0 / 2048.0) + 1e-06)
    goal = iota((256, 256), 1)
    source = ((goal % 128) // 16) * 32 + (goal // 128) * 16 + goal % 16
    moves = jnp.where(iota((256, 256), 0) == source, 1.0, 0.0).astype(BF16)
    for j, part in enumerate(parts):
        normed = (part * inverse_rms * gain_ref[j : j + 1, :]).astype(BF16)
        for h in range(2):
            moved = jnp.dot(
                normed[:, h * 256 : h * 256 + 256], moves, preferred_element_type=F32
            ).astype(BF16)
            z = j * 2 + h
            normed_ref[0, :, z * 128 : z * 128 + 128] = moved[:, :128]
            normed_ref[1, :, z * 128 : z * 128 + 128] = moved[:, 128:]


def projected(index, core, pieces, normed_ref, weights):
    def store(row, piece, b):
        for m in range(MATS):
            lanes = slice((m % 2) * 128, (m % 2) * 128 + 128)
            weights[m // 2, pl.ds(row, 16), lanes] = piece[b, m * 16 : m * 16 + 16, :]

    fill_rows(index, core, pieces, lambda z, y, c: (z * 8 + y) * 16, store)
    normed = normed_ref[core % 2]
    return [jnp.dot(normed, weights[p], preferred_element_type=F32) for p in range(MATS // 2)]


def half_kernel(place_ref, p0, p1, p2, p3, normed_ref, out_ref, weights):
    index = place_ref[0]
    products = projected(index, index % 2, (p0, p1, p2, p3), normed_ref, weights)
    for p in range(MATS // 2):
        out_ref[p] = products[p]


def local_kernel(
    core_ref,
    p0,
    p1,
    p2,
    p3,
    normed_ref,
    half_ref,
    table_ref,
    extra_ref,
    mine_ref,
    theirs_ref,
    gate_ref,
    conv_ref,
    rim_ref,
    tables_ref,
    solved_ref,
    steps_ref,
    weights,
):
    core = core_ref[0] % 2
    products = []
    others = projected(core_ref[0], 1 - core, (p0, p1, p2, p3), normed_ref, weights)
    for p, product in enumerate(others):
        product = (product + half_ref[p]).astype(BF16).astype(F32)
        products += [product[:, :128], product[:, 128:]]
    recept, keys, values, decay_pre, removal_pre, gate_pre, conv_value, conv_gate = products
    key_gain, removal_gain, removal_bias, decay_bias, norm_out = (
        table_ref[k : k + 1, :] for k in range(5)
    )
    gate_ref[...] = norm_out * jax.nn.sigmoid(gate_pre)
    conv_input = (conv_value * jax.nn.sigmoid(conv_gate)).astype(BF16)
    conv_ref[...] = conv_input
    rim_ref[...] = conv_input[LENGTH - 32 :]

    rate = 0.6065306597126334 * jax.nn.sigmoid(decay_bias + decay_pre) + extra_ref[...]
    removal = jax.nn.sigmoid(removal_bias + removal_pre)
    lane = iota((LENGTH, 128), 1)
    first = lane < HEAD
    scaled = keys * key_gain
    square = scaled * scaled
    low = jnp.sum(jnp.where(first, square, 0.0), axis=-1, keepdims=True)
    high = jnp.sum(jnp.where(first, 0.0, square), axis=-1, keepdims=True)
    unit = scaled * lax.rsqrt(jnp.where(first, low, high) + 1e-06)
    written = keys * (1.0 + (removal - 1.0) * removal_gain)

    row, column = iota((LENGTH, LENGTH), 0), iota((LENGTH, LENGTH), 1)
    same = (row // BLOCK) == (column // BLOCK)
    strict = same & (row > column)
    inclusive = same & (row >= column)
    falling = -sums_of(jnp.where(inclusive, 1.0, 0.0).astype(BF16), rate)
    before = falling + rate
    by_block = falling.reshape(BLOCKS, BLOCK, 128)
    middle = jnp.broadcast_to(
        by_block[:, BLOCK // 2 : BLOCK // 2 + 1], (BLOCKS, BLOCK, 128)
    ).reshape(LENGTH, 128)
    ending = jnp.broadcast_to(by_block[:, BLOCK - 1 :], (BLOCKS, BLOCK, 128)).reshape(LENGTH, 128)
    beta = unit * removal
    rising = jnp.exp(middle - falling)
    alpha_mid = -unit * jnp.exp(before - middle)
    tables_ref[0] = recept * jnp.exp(falling - middle)
    right = jnp.concatenate([beta * rising, written * rising], axis=0)
    start_alpha = -unit * jnp.exp(before)
    tables_ref[1] = recept * jnp.exp(falling)
    closing = jnp.exp(ending - falling)
    end_beta = beta * closing
    end_keys = written * closing
    kept = jnp.exp(by_block[:, BLOCK - 1, :])
    turned_values = pltpu.roll(values, HEAD, 1)
    tables_ref[2] = right[:LENGTH]
    tables_ref[3] = right[LENGTH:]
    tables_ref[4] = turned_values

    square_row, square_lane = iota((128, 128), 0), iota((128, 128), 1)
    diagonal = square_row == square_lane
    own = [first, jnp.logical_not(first)]
    own_row = [square_row < HEAD, square_row >= HEAD]
    power, solved, value_rows = [], [], []
    for h in range(2):
        pairs = dot3(jnp.where(own[h], alpha_mid, 0.0), right, NT)
        power.append(jnp.where(strict, pairs[:, :LENGTH], 0.0))
        alpha_keys = jnp.where(strict, pairs[:, LENGTH:], 0.0)
        value_rows.append(jnp.where(own[h], 0.0, turned_values))
        solved.append(jnp.where(own[h], start_alpha, dot3(alpha_keys, value_rows[h])))
    for step in range(5):
        solved = [solved[h] + dot3(power[h], solved[h]) for h in range(2)]
        if step < 4:
            power = [dot3(power[h], power[h]) for h in range(2)]
    for h in range(2):
        solved_ref[h] = solved[h]
    steps = [[], []]
    whole = jnp.where(diagonal, 1.0, 0.0)
    for b in range(BLOCKS):
        rows = slice(b * BLOCK, b * BLOCK + BLOCK)
        ends = jnp.concatenate([end_beta[rows], end_keys[rows]], axis=0)
        held = jnp.where(diagonal, jnp.broadcast_to(kept[b : b + 1], (128, 128)), 0.0)
        for h in range(2):
            known = jnp.concatenate([solved[h][rows], value_rows[h][rows]], axis=0)
            steps[h].append(jnp.where(own_row[h], dot3(ends, known, TN) + held, whole))
    one = [dot3(steps[h][1], steps[h][0]) for h in range(2)]
    two = [dot3(steps[h][3], steps[h][2]) for h in range(2)]
    three = [dot3(steps[h][5], steps[h][4]) for h in range(2)]
    four = [dot3(two[h], one[h]) for h in range(2)]
    finals = [dot3(three[h], four[h])[h * HEAD : h * HEAD + HEAD] for h in range(2)]
    finals[1] = pltpu.roll(finals[1], HEAD, 1)
    mine_ref[...] = jnp.where(core == 0, finals[0], finals[1])
    theirs_ref[...] = jnp.where(core == 0, finals[1], finals[0])
    for h in range(2):
        for k, step in enumerate((steps[h][0], one[h], steps[h][2], four[h], steps[h][4])):
            steps_ref[h, k] = step[h * HEAD : h * HEAD + HEAD]


def reads_kernel(place_ref, tables_ref, solved_ref, steps_ref, reads_ref):
    recept_mid, start_recept, turned_values = tables_ref[0], tables_ref[1], tables_ref[4]
    right = jnp.concatenate([tables_ref[2], tables_ref[3]], axis=0)
    first = iota((LENGTH, 128), 1) < HEAD
    wide_row, wide_column = iota((LENGTH, 2 * LENGTH), 0), iota((LENGTH, 2 * LENGTH), 1)
    wide_column = jnp.where(wide_column >= LENGTH, wide_column - LENGTH, wide_column)
    inclusive_twice = ((wide_row // BLOCK) == (wide_column // BLOCK)) & (wide_row >= wide_column)
    own = [first, jnp.logical_not(first)]
    query = []
    for h in range(2):
        pairs = dot3(jnp.where(own[h], recept_mid, 0.0), right, NT)
        pairs = jnp.where(inclusive_twice, pairs, 0.0)
        known = jnp.concatenate(
            [solved_ref[h], jnp.where(own[h], 0.0, turned_values)], axis=0
        )
        query.append(jnp.where(own[h], start_recept, 0.0) + dot3(pairs, known))
    lane, equal = iota((HEAD, 128), 1), iota((HEAD, 128), 0)
    for h in range(2):
        rest = jnp.where(lane == equal + (HEAD if h == 0 else 0), 1.0, 0.0)
        zero, one, two, four, five = (
            jnp.concatenate(
                [steps_ref[h, k], rest] if h == 0 else [rest, steps_ref[h, k]], axis=0
            )
            for k in range(5)
        )
        prefixes = (None, zero, one, dot3(two, one), four, dot3(five, four))
        reads_ref[h, 0:BLOCK, :] = query[h][0:BLOCK]
        for b in range(1, BLOCKS):
            rows = slice(b * BLOCK, b * BLOCK + BLOCK)
            reads_ref[h, rows, :] = dot3(query[h][rows], prefixes[b])


WEIGHTS = (MATS // 2, 1024, 256)


def after(later, earlier):
    product = dot3(later[:, :HEAD], earlier)
    return product + jnp.where(iota((HEAD, 128), 1) < HEAD, 0.0, later)


def chained(steps):
    while len(steps) > 1:
        steps = [after(steps[k + 1], steps[k]) for k in range(0, len(steps), 2)]
    return steps[0]


def nothing():
    return jnp.where(iota((HEAD, 128), 0) == iota((HEAD, 128), 1), 1.0, 0.0)


def sent(step):
    return jnp.broadcast_to((step - nothing()).astype(BF16)[None], (8, HEAD, 128))


def received(steps_ref):
    return [steps_ref[k].astype(F32) + nothing() for k in range(8)]


def chip_kernel(core_ref, mine_ref, theirs_ref, out_ref):
    core = core_ref[0] % 2
    mine, theirs = mine_ref[...], theirs_ref[...]
    earlier = jnp.where(core == 0, mine, theirs)
    later = jnp.where(core == 0, theirs, mine)
    out_ref[...] = sent(after(later, earlier))


def row_kernel(place_ref, steps_ref, before_ref, total_ref):
    here = (place_ref[0] // 2) % 8
    steps = received(steps_ref)
    total_ref[...] = sent(chained(steps))
    before_ref[...] = chained([jnp.where(k < here, steps[k], nothing()) for k in range(8)])


def incoming_kernel(place_ref, steps_ref, before_ref, mine_ref, theirs_ref, own_ref, sent_ref):
    here, core = place_ref[0] // 16, place_ref[0] % 2
    steps = received(steps_ref)
    start = chained([jnp.where(k < here, steps[k], nothing()) for k in range(8)])
    at_chip = after(before_ref[...], start)
    earlier = jnp.where(core == 0, mine_ref[...], theirs_ref[...])
    at_second = after(earlier, at_chip)
    own_ref[...] = jnp.where(core == 0, at_chip, at_second)
    sent_ref[...] = jnp.where(core == 0, at_second, at_chip)


def conv_kernel(place_ref, input_ref, rim_ref, table_ref, filtered_ref, sums_ref):
    padded = jnp.concatenate([rim_ref[...], input_ref[...]], axis=0).astype(F32)
    filtered = jnp.broadcast_to(table_ref[5:6, :], (LENGTH, 128))
    for k in range(TAPS):
        filtered = filtered + table_ref[8 + k : 9 + k, :] * padded[k + 2 : k + 2 + LENGTH]
    filtered_ref[...] = filtered
    ones = jnp.ones((8, 128), F32)
    square = filtered * filtered
    rest = jnp.concatenate([filtered[128:], square[128:]], axis=0)
    at = iota((8, 128), 0)
    sums = jnp.where(at == 0, exact(ones, filtered[:128], NT), 0.0)
    sums = jnp.where(at == 1, exact(ones, square[:128], NT), sums)
    sums_ref[...] = jnp.where(at == 2, exact(ones, rest, NT), sums)


def columns_kernel(core_ref, *refs):
    index, out_ref = core_ref[0], refs[-1]
    core = index % 2

    def store(row, piece, b):
        for m in range(2):
            at = (MATS + m) * 16
            out_ref[pl.ds(row, 16), m * 128 : m * 128 + 128] = piece[b, at : at + 16, :]

    height = lambda z, y, c: place(z, y, c) * 16
    fill_rows(index, core, refs[:4], height, store)
    fill_rows(index, 1 - core, refs[4:8], height, store)


def final_kernel(
    core_ref,
    reads_ref,
    mine_ref,
    theirs_ref,
    gate_ref,
    filtered_ref,
    sums_ref,
    columns_ref,
    table_ref,
    out_ref,
):
    core = core_ref[0] % 2
    mine, theirs = mine_ref[...], theirs_ref[...]
    head0 = jnp.where(core == 0, mine, theirs)
    head1 = jnp.where(core == 0, theirs, mine)
    lane = iota((HEAD, 128), 1)
    equal = iota((HEAD, 128), 0)
    zero = jnp.zeros((HEAD, 128), F32)
    right0 = jnp.concatenate(
        [
            jnp.where(lane < HEAD, pltpu.roll(head0, HEAD, 1), zero),
            jnp.where(lane == equal, 1.0, 0.0),
        ],
        axis=0,
    )
    right1 = jnp.concatenate(
        [jnp.where(lane == equal + HEAD, 1.0, 0.0), jnp.where(lane < HEAD, zero, head1)], axis=0
    )
    reads = exact(reads_ref[0], right0) + exact(reads_ref[1], right1)
    first = iota((LENGTH, 128), 1) < HEAD

    def head_mean(x):
        low = jnp.sum(jnp.where(first, x, 0.0), axis=-1, keepdims=True)
        high = jnp.sum(jnp.where(first, 0.0, x), axis=-1, keepdims=True)
        return jnp.where(first, low, high) * (1.0 / HEAD)

    centered = reads - head_mean(reads)
    spread = head_mean(centered * centered)
    scan_out = (centered * lax.rsqrt(spread + 0.00064) * gate_ref[...]).astype(BF16)

    sums = sums_ref[...]

    def spread_out(k):
        return exact(sums, jnp.where(iota((8, 128), 0) == k, 1.0 / 512.0, 0.0), TN)

    rest = spread_out(2)
    center = jnp.concatenate([spread_out(0), rest[:64]], axis=0)
    second = jnp.concatenate([spread_out(1), rest[64:]], axis=0)
    scaled = (
        (filtered_ref[...] - center)
        * lax.rsqrt(second - center * center + 1e-05)
        * table_ref[6:7, :]
    )
    conv_out = (scaled * jax.nn.sigmoid(scaled)).astype(BF16)
    features = jnp.concatenate([scan_out, conv_out], axis=1)
    for j in range(4):
        out_ref[j] = lax.dot_general(
            features, columns_ref[j * 512 : j * 512 + 512, :], NT, preferred_element_type=F32
        ).astype(BF16)


def to_each(x, groups):
    return lax.all_to_all(x, "sp", 0, 0, tiled=True, axis_index_groups=groups)


def layer(
    tokens,
    norm_gain,
    query_weight,
    key_weight,
    value_weight,
    decay_weight,
    removal_weight,
    gate_weight,
    key_gain,
    removal_gain,
    removal_bias,
    decay_bias,
    decay_extra,
    scan_norm_gain,
    conv_value_weight,
    conv_gate_weight,
    conv_taps,
    conv_bias,
    conv_norm_gain,
    out_scan_weight,
    out_conv_weight,
):
    index = lax.axis_index("sp").astype(jnp.int32)[None]
    row = lambda v: v.reshape(1, -1)

    packed = pack(
        query_weight,
        key_weight,
        value_weight,
        decay_weight,
        removal_weight,
        gate_weight,
        conv_value_weight,
        conv_gate_weight,
        out_scan_weight.T,
        out_conv_weight.T,
    )
    plane = to_each(packed, FAR)
    whole = lax.all_gather(tokens, "tp")
    table, extra = on_core(
        table_kernel,
        (vmem((40, 128), F32), vmem((LENGTH, 128), F32)),
        index,
        given=(
            row(key_gain),
            row(removal_gain),
            row(removal_bias),
            row(decay_bias),
            row(scan_norm_gain),
            row(conv_bias),
            row(conv_norm_gain),
            conv_taps,
            decay_extra,
        ),
    )
    normed = on_core(
        norm_kernel, vmem((2, LENGTH, 1024), BF16), index, whole, given=(norm_gain.reshape(4, 512),)
    )
    pieces = [plane]
    for along_z, along_y in FLIPS[1:]:
        pieces.append(lax.ppermute(pieces[0], "sp", neighbours(along_z, along_y)))
    swapped = []
    for piece in pieces:
        swapped.append(lax.ppermute(piece, "sp", SWAP))
    half = on_core(
        half_kernel,
        vmem((MATS // 2, LENGTH, 256), F32),
        index,
        *pieces,
        normed,
        scratch=[pltpu.VMEM(WEIGHTS, BF16)],
        limit=16,
    )
    mine, theirs, gate, conv_input, rim, tables, solved, steps = on_core(
        local_kernel,
        (
            vmem((HEAD, 128), F32),
            vmem((HEAD, 128), F32),
            vmem((LENGTH, 128), F32),
            vmem((LENGTH, 128), BF16),
            vmem((32, 128), BF16),
            vmem((5, LENGTH, 128), F32),
            vmem((2, LENGTH, 128), F32),
            vmem((2, 5, HEAD, 128), F32),
        ),
        index,
        *swapped,
        normed,
        half,
        table,
        extra,
        scratch=[pltpu.VMEM(WEIGHTS, BF16)],
        limit=28,
    )

    theirs = lax.ppermute(theirs, "sp", SWAP)
    rim = lax.ppermute(rim, "sp", ONWARD)
    message = vmem((8, HEAD, 128), BF16)
    step = vmem((HEAD, 128), F32)
    chip = on_core(chip_kernel, message, index, mine, theirs)
    chips = to_each(chip, Y_AXIS)
    before, total = on_core(row_kernel, (step, message), index, chips)
    totals = to_each(total, Z_AXIS)
    own_state, sent_state = on_core(
        incoming_kernel, (step, step), index, totals, before, mine, theirs
    )
    other_state = lax.ppermute(sent_state, "sp", SWAP)

    filtered, sums = on_core(
        conv_kernel, (vmem((LENGTH, 128), F32), vmem((8, 128), F32)), index, conv_input, rim, table
    )
    sums = lax.psum(sums, "tp")
    reads = on_core(
        reads_kernel, vmem((2, LENGTH, 128), F32), index, tables, solved, steps, limit=12
    )
    columns = on_core(columns_kernel, vmem((2048, 256), BF16), index, *pieces, *swapped)

    terms = on_core(
        final_kernel,
        vmem((4, LENGTH, 512), BF16),
        index,
        reads,
        own_state,
        other_state,
        gate,
        filtered,
        sums,
        columns,
        table,
    )
    parts = lax.all_to_all(terms, "tp", 0, 0, tiled=True)
    return jnp.sum(parts.astype(F32), axis=0).astype(BF16)


def solution(mesh):
    weights = P("sp", "tp")
    in_specs = (
        (P("sp", "tp"), P())
        + (weights,) * 6
        + (P("tp"),) * 4
        + (P("sp", "tp"), P("tp"), weights, weights, P(None, "tp"), P("tp"), P("tp"))
        + (P("tp", "sp"), P("tp", "sp"))
    )
    return jax.shard_map(
        layer, mesh=mesh, in_specs=in_specs, out_specs=P("sp", "tp"), check_vma=False
    )
```
